32 devices in a mesh: grp: 2 (over y), sp: 4 (over z), tp: 4 (over x, core).
Axes of the slice: x: 2, y: 2, z: 4, core: 2. Of those that a mesh axis runs over, the one named last changes fastest.
Arguments:
- resid: bfloat16 [5120, 2048], P(('grp', 'sp'), 'tp'), parts along dimension 0, may hold values from -6 to 6
- queries: bfloat16 [5120, 2048], P(('grp', 'sp'), 'tp'), parts along dimension 0, may hold values from -150 to 150
- keys_values: bfloat16 [5120, 8, 128], P(('grp', 'sp'), 'tp'), parts along dimension 0, may hold values from -4.5 to 4.5
- sink: float32 [32], P('tp'), may hold values from 3 to 7
- out_weight: bfloat16 [2048, 2048], P('tp'), may hold values from -2.390625 to 2.390625
- norm_gain: float32 [2048], replicated, may hold values from 0.1 to 1.9
- gate_weight: bfloat16 [2048, 5632], P('sp', 'tp'), may hold values from -0.125 to 0.125
- up_weight: bfloat16 [2048, 5632], P('sp', 'tp'), may hold values from -0.125 to 0.125
- down_weight: bfloat16 [5632, 2048], P('tp', 'sp'), may hold values from -0.078125 to 0.078125
Outputs:
- mixed: bfloat16 [5120, 2048], P(('grp', 'sp'), 'tp'), parts along dimension 0
The draws below stay inside these ranges and needn't reach their ends.
There are 2 independent parts, one for each index of `grp`. The reference program is written for one: setup_inputs(seed, part) draws one part's arguments, and reference() takes and returns one part's arrays. A program takes and returns all parts, laid end to end along the dimension named above; an argument that names none is the same for every part. Nothing has to cross between parts.
All inputs are finite; a program needn't handle non-finite values.
Results may differ from the reference program's by a relative error of at most 0.008.
Values may be sent and summed in bfloat16 or wider, within the bound.
A program may use at most 128 MiB of HBM per device.

```python
import jax
import jax.numpy as jnp
from jax import lax

D = 2048
HEADS = 32
KV_HEADS = 8
HEAD_DIM = 64
FF = 5632
WINDOW = 128
GRID_W = 64
TOKENS = 2560


def joint_draw(key):
    both = jnp.clip(jax.random.normal(jax.random.fold_in(key, 11), (TOKENS, KV_HEADS, 2 * HEAD_DIM), jnp.float32), -4.5, 4.5)
    drawn = jnp.clip(jax.random.normal(jax.random.fold_in(key, 12), (TOKENS, HEADS * HEAD_DIM), jnp.float32), -4.5, 4.5)
    return (drawn, both)


def draw_queries(key, part):
    drawn, both = joint_draw(key)
    return drawn.astype(jnp.bfloat16)


def draw_keys_values(key, part):
    drawn, both = joint_draw(key)
    return both.astype(jnp.bfloat16)


def shard_levels(rng, extent, split, smallest, largest):
    gain, own = 1.0, jax.random.fold_in(rng, 6)
    for dim, blocks in split:
        steps = jnp.exp(jax.random.uniform(jax.random.fold_in(own, dim), (blocks,), jnp.float32, smallest / len(split), largest / len(split)))
        gain = gain * jnp.repeat(steps, extent[dim] // blocks).reshape([-1 if axis == dim else 1 for axis in range(len(extent))])
    return gain


def normal_values(key, dims, deviation, most, split=(), held_as=jnp.bfloat16):
    entries = jax.random.normal(key, dims, jnp.float32) * deviation
    if len(split) > 0:
        entries = shard_levels(key, dims, split, -0.22, 0.18) * entries
    return jnp.clip(entries, min=-most, max=most).astype(held_as)


def setup_inputs(seed: int = 0, part: int = 0) -> dict:
    streams_of = jax.random.split(jax.random.key(seed), 10)
    part_keys = jax.random.split(jax.random.fold_in(streams_of[9], part), 10)
    return {
        "resid": normal_values(part_keys[0], (TOKENS, D), 1.0, 6.0, ((0, 4), (1, 4))),
        "queries": draw_queries(jax.random.fold_in(jax.random.fold_in(streams_of[9], part), 71), part),
        "keys_values": draw_keys_values(jax.random.fold_in(jax.random.fold_in(streams_of[9], part), 71), part),
        "sink": jnp.clip(3.0 + 4.0 * jax.random.uniform(streams_of[3], (HEADS,), jnp.float32) ** shard_levels(streams_of[3], (HEADS,), ((0, 4),), -0.2, 0.2), 3.0, 7.0),
        "out_weight": normal_values(streams_of[4], (HEADS * HEAD_DIM, D), 0.4, 2.390625, ((0, 4),)),
        "norm_gain": jnp.clip(1.0 + 0.18 * jax.random.normal(streams_of[5], (D,), jnp.float32), 0.1, 1.9),
        "gate_weight": normal_values(streams_of[6], (D, FF), D ** -0.5, 0.125, ((0, 4), (1, 4))),
        "up_weight": normal_values(streams_of[7], (D, FF), D ** -0.5, 0.125, ((0, 4), (1, 4))),
        "down_weight": normal_values(streams_of[8], (FF, D), FF ** -0.5, 0.078125, ((0, 4), (1, 4))),
    }


def rotate(values, positions):
    quarter = 16
    inverse = 10000.0 ** (-jnp.arange(quarter, dtype=jnp.float32) / quarter)

    def turn(part, place):
        angle = place.astype(jnp.float32)[:, None] * inverse[None, :]
        cosine = jnp.cos(angle)[:, None, :]
        sine = jnp.sin(angle)[:, None, :]
        first, second = (part[..., :quarter], part[..., quarter:])
        return jnp.concatenate([first * cosine - second * sine, second * cosine + first * sine], axis=-1)
    grid_row = positions // GRID_W
    grid_col = positions % GRID_W
    return jnp.concatenate([turn(values[..., :32], grid_row), turn(values[..., 32:], grid_col)], axis=-1)

def reference(resid, queries, keys_values, sink, out_weight, norm_gain, gate_weight, up_weight, down_weight):
    group = HEADS // KV_HEADS
    positions = jnp.arange(TOKENS, dtype=jnp.int32)
    rotated_q = rotate(queries.astype(jnp.float32).reshape(TOKENS, HEADS, HEAD_DIM), positions).astype(jnp.bfloat16)
    rotated_k = rotate(keys_values[..., :HEAD_DIM].astype(jnp.float32), positions).astype(jnp.bfloat16)
    padded_k = jnp.pad(rotated_k, ((WINDOW, WINDOW), (0, 0), (0, 0)))
    padded_v = jnp.pad(keys_values[..., HEAD_DIM:], ((WINDOW, WINDOW), (0, 0), (0, 0)))
    sink_grid = sink.reshape(KV_HEADS, group)[:, :, None]

    def block(index):
        start = (index * WINDOW).astype(jnp.int32)
        zero = jnp.int32(0)
        query_block = lax.dynamic_slice(rotated_q, (start, zero, zero), (WINDOW, HEADS, HEAD_DIM))
        key_block = lax.dynamic_slice(padded_k, (start, zero, zero), (3 * WINDOW, KV_HEADS, HEAD_DIM))
        value_block = lax.dynamic_slice(padded_v, (start, zero, zero), (3 * WINDOW, KV_HEADS, HEAD_DIM))
        grouped = query_block.astype(jnp.float32).reshape(WINDOW, KV_HEADS, group, HEAD_DIM)
        scores = jnp.einsum('qkgd,jkd->kgqj', grouped, key_block.astype(jnp.float32)) * HEAD_DIM ** (-0.5)
        query_pos = start + jnp.arange(WINDOW, dtype=jnp.int32)
        key_pos = start - WINDOW + jnp.arange(3 * WINDOW, dtype=jnp.int32)
        valid = (jnp.abs(query_pos[:, None] - key_pos[None, :]) <= WINDOW) & (key_pos[None, :] >= 0) & (key_pos[None, :] < TOKENS)
        scores = jnp.where(valid[None, None], scores, jnp.float32(-1e+30))
        top = jnp.maximum(lax.optimization_barrier(jnp.max(scores, axis=-1)), sink_grid)
        expo = jnp.exp(scores - top[..., None])
        total = lax.optimization_barrier(jnp.sum(expo, axis=-1)) + jnp.exp(sink_grid - top)
        probs = (expo / total[..., None]).astype(jnp.bfloat16)
        result = jnp.einsum('kgqj,jkd->qkgd', probs.astype(jnp.float32), value_block.astype(jnp.float32))
        return result.astype(jnp.bfloat16).reshape(WINDOW, HEADS * HEAD_DIM)
    attended = lax.map(block, jnp.arange(TOKENS // WINDOW, dtype=jnp.int32)).reshape(TOKENS, HEADS * HEAD_DIM)
    stream = (resid.astype(jnp.float32) + jnp.dot(attended, out_weight, preferred_element_type=jnp.float32)).astype(jnp.bfloat16)
    widened = stream.astype(jnp.float32)
    normed = (widened * lax.rsqrt(lax.optimization_barrier(jnp.mean(widened * widened, axis=-1, keepdims=True)) + 1e-06) * norm_gain).astype(jnp.bfloat16)
    gate = jnp.dot(normed, gate_weight, preferred_element_type=jnp.float32)
    up = jnp.dot(normed, up_weight, preferred_element_type=jnp.float32)
    hidden = (jax.nn.silu(gate) * up).astype(jnp.bfloat16)
    return (stream.astype(jnp.float32) + jnp.dot(hidden, down_weight, preferred_element_type=jnp.float32)).astype(jnp.bfloat16)
```

```python
import jax
import jax.numpy as jnp
from jax import lax
from jax.experimental import pallas as pl
from jax.experimental.pallas import tpu as pltpu
from jax.sharding import PartitionSpec as P
import numpy as np

HEAD_DIM = 64
WINDOW = 128
GRID_W = 64


def with_halo(cells, sides, width):
    for axis, dim in sides:
        count = lax.axis_size(axis)
        ends = count - 1
        head = lax.slice_in_dim(cells, 0, width, axis=dim)
        tail = lax.slice_in_dim(cells, cells.shape[dim] - width, cells.shape[dim], axis=dim)
        cells = jnp.concatenate(
            [
                lax.ppermute(tail, axis, [(i, (i + 1) % count) for i in range(ends)]),
                cells,
                lax.ppermute(head, axis, [((i + 1) % count, i) for i in range(ends)]),
            ],
            axis=dim,
        )
    return cells


def rotate(values, positions):
    quarter = 16
    inverse = 10000.0 ** (-jnp.arange(quarter, dtype=jnp.float32) / quarter)

    def turn(part, place):
        angle = place.astype(jnp.float32)[:, None] * inverse[None, :]
        cosine = jnp.cos(angle)[:, None, :]
        sine = jnp.sin(angle)[:, None, :]
        first, second = (part[..., :quarter], part[..., quarter:])
        return jnp.concatenate(
            [first * cosine - second * sine, second * cosine + first * sine], axis=-1
        )

    grid_row = positions // GRID_W
    grid_col = positions % GRID_W
    return jnp.concatenate(
        [turn(values[..., :32], grid_row), turn(values[..., 32:], grid_col)], axis=-1
    )


def share(weight, axis):
    parts = lax.axis_size("grp")
    size = weight.shape[axis] // parts
    part = lax.dynamic_slice_in_dim(weight, lax.axis_index("grp") * size, size, axis)
    return lax.all_gather(part, ("sp", "grp"), axis=axis, tiled=True)


def relay(blocks, axes, first_column):
    count, parts = lax.axis_size("sp"), lax.axis_size("grp")
    here, group = lax.axis_index("sp"), lax.axis_index("grp")

    def place(whole, value, axis, block, source, part):
        rows = block.shape[0]
        start = part * (rows // parts)
        at = (source * rows + start, 0)
        if axis == 1:
            columns = block.shape[1] * count
            at = (start, lax.rem(source * block.shape[1] + columns - first_column, columns))
        if axis == 1 and part is not group:
            value = jnp.where(here < count, value, jnp.zeros_like(value))
        return lax.dynamic_update_slice(whole, value, at)

    wholes, right, left, late = [], [], [], []
    for block, axis in zip(blocks, axes):
        shape = list(block.shape)
        shape[axis] *= count
        wholes.append(place(jnp.zeros(shape, block.dtype), block, axis, block, here, 0))
        rows = block.shape[0] // parts
        part = lax.dynamic_slice_in_dim(block, group * rows, rows, 0)
        right.append([part])
        left.append([part])
    for step in range(1, count):
        source = jnp.where(here >= step, here - step, step)
        for index, (block, axis) in enumerate(zip(blocks, axes)):
            right[index].append(
                lax.ppermute(
                    right[index][-1], "sp", [(i, i + 1) for i in range(step - 1, count - 1)]
                )
            )
            left[index].append(
                lax.ppermute(left[index][-1], "sp", [(i + 1, i) for i in range(count - step)])
            )
            came = [left[index][step - i] for i in range(step)] + [right[index][step]]
            value = lax.select_n(jnp.minimum(here, step), *came)
            whole = place(wholes[index], value, axis, block, source, group)
            for shift in range(1, parts):
                other = lax.ppermute(value, "grp", [(i, (i + shift) % parts) for i in range(parts)])
                part = (group - shift) % parts
                if step == count - 1 and index == len(blocks) - 1:
                    late.append((other, axis, block, source, part))
                    continue
                whole = place(whole, other, axis, block, source, part)
            wholes[index] = whole

    def finish(whole):
        for piece in late:
            whole = place(whole, *piece)
        return whole

    return wholes, finish


def swap(value, bit):
    return lax.ppermute(value, "tp", [(i, i ^ bit) for i in range(lax.axis_size("tp"))])


def sum_columns(terms, bit):
    here = lax.axis_index("tp")
    while bit:
        half = terms.shape[1] // 2
        mine = jnp.where((here & bit) > 0, half, 0)
        theirs = lax.dynamic_slice_in_dim(terms, half - mine, half, 1).astype(jnp.bfloat16)
        own = lax.dynamic_slice_in_dim(terms, mine, half, 1)
        terms = own + swap(theirs, bit).astype(jnp.float32)
        bit //= 2
    return terms


def body(
    resid, queries, keys_values, sink, out_weight, norm_gain, gate_weight, up_weight, down_weight
):
    tok = queries.shape[0]
    heads_here = queries.shape[1] // HEAD_DIM
    kv_here = keys_values.shape[1]
    group = heads_here // kv_here
    cols = resid.shape[1]
    offset = lax.axis_index("sp") * tok
    total_tokens = tok * lax.axis_size("sp")
    positions = offset + jnp.arange(tok, dtype=jnp.int32)
    rotated_q = rotate(
        queries.astype(jnp.float32).reshape(tok, heads_here, HEAD_DIM), positions
    ).astype(jnp.bfloat16)
    padded = with_halo(keys_values, (("sp", 0),), WINDOW)
    ranks, members = lax.axis_size("sp"), lax.axis_size("tp")
    high = members // 2
    direct = ranks <= 8 and ranks % 2 == 0 and members >= 2 and members & (members - 1) == 0
    if direct:
        half_columns = resid.shape[1] * members // 2
        near = jnp.where((lax.axis_index("tp") & high) > 0, half_columns, 0)
        padded, gate_weight, up_weight, down_weight = lax.optimization_barrier(
            (padded, gate_weight, up_weight, down_weight)
        )
        both = jnp.concatenate([gate_weight, up_weight], axis=1)
        (whole_both, whole_down), late = relay((both, down_weight), (0, 1), near)
    else:
        whole_both = jnp.concatenate([share(gate_weight, 0), share(up_weight, 0)], axis=1)
        whole_down = share(down_weight, 1)
    whole_out = lax.all_gather(out_weight, "tp", axis=0, tiled=True)
    key_positions = offset - WINDOW + jnp.arange(tok + 2 * WINDOW, dtype=jnp.int32)
    rotated_k = rotate(padded[..., :HEAD_DIM].astype(jnp.float32), key_positions).astype(
        jnp.bfloat16
    )
    padded = jnp.concatenate([rotated_k, padded[..., HEAD_DIM:]], axis=-1)
    blocks = tok // WINDOW
    key_blocks = jnp.stack(
        [padded[index * WINDOW : index * WINDOW + 3 * WINDOW] for index in range(blocks)]
    )
    grouped = rotated_q.reshape(blocks, WINDOW, kv_here, group, HEAD_DIM)
    scores = jnp.einsum(
        "nqkgd,njkd->nkgqj", grouped, key_blocks[..., :HEAD_DIM], preferred_element_type=jnp.float32
    ) * HEAD_DIM ** (-0.5)
    block_start = offset + WINDOW * jnp.arange(blocks, dtype=jnp.int32)
    query_pos = block_start[:, None] + jnp.arange(WINDOW, dtype=jnp.int32)[None, :]
    key_pos = block_start[:, None] - WINDOW + jnp.arange(3 * WINDOW, dtype=jnp.int32)[None, :]
    valid = (
        (jnp.abs(query_pos[:, :, None] - key_pos[:, None, :]) <= WINDOW)
        & (key_pos[:, None, :] >= 0)
        & (key_pos[:, None, :] < total_tokens)
    )
    scores = jnp.where(valid[:, None, None], scores, jnp.float32(-1e30))
    sink_grid = sink.reshape(kv_here, group)[None, :, :, None]
    top = jnp.maximum(jnp.max(scores, axis=-1), sink_grid)
    expo = jnp.exp(scores - top[..., None])
    denom = jnp.sum(expo, axis=-1) + jnp.exp(sink_grid - top)
    probs = (expo / denom[..., None]).astype(jnp.bfloat16)
    attended = jnp.einsum(
        "nkgqj,njkd->nqkgd", probs, key_blocks[..., HEAD_DIM:], preferred_element_type=jnp.float32
    )
    attended = attended.astype(jnp.bfloat16).reshape(tok, heads_here * HEAD_DIM)
    attn_rows, resid_rows = (
        lax.all_to_all(attended, "tp", split_axis=0, concat_axis=1, tiled=True),
        lax.all_to_all(resid, "tp", split_axis=0, concat_axis=1, tiled=True),
    )
    stream_part = (
        resid_rows.astype(jnp.float32)
        + jnp.dot(attn_rows, whole_out, preferred_element_type=jnp.float32)
    ).astype(jnp.bfloat16)
    stream = lax.all_gather(stream_part, "tp", axis=0, tiled=True)
    stream_cols = lax.dynamic_slice_in_dim(stream, lax.axis_index("tp") * cols, cols, 1)
    widened = stream.astype(jnp.float32)
    normed = (
        widened * lax.rsqrt(jnp.mean(widened * widened, axis=-1, keepdims=True) + 1e-06) * norm_gain
    ).astype(jnp.bfloat16)
    gate_up = jnp.dot(normed, whole_both, preferred_element_type=jnp.float32)
    gate, up = jnp.split(gate_up, 2, axis=1)
    hidden = (jax.nn.silu(gate) * up).astype(jnp.bfloat16)
    if direct:
        hidden, whole_down = lax.optimization_barrier((hidden, whole_down))
        whole_down = late(whole_down)
        far_terms = jnp.dot(
            hidden, whole_down[:, half_columns:], preferred_element_type=jnp.float32
        )
        far_sum = swap(sum_columns(far_terms, high // 2).astype(jnp.bfloat16), high)
        near_terms = jnp.dot(
            hidden, whole_down[:, :half_columns], preferred_element_type=jnp.float32
        )
        near_sum = sum_columns(near_terms, high // 2)
        return (
            stream_cols.astype(jnp.float32) + (near_sum + far_sum.astype(jnp.float32))
        ).astype(jnp.bfloat16)
    terms = jnp.dot(
        hidden,
        whole_down,
        preferred_element_type=jnp.float32,
    )
    summed = lax.psum_scatter(
        terms.astype(jnp.bfloat16), "tp", scatter_dimension=1, tiled=True
    ).astype(jnp.float32)
    return (stream_cols.astype(jnp.float32) + summed).astype(jnp.bfloat16)


LANE = 128
CHUNK = 128
BF = jnp.bfloat16
F32 = jnp.float32
WHOLE_VMEM = 67_043_328


def fits(mesh):
    return mesh.shape["sp"] == 4 and mesh.shape["tp"] == 4 and mesh.shape["grp"] == 2


def angle_tables(total):
    halo = WINDOW // GRID_W
    rows = np.arange(-halo, total // GRID_W + halo, dtype=np.float64)
    cols = np.arange(GRID_W, dtype=np.float64)
    entry = np.arange(LANE) % HEAD_DIM
    rate = 10000.0 ** (-(entry % 16) / 16.0)
    by_row = (entry // 32 == 0).astype(np.float64)
    sign = np.where(entry % 32 < 16, -1.0, 1.0)

    def table(places, used, wave, scale):
        return jnp.asarray(wave(places[:, None] * rate) * scale * used, jnp.float32)

    return (
        table(rows, by_row, np.cos, 1.0),
        table(rows, by_row, np.sin, sign),
        table(cols, 1 - by_row, np.cos, 1.0),
        table(cols, 1 - by_row, np.sin, sign),
    )


def fused_kernel(
    sink, row_cos, row_sin, col_cos, col_sin, gain,
    resid_in, q_in, kv_in, out_w_in, gate_in, up_in, down_in,
    out,
    q, resid, kv, cos, sin, kd, vd, out_w,
    wg, wu, wd, st, nrm, hid,
    own, c_out, c_in, x_out, x_in,
    ec_out, ec_in, e_own, ex_out, ex_in, ez_out, ez_in, e_fin,
    local_sem, h_s, h_r,
    zg_s, zg_r, yg_s, yg_r, zd_s, zd_r, yd_s, yd_r,
    c_s, c_r, x_s, x_r,
    ac_s, ac_r, ax_s, ax_r, af_s, af_r, az_s, az_r,
    ec_s, ec_r, ex_s, ex_r, ez_s, ez_r,
):
    tok, cols = q.shape
    blocks = tok // WINDOW
    depth, ff = gate_in.shape
    tiles = ff // LANE
    n_end = (tiles // 2) * LANE
    n_mid = ff - n_end
    half_d = depth // 2
    half_c = cols // 2
    subs = half_c // CHUNK
    nch = cols // CHUNK

    g, s, t = lax.axis_index("grp"), lax.axis_index("sp"), lax.axis_index("tp")
    x, c = lax.div(t, 2), lax.rem(t, 2)
    par = lax.rem(s, 2)
    mid = lax.rem(lax.div(s + 1, 2), 2)
    way = 1 - 2 * lax.div(s, 2)
    c_peer = {"tp": t + 1 - 2 * c}
    x_peer = {"tp": t + 2 - 4 * x}
    y_peer = {"grp": 1 - g}
    z_peer = {"sp": s + 1 - 2 * par}
    t_x = t + 2 - 4 * x
    t_c = t + 1 - 2 * c

    def order(i):
        return lax.rem(s + way * i + 4, 4)

    def when(flag, fn):
        pl.when(flag)(fn)

    def by_role(fn):
        when(mid == 1, lambda: fn(n_mid, n_end))
        when(mid == 0, lambda: fn(n_end, 0))

    def span(start, size, unit):
        return pl.ds(pl.multiple_of(start, unit), size)

    def remote(src, dst, send, recv, to):
        return pltpu.make_async_remote_copy(
            src_ref=src, dst_ref=dst, send_sem=send, recv_sem=recv,
            device_id=to, device_id_type=pl.DeviceIdType.MESH,
        )

    barrier = pltpu.get_barrier_semaphore()
    partners = [c_peer, x_peer, y_peer] + [{"sp": lax.rem(s + k, 4)} for k in (1, 2, 3)]
    for to in partners:
        pl.semaphore_signal(barrier, inc=1, device_id=to, device_id_type=pl.DeviceIdType.MESH)
    pl.semaphore_wait(barrier, len(partners))

    def halo_right():
        return remote(kv_in.at[pl.ds(tok - WINDOW, WINDOW)], kv.at[pl.ds(0, WINDOW)],
                      h_s.at[0], h_r.at[0], {"sp": lax.rem(s + 1, 4)})

    def halo_left():
        return remote(kv_in.at[pl.ds(0, WINDOW)], kv.at[pl.ds(tok + WINDOW, WINDOW)],
                      h_s.at[1], h_r.at[1], {"sp": lax.rem(s + 3, 4)})

    when(s < 3, lambda: halo_right().start())
    when(s > 0, lambda: halo_left().start())

    locals_ = [
        pltpu.make_async_copy(kv_in, kv.at[pl.ds(WINDOW, tok)], local_sem.at[0]),
        pltpu.make_async_copy(q_in, q, local_sem.at[1]),
        pltpu.make_async_copy(out_w_in, out_w, local_sem.at[2]),
        pltpu.make_async_copy(resid_in, resid, local_sem.at[3]),
    ]
    for copy in locals_:
        copy.start()

    def gu_send(kind, d):
        n, at = (n_mid, n_end) if d in (1, 2) else (n_end, 0)
        src, dst = ((gate_in, wg), (up_in, wu))[kind]
        return remote(
            src.at[span(half_d * g, half_d, half_d), pl.ds(at, n)],
            dst.at[span(depth * s + half_d * g, half_d, half_d), pl.ds(0, n)],
            zg_s.at[kind, d], zg_r.at[kind, s], {"sp": d},
        )

    def dn_send(k, d):
        n, at = (n_mid, n_end) if d in (1, 2) else (n_end, 0)
        return remote(
            down_in.at[pl.ds(at, n), span(half_c * g + CHUNK * k, CHUNK, CHUNK)],
            wd.at[pl.ds(0, n), span(cols * s + half_c * g + CHUNK * k, CHUNK, CHUNK)],
            zd_s.at[k, d], zd_r.at[k, s], {"sp": d},
        )

    pair = s + 1 - 2 * par

    def far_of(d):
        return (s != d) & (pair != d)

    def gu_far():
        for d in (1, 2, 0, 3):
            when(far_of(d), lambda d=d: [gu_send(kind, d).start() for kind in (0, 1)] and None)

    def gu_near():
        for d in range(4):
            when(pair == d, lambda d=d: [gu_send(kind, d).start() for kind in (0, 1)] and None)

    def dn_far():
        for d in (1, 2, 0, 3):
            when(far_of(d), lambda d=d: [dn_send(k, d).start() for k in range(subs)] and None)

    def dn_near():
        for d in range(4):
            when(pair == d, lambda d=d: [dn_send(k, d).start() for k in range(subs)] and None)

    gu_far()

    def early():
        gu_near()
        dn_far()

    when(mid == 1, early)

    def own_copies(n, at):
        return [
            pltpu.make_async_copy(gate_in.at[:, pl.ds(at, n)],
                                  wg.at[span(depth * s, depth, depth), pl.ds(0, n)], local_sem.at[4]),
            pltpu.make_async_copy(up_in.at[:, pl.ds(at, n)],
                                  wu.at[span(depth * s, depth, depth), pl.ds(0, n)], local_sem.at[5]),
            pltpu.make_async_copy(down_in.at[pl.ds(at, n), :],
                                  wd.at[pl.ds(0, n), span(cols * s, cols, cols)], local_sem.at[6]),
        ]

    by_role(lambda n, at: [copy.start() for copy in own_copies(n, at)] and None)

    def one_hot(pick):
        i = lax.broadcasted_iota(jnp.int32, (256, 256), 0)
        j = lax.broadcasted_iota(jnp.int32, (256, 256), 1)
        return jnp.where(i == pick(j), 1.0, 0.0).astype(BF)

    swap_m = one_hot(lambda j: j + 16 - 32 * lax.rem(lax.div(j, 16), 2))
    for i in range((tok + 2 * WINDOW) // GRID_W):
        r = lax.div(tok, GRID_W) * s + i
        here = pl.ds(GRID_W * i, GRID_W)
        cos[here, :] = row_cos[pl.ds(r, 1), :] + col_cos[...]
        sin[here, :] = row_sin[pl.ds(r, 1), :] + col_sin[...]

    def no_left():
        kv[pl.ds(0, WINDOW), :] = jnp.zeros((WINDOW, kv.shape[1]), BF)

    def no_right():
        kv[pl.ds(tok + WINDOW, WINDOW), :] = jnp.zeros((WINDOW, kv.shape[1]), BF)

    when(s == 0, no_left)
    when(s == 3, no_right)
    if n_mid > n_end:
        def no_pad():
            wd[pl.ds(n_end, n_mid - n_end), :] = jnp.zeros((n_mid - n_end, wd.shape[1]), BF)
            hid[:, pl.ds(n_end, n_mid - n_end)] = jnp.zeros((hid.shape[0], n_mid - n_end), BF)

        when(mid == 0, no_pad)

    locals_[0].wait()
    when(s > 0, lambda: halo_right().wait_recv())
    when(s < 3, lambda: halo_left().wait_recv())

    for i in range(tok // WINDOW + 2):
        here = pl.ds(WINDOW * i, WINDOW)
        raw = kv[here, :]
        lane = lax.broadcasted_iota(jnp.int32, (WINDOW, 256), 1)
        is_key = lax.rem(lane, 128) < HEAD_DIM
        turn_c = jnp.concatenate([cos[here, :]] * 2, axis=1)
        turn_s = jnp.concatenate([sin[here, :]] * 2, axis=1)
        other = jnp.dot(raw, swap_m, preferred_element_type=F32)
        value = raw.astype(F32)
        turned = jnp.where(is_key, value * turn_c + other * turn_s, value).astype(BF)
        for k in range(2):
            kd[k, here, :] = jnp.dot(
                turned, one_hot(lambda j: 128 * k + lax.rem(j, 64)), preferred_element_type=F32
            ).astype(BF)
            vd[k, here, :] = jnp.dot(
                turned, one_hot(lambda j: 128 * k + 64 + lax.rem(j, 64)), preferred_element_type=F32
            ).astype(BF)

    locals_[1].wait()
    locals_[2].wait()
    locals_[3].wait()

    def c_copy(b):
        return remote(c_out.at[b], c_in.at[b], c_s.at[b], c_r.at[b], c_peer)

    def x_copy(b):
        return remote(x_out.at[b], x_in.at[b], x_s.at[b], x_r.at[b], x_peer)

    def part(slot, b, owner):
        return st.at[span(tok * slot + WINDOW * b, WINDOW, WINDOW), span(cols * owner, cols, cols)]

    def ag_c(slot, b):
        ref = part(slot, b, t)
        return remote(ref, ref, ac_s.at[slot, b], ac_r.at[slot, b], c_peer)

    def ag_x(slot, b):
        ref = part(slot, b, t)
        return remote(ref, ref, ax_s.at[slot, b], ax_r.at[slot, b], x_peer)

    def ag_f(slot, b):
        ref = part(slot, b, t_x)
        return remote(ref, ref, af_s.at[slot, b], af_r.at[slot, b], c_peer)

    def ag_z(slot, b):
        ref = part(slot, b, t)
        return remote(ref, ref, az_s.at[b], az_r.at[b], z_peer)

    total = tok * 4

    def attend(b):
        rows = span(WINDOW * b, WINDOW, WINDOW)
        keys_at = span(WINDOW * b, 3 * WINDOW, WINDOW)
        place = span(WINDOW * b + WINDOW, WINDOW, WINDOW)
        turn_c = jnp.concatenate([cos[place, :]] * 2, axis=1)
        turn_s = jnp.concatenate([sin[place, :]] * 2, axis=1)
        head_of = lax.div(lax.broadcasted_iota(jnp.int32, (WINDOW, 256), 1), HEAD_DIM)
        i = lax.broadcasted_iota(jnp.int32, (WINDOW, 3 * WINDOW), 0)
        j = lax.broadcasted_iota(jnp.int32, (WINDOW, 3 * WINDOW), 1)
        first = tok * s + WINDOW * b - WINDOW
        valid = (j >= i) & (j <= i + 2 * WINDOW) & (j >= -first) & (j < total - first)
        bias = jnp.where(valid, 0.0, -1e30)
        outs = []
        for k in range(2):
            raw = q[rows, pl.ds(256 * k, 256)]
            other = jnp.dot(raw, swap_m, preferred_element_type=F32)
            turned = raw.astype(F32) * turn_c + other * turn_s
            stacked = jnp.concatenate(
                [jnp.where(head_of == h, turned, 0.0) for h in range(4)], axis=0
            ).astype(BF)
            scores = lax.dot_general(
                stacked, kd[k, keys_at, :], (((1,), (1,)), ((), ())), preferred_element_type=F32
            )
            probs = []
            for h in range(4):
                one = scores[WINDOW * h : WINDOW * (h + 1)] * HEAD_DIM ** (-0.5) + bias
                level = sink[4 * k + h]
                top = jnp.maximum(jnp.max(one, axis=1, keepdims=True), level)
                expo = jnp.exp(one - top)
                denom = jnp.sum(expo, axis=1, keepdims=True) + jnp.exp(level - top)
                probs.append((expo * (1.0 / denom)).astype(BF))
            mixed = jnp.dot(
                jnp.concatenate(probs, axis=0), vd[k, keys_at, :], preferred_element_type=F32
            )
            acc = jnp.zeros((WINDOW, 256), F32)
            for h in range(4):
                acc = jnp.where(head_of == h, mixed[WINDOW * h : WINDOW * (h + 1)], acc)
            outs.append(acc.astype(BF))
        att = jnp.concatenate(outs, axis=1)
        for xx in range(2):
            at = pl.ds(cols * xx, cols)
            c_out[b, :, at] = jnp.dot(
                att, out_w[:, span((2 * xx + 1 - c) * cols, cols, cols)], preferred_element_type=F32
            ).astype(BF)
            own[b, :, at] = jnp.dot(
                att, out_w[:, span((2 * xx + c) * cols, cols, cols)], preferred_element_type=F32
            )
        c_copy(b).start()

    def over_x(b):
        c_copy(b).wait_recv()
        mine, theirs = span(cols * x, cols, cols), span(cols * (1 - x), cols, cols)
        x_out[b] = (own[b, :, theirs] + c_in[b, :, theirs].astype(F32)).astype(BF)
        own[b, :, mine] = own[b, :, mine] + c_in[b, :, mine].astype(F32)
        x_copy(b).start()

    def to_stream(b):
        x_copy(b).wait_recv()
        rows = span(WINDOW * b, WINDOW, WINDOW)
        value = resid[rows, :].astype(F32) + (
            own[b, :, span(cols * x, cols, cols)] + x_in[b].astype(F32)
        )
        st[span(tok * par + WINDOW * b, WINDOW, WINDOW), span(cols * t, cols, cols)] = value.astype(BF)
        ag_z(par, b).start()
        ag_x(par, b).start()
        ag_c(par, b).start()


    def recv_x(slot, b):
        ref = part(slot, b, t_x)
        remote(ref, ref, ax_s.at[slot, b], ax_r.at[slot, b], x_peer).wait_recv()

    def recv_c(slot, b):
        ref = part(slot, b, t_c)
        remote(ref, ref, ac_s.at[slot, b], ac_r.at[slot, b], c_peer).wait_recv()

    def recv_f(slot, b):
        ref = part(slot, b, t_c + 2 - 4 * x)
        remote(ref, ref, af_s.at[slot, b], af_r.at[slot, b], c_peer).wait_recv()

    def recv_z(slot, b):
        ref = part(slot, b, t)
        remote(ref, ref, az_s.at[b], az_r.at[b], z_peer).wait_recv()

    def step(i, _):
        when(i < blocks, lambda: attend(i))
        when((i >= 1) & (i < blocks + 1), lambda: over_x(i - 1))
        when((i >= 2) & (i < blocks + 2), lambda: to_stream(i - 2))
        return 0

    lax.fori_loop(0, blocks + 2, step, 0)

    def late():
        gu_near()
        dn_far()

    when(mid == 0, late)
    dn_near()

    def own_pass(b, _):
        recv_x(par, b)
        ag_f(par, b).start()
        return 0

    lax.fori_loop(0, blocks, own_pass, 0)

    def gu_pass(kind, src):
        ref = (wg, wu)[kind]

        def go(n, at):
            piece = ref.at[span(depth * src + half_d * g, half_d, half_d), pl.ds(0, n)]
            remote(piece, piece, zg_s.at[kind, src], zg_r.at[kind, src], z_peer).wait_recv()
            remote(piece, piece, yg_s.at[kind, src], yg_r.at[kind, src], y_peer).start()

        by_role(go)

    def gu_got(kind, src):
        ref = (wg, wu)[kind]

        def go(n, at):
            piece = ref.at[span(depth * src + half_d * (1 - g), half_d, half_d), pl.ds(0, n)]
            remote(piece, piece, yg_s.at[kind, src], yg_r.at[kind, src], y_peer).wait_recv()

        by_role(go)

    def dn_pass(k, src):
        def go(n, at):
            piece = wd.at[pl.ds(0, n), span(cols * src + half_c * g + CHUNK * k, CHUNK, CHUNK)]
            remote(piece, piece, zd_s.at[k, src], zd_r.at[k, src], z_peer).wait_recv()
            remote(piece, piece, yd_s.at[k, src], yd_r.at[k, src], y_peer).start()

        by_role(go)

    def dn_got(k, src):
        def go(n, at):
            piece = wd.at[pl.ds(0, n), span(cols * src + half_c * (1 - g) + CHUNK * k, CHUNK, CHUNK)]
            remote(piece, piece, yd_s.at[k, src], yd_r.at[k, src], y_peer).wait_recv()

        by_role(go)

    def normalize(slot):
        rows_at_once = 32

        def rows_of(i, _):
            here = span(tok * slot + rows_at_once * i, rows_at_once, rows_at_once)
            wide = st[here, :].astype(F32)
            scale = lax.rsqrt(jnp.mean(wide * wide, axis=1, keepdims=True) + 1e-06)
            nrm[here, :] = (wide * scale * gain[...]).astype(BF)
            return 0

        lax.fori_loop(0, tok // rows_at_once, rows_of, 0)

    gu_pass(0, order(1))

    def own_in(b, _):
        recv_c(par, b)
        recv_f(par, b)
        return 0

    lax.fori_loop(0, blocks, own_in, 0)
    normalize(par)
    gu_pass(1, order(1))

    other_par = 1 - par

    def pair_pass(b, _):
        def first():
            recv_z(other_par, b)
            ag_x(other_par, b).start()
            ag_c(other_par, b).start()

        def second():
            recv_x(other_par, b - 2)
            ag_f(other_par, b - 2).start()

        when(b < blocks, first)
        when(b >= 2, second)
        return 0

    lax.fori_loop(0, blocks + 2, pair_pass, 0)
    gu_pass(0, order(2))
    gu_pass(1, order(2))

    def pair_in(b, _):
        recv_c(other_par, b)
        recv_f(other_par, b)
        return 0

    lax.fori_loop(0, blocks, pair_in, 0)
    normalize(other_par)
    gu_pass(0, order(3))
    gu_pass(1, order(3))
    by_role(lambda n, at: [copy.wait() for copy in own_copies(n, at)] and None)
    for kind in range(2):
        for i in (1, 2, 3):
            gu_got(kind, order(i))

    def gate_up(j, _):
        at = span(LANE * j, LANE, LANE)
        both = jnp.concatenate([wg[:, at], wu[:, at]], axis=1)
        value = jnp.dot(nrm[...], both, preferred_element_type=F32)
        gate, up = value[:, :LANE], value[:, LANE:]
        hid[:, at] = (gate / (1.0 + jnp.exp(-gate)) * up).astype(BF)
        return 0

    lax.fori_loop(0, n_end // LANE + mid * ((n_mid - n_end) // LANE), gate_up, 0)

    def chunk(i):
        b = lax.div(i, nch)
        ci = lax.rem(i, nch)
        first = lax.div(ci, subs)
        k = lax.rem(ci, subs)
        half = first * (1 - g) + (1 - first) * g
        source = order(b)
        return b, first, k, half * subs + k, source

    def ec(xo, ch):
        return remote(ec_out.at[xo, ch], ec_in.at[xo, ch], ec_s.at[xo, ch], ec_r.at[xo, ch], c_peer)

    def ex(ch):
        return remote(ex_out.at[ch], ex_in.at[ch], ex_s.at[ch], ex_r.at[ch], x_peer)

    def ez(ch):
        return remote(ez_out.at[ch], ez_in.at[ch], ez_s.at[ch], ez_r.at[ch], z_peer)

    def produce(i):
        b, first, k, ch, source = chunk(i)
        when((b > 0) & (first == 1), lambda: dn_got(k, source))
        xo, co = lax.div(source, 2), lax.rem(source, 2)
        term = jnp.dot(
            hid[...], wd[:, span(cols * source + CHUNK * ch, CHUNK, CHUNK)],
            preferred_element_type=F32,
        )

        def send():
            ec_out[xo, ch] = term.astype(BF)
            ec(xo, ch).start()

        def keep():
            e_own[xo, ch] = term

        when(co != c, send)
        when(co == c, keep)
        when((first == 0) & (k == subs - 1) & (b < 3),
             lambda: [dn_pass(kk, order(b + 1)) for kk in range(subs)] and None)

    def combine(i):
        _, _, _, ch, source = chunk(i)
        xo, co = lax.div(source, 2), lax.rem(source, 2)

        def mine():
            ec(xo, ch).wait_recv()
            value = e_own[xo, ch] + ec_in[xo, ch].astype(F32)

            def send():
                ex_out[ch] = value.astype(BF)
                ex(ch).start()

            def keep():
                e_own[xo, ch] = value

            when(xo != x, send)
            when(xo == x, keep)

        when(co == c, mine)

    def deliver(i):
        _, _, _, ch, source = chunk(i)

        def mine():
            ex(ch).wait_recv()
            theirs = span(tok * other_par, tok, tok)
            ours = span(tok * par, tok, tok)
            ez_out[ch] = (e_own[x, ch, theirs, :] + ex_in[ch, theirs, :].astype(F32)).astype(BF)
            ez(ch).start()
            e_fin[ch] = e_own[x, ch, ours, :] + ex_in[ch, ours, :].astype(F32)

        when(source == t, mine)

    steps = 4 * nch

    def tail(i, _):
        when(i < steps, lambda: produce(i))
        when((i >= 1) & (i < steps + 1), lambda: combine(i - 1))
        when(i >= 2, lambda: deliver(i - 2))
        return 0

    lax.fori_loop(0, steps + 2, tail, 0)

    def finish(ch, _):
        ez(ch).wait_recv()
        at = span(CHUNK * ch, CHUNK, CHUNK)
        base = st[span(tok * par, tok, tok), span(cols * t + CHUNK * ch, CHUNK, CHUNK)]
        out[:, at] = (base.astype(F32) + (e_fin[ch] + ez_in[ch].astype(F32))).astype(BF)
        return 0

    lax.fori_loop(0, nch, finish, 0)

    when(s < 3, lambda: halo_right().wait_send())
    when(s > 0, lambda: halo_left().wait_send())
    for d in range(4):
        def sent(d=d):
            for kind in range(2):
                gu_send(kind, d).wait_send()
            for k in range(subs):
                dn_send(k, d).wait_send()

        when(s != d, sent)

    def relayed(n, at):
        for i in (1, 2, 3):
            src = order(i)
            for kind, ref in enumerate((wg, wu)):
                piece = ref.at[span(depth * src + half_d * g, half_d, half_d), pl.ds(0, n)]
                remote(piece, piece, yg_s.at[kind, src], yg_r.at[kind, src], y_peer).wait_send()
            for k in range(subs):
                piece = wd.at[pl.ds(0, n), span(cols * src + half_c * g + CHUNK * k, CHUNK, CHUNK)]
                remote(piece, piece, yd_s.at[k, src], yd_r.at[k, src], y_peer).wait_send()

    by_role(relayed)

    def blocks_sent(b, _):
        c_copy(b).wait_send()
        x_copy(b).wait_send()
        ag_z(par, b).wait_send()
        for slot in range(2):
            ag_c(slot, b).wait_send()
            ag_x(slot, b).wait_send()
            ag_f(slot, b).wait_send()
        return 0

    lax.fori_loop(0, blocks, blocks_sent, 0)

    def chunks_sent(ch, _):
        for xo in range(2):
            ec(xo, ch).wait_send()
        ex(ch).wait_send()
        ez(ch).wait_send()
        return 0

    lax.fori_loop(0, nch, chunks_sent, 0)


def fused_body(
    resid, queries, keys_values, sink, out_weight, norm_gain, gate_weight, up_weight, down_weight
):
    tok, cols = queries.shape
    width = norm_gain.shape[0]
    ff = gate_weight.shape[1]
    n_mid = ff - (ff // LANE // 2) * LANE
    blocks = tok // WINDOW
    padded = tok + 2 * WINDOW
    nch = cols // CHUNK
    subs = nch // 2
    vmem = lambda shape, dtype=BF: pltpu.VMEM(shape, dtype)
    dma = lambda *shape: pltpu.SemaphoreType.DMA(shape)
    in_vmem = pl.BlockSpec(memory_space=pltpu.VMEM)
    in_hbm = pl.BlockSpec(memory_space=pl.ANY)
    scratch = [
        vmem((tok, cols)), vmem((tok, cols)), vmem((padded, 256)),
        vmem((padded, LANE), F32), vmem((padded, LANE), F32),
        vmem((2, padded, 256)), vmem((2, padded, 256)), vmem(out_weight.shape),
        vmem((width, n_mid)), vmem((width, n_mid)), vmem((n_mid, width)),
        vmem((2 * tok, width)), vmem((2 * tok, width)), vmem((2 * tok, n_mid)),
        vmem((blocks, WINDOW, 2 * cols), F32), vmem((blocks, WINDOW, 2 * cols)),
        vmem((blocks, WINDOW, 2 * cols)), vmem((blocks, WINDOW, cols)), vmem((blocks, WINDOW, cols)),
        vmem((2, nch, 2 * tok, CHUNK)), vmem((2, nch, 2 * tok, CHUNK)),
        vmem((2, nch, 2 * tok, CHUNK), F32),
        vmem((nch, 2 * tok, CHUNK)), vmem((nch, 2 * tok, CHUNK)),
        vmem((nch, tok, CHUNK)), vmem((nch, tok, CHUNK)), vmem((nch, tok, CHUNK), F32),
        dma(7), dma(2), dma(2),
        dma(2, 4), dma(2, 4), dma(2, 4), dma(2, 4),
        dma(subs, 4), dma(subs, 4), dma(subs, 4), dma(subs, 4),
        dma(blocks), dma(blocks), dma(blocks), dma(blocks),
        dma(2, blocks), dma(2, blocks), dma(2, blocks), dma(2, blocks),
        dma(2, blocks), dma(2, blocks), dma(blocks), dma(blocks),
        dma(2, nch), dma(2, nch), dma(nch), dma(nch), dma(nch), dma(nch),
    ]
    return pl.pallas_call(
        fused_kernel,
        out_shape=jax.ShapeDtypeStruct((tok, cols), BF),
        in_specs=[pl.BlockSpec(memory_space=pltpu.SMEM)] + [in_vmem] * 5 + [in_hbm] * 7,
        out_specs=in_vmem,
        scratch_shapes=scratch,
        compiler_params=pltpu.CompilerParams(
            collective_id=0, has_side_effects=True, vmem_limit_bytes=WHOLE_VMEM
        ),
    )(
        sink, *angle_tables(tok * 4), norm_gain.reshape(1, width),
        resid, queries, keys_values.reshape(tok, -1), out_weight, gate_weight, up_weight, down_weight,
    )


def solution(mesh):
    return jax.shard_map(
        fused_body if fits(mesh) else body,
        mesh=mesh,
        in_specs=(
            P(("grp", "sp"), "tp"),
            P(("grp", "sp"), "tp"),
            P(("grp", "sp"), "tp", None),
            P("tp"),
            P("tp", None),
            P(),
            P("sp", "tp"),
            P("sp", "tp"),
            P("tp", "sp"),
        ),
        out_specs=P(("grp", "sp"), "tp"),
        check_vma=False,
    )
```

```python
import jax
import jax.numpy as jnp
from jax import lax
from jax.experimental import pallas as pl
from jax.experimental.pallas import tpu as pltpu
from jax.sharding import PartitionSpec as P
import numpy as np

HEAD_DIM = 64
WINDOW = 128
GRID_W = 64


def with_halo(cells, sides, width):
    for axis, dim in sides:
        count = lax.axis_size(axis)
        ends = count - 1
        head = lax.slice_in_dim(cells, 0, width, axis=dim)
        tail = lax.slice_in_dim(cells, cells.shape[dim] - width, cells.shape[dim], axis=dim)
        cells = jnp.concatenate(
            [
                lax.ppermute(tail, axis, [(i, (i + 1) % count) for i in range(ends)]),
                cells,
                lax.ppermute(head, axis, [((i + 1) % count, i) for i in range(ends)]),
            ],
            axis=dim,
        )
    return cells


def rotate(values, positions):
    quarter = 16
    inverse = 10000.0 ** (-jnp.arange(quarter, dtype=jnp.float32) / quarter)

    def turn(part, place):
        angle = place.astype(jnp.float32)[:, None] * inverse[None, :]
        cosine = jnp.cos(angle)[:, None, :]
        sine = jnp.sin(angle)[:, None, :]
        first, second = (part[..., :quarter], part[..., quarter:])
        return jnp.concatenate(
            [first * cosine - second * sine, second * cosine + first * sine], axis=-1
        )

    grid_row = positions // GRID_W
    grid_col = positions % GRID_W
    return jnp.concatenate(
        [turn(values[..., :32], grid_row), turn(values[..., 32:], grid_col)], axis=-1
    )


def share(weight, axis):
    parts = lax.axis_size("grp")
    size = weight.shape[axis] // parts
    part = lax.dynamic_slice_in_dim(weight, lax.axis_index("grp") * size, size, axis)
    return lax.all_gather(part, ("sp", "grp"), axis=axis, tiled=True)


def relay(blocks, axes, first_column):
    count, parts = lax.axis_size("sp"), lax.axis_size("grp")
    here, group = lax.axis_index("sp"), lax.axis_index("grp")

    def place(whole, value, axis, block, source, part):
        rows = block.shape[0]
        start = part * (rows // parts)
        at = (source * rows + start, 0)
        if axis == 1:
            columns = block.shape[1] * count
            at = (start, lax.rem(source * block.shape[1] + columns - first_column, columns))
        if axis == 1 and part is not group:
            value = jnp.where(here < count, value, jnp.zeros_like(value))
        return lax.dynamic_update_slice(whole, value, at)

    wholes, right, left, late = [], [], [], []
    for block, axis in zip(blocks, axes):
        shape = list(block.shape)
        shape[axis] *= count
        wholes.append(place(jnp.zeros(shape, block.dtype), block, axis, block, here, 0))
        rows = block.shape[0] // parts
        part = lax.dynamic_slice_in_dim(block, group * rows, rows, 0)
        right.append([part])
        left.append([part])
    for step in range(1, count):
        source = jnp.where(here >= step, here - step, step)
        for index, (block, axis) in enumerate(zip(blocks, axes)):
            right[index].append(
                lax.ppermute(
                    right[index][-1], "sp", [(i, i + 1) for i in range(step - 1, count - 1)]
                )
            )
            left[index].append(
                lax.ppermute(left[index][-1], "sp", [(i + 1, i) for i in range(count - step)])
            )
            came = [left[index][step - i] for i in range(step)] + [right[index][step]]
            value = lax.select_n(jnp.minimum(here, step), *came)
            whole = place(wholes[index], value, axis, block, source, group)
            for shift in range(1, parts):
                other = lax.ppermute(value, "grp", [(i, (i + shift) % parts) for i in range(parts)])
                part = (group - shift) % parts
                if step == count - 1 and index == len(blocks) - 1:
                    late.append((other, axis, block, source, part))
                    continue
                whole = place(whole, other, axis, block, source, part)
            wholes[index] = whole

    def finish(whole):
        for piece in late:
            whole = place(whole, *piece)
        return whole

    return wholes, finish


def swap(value, bit):
    return lax.ppermute(value, "tp", [(i, i ^ bit) for i in range(lax.axis_size("tp"))])


def sum_columns(terms, bit):
    here = lax.axis_index("tp")
    while bit:
        half = terms.shape[1] // 2
        mine = jnp.where((here & bit) > 0, half, 0)
        theirs = lax.dynamic_slice_in_dim(terms, half - mine, half, 1).astype(jnp.bfloat16)
        own = lax.dynamic_slice_in_dim(terms, mine, half, 1)
        terms = own + swap(theirs, bit).astype(jnp.float32)
        bit //= 2
    return terms


def body(
    resid, queries, keys_values, sink, out_weight, norm_gain, gate_weight, up_weight, down_weight
):
    tok = queries.shape[0]
    heads_here = queries.shape[1] // HEAD_DIM
    kv_here = keys_values.shape[1]
    group = heads_here // kv_here
    cols = resid.shape[1]
    offset = lax.axis_index("sp") * tok
    total_tokens = tok * lax.axis_size("sp")
    positions = offset + jnp.arange(tok, dtype=jnp.int32)
    rotated_q = rotate(
        queries.astype(jnp.float32).reshape(tok, heads_here, HEAD_DIM), positions
    ).astype(jnp.bfloat16)
    padded = with_halo(keys_values, (("sp", 0),), WINDOW)
    ranks, members = lax.axis_size("sp"), lax.axis_size("tp")
    high = members // 2
    direct = ranks <= 8 and ranks % 2 == 0 and members >= 2 and members & (members - 1) == 0
    if direct:
        half_columns = resid.shape[1] * members // 2
        near = jnp.where((lax.axis_index("tp") & high) > 0, half_columns, 0)
        padded, gate_weight, up_weight, down_weight = lax.optimization_barrier(
            (padded, gate_weight, up_weight, down_weight)
        )
        both = jnp.concatenate([gate_weight, up_weight], axis=1)
        (whole_both, whole_down), late = relay((both, down_weight), (0, 1), near)
    else:
        whole_both = jnp.concatenate([share(gate_weight, 0), share(up_weight, 0)], axis=1)
        whole_down = share(down_weight, 1)
    whole_out = lax.all_gather(out_weight, "tp", axis=0, tiled=True)
    key_positions = offset - WINDOW + jnp.arange(tok + 2 * WINDOW, dtype=jnp.int32)
    rotated_k = rotate(padded[..., :HEAD_DIM].astype(jnp.float32), key_positions).astype(
        jnp.bfloat16
    )
    padded = jnp.concatenate([rotated_k, padded[..., HEAD_DIM:]], axis=-1)
    blocks = tok // WINDOW
    key_blocks = jnp.stack(
        [padded[index * WINDOW : index * WINDOW + 3 * WINDOW] for index in range(blocks)]
    )
    grouped = rotated_q.reshape(blocks, WINDOW, kv_here, group, HEAD_DIM)
    scores = jnp.einsum(
        "nqkgd,njkd->nkgqj", grouped, key_blocks[..., :HEAD_DIM], preferred_element_type=jnp.float32
    ) * HEAD_DIM ** (-0.5)
    block_start = offset + WINDOW * jnp.arange(blocks, dtype=jnp.int32)
    query_pos = block_start[:, None] + jnp.arange(WINDOW, dtype=jnp.int32)[None, :]
    key_pos = block_start[:, None] - WINDOW + jnp.arange(3 * WINDOW, dtype=jnp.int32)[None, :]
    valid = (
        (jnp.abs(query_pos[:, :, None] - key_pos[:, None, :]) <= WINDOW)
        & (key_pos[:, None, :] >= 0)
        & (key_pos[:, None, :] < total_tokens)
    )
    scores = jnp.where(valid[:, None, None], scores, jnp.float32(-1e30))
    sink_grid = sink.reshape(kv_here, group)[None, :, :, None]
    top = jnp.maximum(jnp.max(scores, axis=-1), sink_grid)
    expo = jnp.exp(scores - top[..., None])
    denom = jnp.sum(expo, axis=-1) + jnp.exp(sink_grid - top)
    probs = (expo / denom[..., None]).astype(jnp.bfloat16)
    attended = jnp.einsum(
        "nkgqj,njkd->nqkgd", probs, key_blocks[..., HEAD_DIM:], preferred_element_type=jnp.float32
    )
    attended = attended.astype(jnp.bfloat16).reshape(tok, heads_here * HEAD_DIM)
    attn_rows, resid_rows = (
        lax.all_to_all(attended, "tp", split_axis=0, concat_axis=1, tiled=True),
        lax.all_to_all(resid, "tp", split_axis=0, concat_axis=1, tiled=True),
    )
    stream_part = (
        resid_rows.astype(jnp.float32)
        + jnp.dot(attn_rows, whole_out, preferred_element_type=jnp.float32)
    ).astype(jnp.bfloat16)
    stream = lax.all_gather(stream_part, "tp", axis=0, tiled=True)
    stream_cols = lax.dynamic_slice_in_dim(stream, lax.axis_index("tp") * cols, cols, 1)
    widened = stream.astype(jnp.float32)
    normed = (
        widened * lax.rsqrt(jnp.mean(widened * widened, axis=-1, keepdims=True) + 1e-06) * norm_gain
    ).astype(jnp.bfloat16)
    gate_up = jnp.dot(normed, whole_both, preferred_element_type=jnp.float32)
    gate, up = jnp.split(gate_up, 2, axis=1)
    hidden = (jax.nn.silu(gate) * up).astype(jnp.bfloat16)
    if direct:
        hidden, whole_down = lax.optimization_barrier((hidden, whole_down))
        whole_down = late(whole_down)
        far_terms = jnp.dot(
            hidden, whole_down[:, half_columns:], preferred_element_type=jnp.float32
        )
        far_sum = swap(sum_columns(far_terms, high // 2).astype(jnp.bfloat16), high)
        near_terms = jnp.dot(
            hidden, whole_down[:, :half_columns], preferred_element_type=jnp.float32
        )
        near_sum = sum_columns(near_terms, high // 2)
        return (
            stream_cols.astype(jnp.float32) + (near_sum + far_sum.astype(jnp.float32))
        ).astype(jnp.bfloat16)
    terms = jnp.dot(
        hidden,
        whole_down,
        preferred_element_type=jnp.float32,
    )
    summed = lax.psum_scatter(
        terms.astype(jnp.bfloat16), "tp", scatter_dimension=1, tiled=True
    ).astype(jnp.float32)
    return (stream_cols.astype(jnp.float32) + summed).astype(jnp.bfloat16)


LANE = 128
CHUNK = 128
BF = jnp.bfloat16
F32 = jnp.float32
WHOLE_VMEM = 67_043_328


def fits(mesh):
    return mesh.shape["sp"] == 4 and mesh.shape["tp"] == 4 and mesh.shape["grp"] == 2


def angle_tables(total):
    halo = WINDOW // GRID_W
    rows = np.arange(-halo, total // GRID_W + halo, dtype=np.float64)
    cols = np.arange(GRID_W, dtype=np.float64)
    entry = np.arange(LANE) % HEAD_DIM
    rate = 10000.0 ** (-(entry % 16) / 16.0)
    by_row = (entry // 32 == 0).astype(np.float64)
    sign = np.where(entry % 32 < 16, -1.0, 1.0)

    def table(places, used, wave, scale):
        return jnp.asarray(wave(places[:, None] * rate) * scale * used, jnp.float32)

    return (
        table(rows, by_row, np.cos, 1.0),
        table(rows, by_row, np.sin, sign),
        table(cols, 1 - by_row, np.cos, 1.0),
        table(cols, 1 - by_row, np.sin, sign),
    )


def fused_kernel(
    sink, row_cos, row_sin, col_cos, col_sin, gain,
    resid_in, q_in, kv_in, out_w_in, gate_in, up_in, down_in,
    out,
    q, resid, kv, cos, sin, kd, vd, out_w,
    wg, wu, wd, st, nrm, hid, ga, upa,
    own, c_out, c_in, x_out, x_in,
    ec_out, ec_in, e_own, ex_out, ex_in, ez_out, ez_in, e_fin,
    local_sem, h_s, h_r,
    zg_s, zg_r, yg_s, yg_r, zd_s, zd_r, yd_s, yd_r, hg_s, hd_s,
    c_s, c_r, x_s, x_r,
    ac_s, ac_r, ax_s, ax_r, af_s, af_r, az_s, az_r,
    ec_s, ec_r, ex_s, ex_r, ez_s, ez_r,
):
    tok, cols = q.shape
    blocks = tok // WINDOW
    depth, ff = gate_in.shape
    tiles = ff // LANE
    n_end = (tiles // 2) * LANE
    n_mid = ff - n_end
    half_d = depth // 2
    half_c = cols // 2
    subs = half_c // CHUNK
    nch = cols // CHUNK

    g, s, t = lax.axis_index("grp"), lax.axis_index("sp"), lax.axis_index("tp")
    x, c = lax.div(t, 2), lax.rem(t, 2)
    par = lax.rem(s, 2)
    mid = lax.rem(lax.div(s + 1, 2), 2)
    way = 1 - 2 * lax.div(s, 2)
    c_peer = {"tp": t + 1 - 2 * c}
    x_peer = {"tp": t + 2 - 4 * x}
    y_peer = {"grp": 1 - g}
    z_peer = {"sp": s + 1 - 2 * par}
    t_x = t + 2 - 4 * x
    t_c = t + 1 - 2 * c

    def ring(i):
        return lax.rem(s + way * i + 4, 4)

    near = ring(1 + 2 * mid)
    far = ring(3 - mid)
    adj = ring(2 - mid)

    def pick(i, values):
        found = values[0]
        for at in range(1, len(values)):
            found = jnp.where(i == at, values[at], found)
        return found

    def when(flag, fn):
        pl.when(flag)(fn)

    def by_role(fn):
        when(mid == 1, lambda: fn(n_mid, n_end))
        when(mid == 0, lambda: fn(n_end, 0))

    def span(start, size, unit):
        return pl.ds(pl.multiple_of(start, unit), size)

    def remote(src, dst, send, recv, to):
        return pltpu.make_async_remote_copy(
            src_ref=src, dst_ref=dst, send_sem=send, recv_sem=recv,
            device_id=to, device_id_type=pl.DeviceIdType.MESH,
        )

    barrier = pltpu.get_barrier_semaphore()
    partners = [c_peer, x_peer, y_peer] + [{"sp": lax.rem(s + k, 4)} for k in (1, 2, 3)]
    for to in partners:
        pl.semaphore_signal(barrier, inc=1, device_id=to, device_id_type=pl.DeviceIdType.MESH)
    pl.semaphore_wait(barrier, len(partners))

    def halo_right():
        return remote(kv_in.at[pl.ds(tok - WINDOW, WINDOW)], kv.at[pl.ds(0, WINDOW)],
                      h_s.at[0], h_r.at[0], {"sp": lax.rem(s + 1, 4)})

    def halo_left():
        return remote(kv_in.at[pl.ds(0, WINDOW)], kv.at[pl.ds(tok + WINDOW, WINDOW)],
                      h_s.at[1], h_r.at[1], {"sp": lax.rem(s + 3, 4)})

    when(s < 3, lambda: halo_right().start())
    when(s > 0, lambda: halo_left().start())

    locals_ = [
        pltpu.make_async_copy(kv_in, kv.at[pl.ds(WINDOW, tok)], local_sem.at[0]),
        pltpu.make_async_copy(q_in, q, local_sem.at[1]),
        pltpu.make_async_copy(out_w_in, out_w, local_sem.at[2]),
        pltpu.make_async_copy(resid_in, resid, local_sem.at[3]),
    ]
    for copy in locals_:
        copy.start()

    pieces = (
        (gate_in, wg, 0, half_d),
        (up_in, wu, 0, half_d // 2),
        (up_in, wu, half_d // 2, half_d // 2),
    )

    def gu_send(kind, d):
        n, at = (n_mid, n_end) if d in (1, 2) else (n_end, 0)
        src, dst, skip, rows = pieces[kind]
        return remote(
            src.at[span(half_d * g + skip, rows, rows), pl.ds(at, n)],
            dst.at[span(depth * s + half_d * g + skip, rows, rows), pl.ds(0, n)],
            zg_s.at[kind, d], zg_r.at[kind, s], {"sp": d},
        )

    def gu_piece(kind, src, which, n):
        _, ref, skip, rows = pieces[kind]
        return ref.at[span(depth * src + half_d * which + skip, rows, rows), pl.ds(0, n)]

    def dn_send(k, d):
        n, at = (n_mid, n_end) if d in (1, 2) else (n_end, 0)
        return remote(
            down_in.at[pl.ds(at, n), span(half_c * g + CHUNK * k, CHUNK, CHUNK)],
            wd.at[pl.ds(0, n), span(cols * s + half_c * g + CHUNK * k, CHUNK, CHUNK)],
            zd_s.at[k, d], zd_r.at[k, s], {"sp": d},
        )

    pair = s + 1 - 2 * par

    def to(d, send):
        for static in range(4):
            when(d == static, lambda static=static: send(static))

    def gu_to(d, kinds):
        to(d, lambda at: [gu_send(kind, at).start() for kind in kinds] and None)

    def dn_to(d):
        to(d, lambda at: [dn_send(k, at).start() for k in range(subs)] and None)

    gate_kind, up_kinds = (0,), (1, 2)

    def first_sends(inner):
        gu_to(pair, gate_kind)
        if inner:
            gu_to(adj, gate_kind)
            gu_to(far, gate_kind)
            gu_to(pair, up_kinds)
            gu_to(adj, up_kinds)
        else:
            gu_to(far, gate_kind)
            gu_to(pair, up_kinds)

    when(mid == 1, lambda: first_sends(True))
    when(mid == 0, lambda: first_sends(False))

    def own_copies(n, at):
        return [
            pltpu.make_async_copy(gate_in.at[:, pl.ds(at, n)],
                                  wg.at[span(depth * s, depth, depth), pl.ds(0, n)], local_sem.at[4]),
            pltpu.make_async_copy(up_in.at[:, pl.ds(at, n)],
                                  wu.at[span(depth * s, depth, depth), pl.ds(0, n)], local_sem.at[5]),
            pltpu.make_async_copy(down_in.at[pl.ds(at, n), :],
                                  wd.at[pl.ds(0, n), span(cols * s, cols, cols)], local_sem.at[6]),
        ]

    by_role(lambda n, at: [copy.start() for copy in own_copies(n, at)] and None)

    def one_hot(pick):
        i = lax.broadcasted_iota(jnp.int32, (256, 256), 0)
        j = lax.broadcasted_iota(jnp.int32, (256, 256), 1)
        return jnp.where(i == pick(j), 1.0, 0.0).astype(BF)

    swap_m = one_hot(lambda j: j + 16 - 32 * lax.rem(lax.div(j, 16), 2))
    for i in range((tok + 2 * WINDOW) // GRID_W):
        r = lax.div(tok, GRID_W) * s + i
        here = pl.ds(GRID_W * i, GRID_W)
        cos[here, :] = row_cos[pl.ds(r, 1), :] + col_cos[...]
        sin[here, :] = row_sin[pl.ds(r, 1), :] + col_sin[...]

    def no_left():
        kv[pl.ds(0, WINDOW), :] = jnp.zeros((WINDOW, kv.shape[1]), BF)

    def no_right():
        kv[pl.ds(tok + WINDOW, WINDOW), :] = jnp.zeros((WINDOW, kv.shape[1]), BF)

    when(s == 0, no_left)
    when(s == 3, no_right)
    if n_mid > n_end:
        def no_pad():
            wd[pl.ds(n_end, n_mid - n_end), :] = jnp.zeros((n_mid - n_end, wd.shape[1]), BF)
            wg[:, pl.ds(n_end, n_mid - n_end)] = jnp.zeros((wg.shape[0], n_mid - n_end), BF)
            wu[:, pl.ds(n_end, n_mid - n_end)] = jnp.zeros((wu.shape[0], n_mid - n_end), BF)

        when(mid == 0, no_pad)

    locals_[0].wait()
    when(s > 0, lambda: halo_right().wait_recv())
    when(s < 3, lambda: halo_left().wait_recv())

    for i in range(tok // WINDOW + 2):
        here = pl.ds(WINDOW * i, WINDOW)
        raw = kv[here, :]
        lane = lax.broadcasted_iota(jnp.int32, (WINDOW, 256), 1)
        is_key = lax.rem(lane, 128) < HEAD_DIM
        turn_c = jnp.concatenate([cos[here, :]] * 2, axis=1)
        turn_s = jnp.concatenate([sin[here, :]] * 2, axis=1)
        other = jnp.dot(raw, swap_m, preferred_element_type=F32)
        value = raw.astype(F32)
        turned = jnp.where(is_key, value * turn_c + other * turn_s, value).astype(BF)
        for k in range(2):
            kd[k, here, :] = jnp.dot(
                turned, one_hot(lambda j: 128 * k + lax.rem(j, 64)), preferred_element_type=F32
            ).astype(BF)
            vd[k, here, :] = jnp.dot(
                turned, one_hot(lambda j: 128 * k + 64 + lax.rem(j, 64)), preferred_element_type=F32
            ).astype(BF)

    locals_[1].wait()
    locals_[2].wait()
    locals_[3].wait()

    def c_copy(b):
        return remote(c_out.at[b], c_in.at[b], c_s.at[b], c_r.at[b], c_peer)

    def x_copy(b):
        return remote(x_out.at[b], x_in.at[b], x_s.at[b], x_r.at[b], x_peer)

    def part(slot, b, owner):
        return st.at[span(tok * slot + WINDOW * b, WINDOW, WINDOW), span(cols * owner, cols, cols)]

    def ag_c(slot, b):
        ref = part(slot, b, t)
        return remote(ref, ref, ac_s.at[slot, b], ac_r.at[slot, b], c_peer)

    def ag_x(slot, b):
        ref = part(slot, b, t)
        return remote(ref, ref, ax_s.at[slot, b], ax_r.at[slot, b], x_peer)

    def ag_f(slot, b):
        ref = part(slot, b, t_x)
        return remote(ref, ref, af_s.at[slot, b], af_r.at[slot, b], c_peer)

    def ag_z(slot, b):
        ref = part(slot, b, t)
        return remote(ref, ref, az_s.at[b], az_r.at[b], z_peer)

    total = tok * 4

    def attend(b):
        rows = span(WINDOW * b, WINDOW, WINDOW)
        keys_at = span(WINDOW * b, 3 * WINDOW, WINDOW)
        place = span(WINDOW * b + WINDOW, WINDOW, WINDOW)
        turn_c = jnp.concatenate([cos[place, :]] * 2, axis=1)
        turn_s = jnp.concatenate([sin[place, :]] * 2, axis=1)
        head_of = lax.div(lax.broadcasted_iota(jnp.int32, (WINDOW, 256), 1), HEAD_DIM)
        i = lax.broadcasted_iota(jnp.int32, (WINDOW, 3 * WINDOW), 0)
        j = lax.broadcasted_iota(jnp.int32, (WINDOW, 3 * WINDOW), 1)
        first = tok * s + WINDOW * b - WINDOW
        valid = (j >= i) & (j <= i + 2 * WINDOW) & (j >= -first) & (j < total - first)
        bias = jnp.where(valid, 0.0, -1e30)
        outs = []
        for k in range(2):
            raw = q[rows, pl.ds(256 * k, 256)]
            other = jnp.dot(raw, swap_m, preferred_element_type=F32)
            turned = raw.astype(F32) * turn_c + other * turn_s
            stacked = jnp.concatenate(
                [jnp.where(head_of == h, turned, 0.0) for h in range(4)], axis=0
            ).astype(BF)
            scores = lax.dot_general(
                stacked, kd[k, keys_at, :], (((1,), (1,)), ((), ())), preferred_element_type=F32
            )
            probs = []
            for h in range(4):
                one = scores[WINDOW * h : WINDOW * (h + 1)] * HEAD_DIM ** (-0.5) + bias
                level = sink[4 * k + h]
                top = jnp.maximum(jnp.max(one, axis=1, keepdims=True), level)
                expo = jnp.exp(one - top)
                denom = jnp.sum(expo, axis=1, keepdims=True) + jnp.exp(level - top)
                probs.append((expo * (1.0 / denom)).astype(BF))
            mixed = jnp.dot(
                jnp.concatenate(probs, axis=0), vd[k, keys_at, :], preferred_element_type=F32
            )
            acc = jnp.zeros((WINDOW, 256), F32)
            for h in range(4):
                acc = jnp.where(head_of == h, mixed[WINDOW * h : WINDOW * (h + 1)], acc)
            outs.append(acc.astype(BF))
        att = jnp.concatenate(outs, axis=1)
        for xx in range(2):
            at = pl.ds(cols * xx, cols)
            c_out[b, :, at] = jnp.dot(
                att, out_w[:, span((2 * xx + 1 - c) * cols, cols, cols)], preferred_element_type=F32
            ).astype(BF)
            own[b, :, at] = jnp.dot(
                att, out_w[:, span((2 * xx + c) * cols, cols, cols)], preferred_element_type=F32
            )
        c_copy(b).start()

    def over_x(b):
        c_copy(b).wait_recv()
        mine, theirs = span(cols * x, cols, cols), span(cols * (1 - x), cols, cols)
        x_out[b] = (own[b, :, theirs] + c_in[b, :, theirs].astype(F32)).astype(BF)
        own[b, :, mine] = own[b, :, mine] + c_in[b, :, mine].astype(F32)
        x_copy(b).start()

    def to_stream(b):
        x_copy(b).wait_recv()
        rows = span(WINDOW * b, WINDOW, WINDOW)
        value = resid[rows, :].astype(F32) + (
            own[b, :, span(cols * x, cols, cols)] + x_in[b].astype(F32)
        )
        st[span(tok * par + WINDOW * b, WINDOW, WINDOW), span(cols * t, cols, cols)] = value.astype(BF)
        ag_z(par, b).start()
        ag_x(par, b).start()
        ag_c(par, b).start()


    def recv_x(slot, b):
        ref = part(slot, b, t_x)
        remote(ref, ref, ax_s.at[slot, b], ax_r.at[slot, b], x_peer).wait_recv()

    def recv_c(slot, b):
        ref = part(slot, b, t_c)
        remote(ref, ref, ac_s.at[slot, b], ac_r.at[slot, b], c_peer).wait_recv()

    def recv_f(slot, b):
        ref = part(slot, b, t_c + 2 - 4 * x)
        remote(ref, ref, af_s.at[slot, b], af_r.at[slot, b], c_peer).wait_recv()

    def recv_z(slot, b):
        ref = part(slot, b, t)
        remote(ref, ref, az_s.at[b], az_r.at[b], z_peer).wait_recv()

    def gu_pass(kind, src, n):
        piece = gu_piece(kind, src, g, n)
        remote(piece, piece, zg_s.at[kind, src], zg_r.at[kind, src], z_peer).wait_recv()
        remote(piece, piece, yg_s.at[kind, src], yg_r.at[kind, src], y_peer).start()
        if src is near and n == n_mid:
            gu_hop(kind).start()

    def gu_hop(kind):
        piece = gu_piece(kind, near, g, n_mid)
        return remote(piece, piece, hg_s.at[kind], zg_r.at[kind, near], {"sp": adj})

    def dn_hop(k):
        piece = wd.at[pl.ds(0, n_mid), span(cols * near + half_c * g + CHUNK * k, CHUNK, CHUNK)]
        return remote(piece, piece, hd_s.at[k], zd_r.at[k, near], {"sp": adj})

    def gu_got(kind, src):
        def go(n, at):
            piece = gu_piece(kind, src, 1 - g, n)
            remote(piece, piece, yg_s.at[kind, src], yg_r.at[kind, src], y_peer).wait_recv()

        by_role(go)

    def dn_pass(k, src):
        def go(n, at):
            piece = wd.at[pl.ds(0, n), span(cols * src + half_c * g + CHUNK * k, CHUNK, CHUNK)]
            remote(piece, piece, zd_s.at[k, src], zd_r.at[k, src], z_peer).wait_recv()
            remote(piece, piece, yd_s.at[k, src], yd_r.at[k, src], y_peer).start()
            if src is near and n == n_mid:
                dn_hop(k).start()

        by_role(go)

    def dn_got(k, src):
        def go(n, at):
            piece = wd.at[pl.ds(0, n), span(cols * src + half_c * (1 - g) + CHUNK * k, CHUNK, CHUNK)]
            remote(piece, piece, yd_s.at[k, src], yd_r.at[k, src], y_peer).wait_recv()

        by_role(go)

    def normalize(slot, b):
        rows_at_once = 32

        def rows_of(i, _):
            here = span(tok * slot + WINDOW * b + rows_at_once * i, rows_at_once, rows_at_once)
            wide = st[here, :].astype(F32)
            scale = lax.rsqrt(jnp.mean(wide * wide, axis=1, keepdims=True) + 1e-06)
            nrm[here, :] = (wide * scale * gain[...]).astype(BF)
            return 0

        lax.fori_loop(0, WINDOW // rows_at_once, rows_of, 0)

    last, third = ring(2), ring(3 - 2 * mid)
    relay_mid = ((gate_kind, near), (gate_kind, adj), (up_kinds, near),
                 (up_kinds, adj), (gate_kind, far), (up_kinds, far))
    relay_end = ((gate_kind, near), (gate_kind, far), (up_kinds, near),
                 (gate_kind, adj), (up_kinds, far), (up_kinds, adj))

    def relay(r):
        def go(table, n):
            kinds, src = table[r]
            for kind in kinds:
                gu_pass(kind, src, n)

        def inner():
            go(relay_mid, n_mid)
            if r == 2:
                gu_to(far, up_kinds)

        when(mid == 1, inner)
        when(mid == 0, lambda: go(relay_end, n_end))

    def own_pass(b):
        recv_x(par, b)
        ag_f(par, b).start()

    def step(i, _):
        for r in range(3):
            when(i == 3 + r, lambda r=r: relay(r))
        when(i < blocks, lambda: attend(i))
        when((i >= 1) & (i < blocks + 1), lambda: over_x(i - 1))
        when((i >= 2) & (i < blocks + 2), lambda: to_stream(i - 2))
        when(i >= 3, lambda: own_pass(i - 3))
        return 0

    lax.fori_loop(0, blocks + 3, step, 0)

    def late():
        gu_to(far, up_kinds)
        dn_to(pair)

    when(mid == 0, late)
    when(mid == 1, lambda: dn_to(pair))
    relay(3)

    other_par = 1 - par

    def pair_pass(b, _):
        def first():
            recv_z(other_par, b)
            ag_x(other_par, b).start()
            ag_c(other_par, b).start()

        def second():
            recv_x(other_par, b - 2)
            ag_f(other_par, b - 2).start()

        def third():
            recv_c(par, b)
            recv_f(par, b)
            normalize(par, b)

        when(b < blocks, first)
        when(b < blocks, third)
        when(b >= 2, second)
        when(b == 3 - mid, lambda: relay(4))
        return 0

    lax.fori_loop(0, blocks + 2, pair_pass, 0)

    def pair_in(b, _):
        recv_c(other_par, b)
        recv_f(other_par, b)
        normalize(other_par, b)
        return 0

    def inner_down():
        for k in range(subs):
            dn_pass(k, near)
        dn_to(far)
        dn_to(adj)

    when(mid == 1, lambda: relay(5))
    when(mid == 1, inner_down)
    lax.fori_loop(0, blocks, pair_in, 0)
    by_role(lambda n, at: [copy.wait() for copy in own_copies(n, at)] and None)
    for src in (near, adj, far):
        gu_got(0, src)
    wide = 2 * LANE

    def gate_tile(j, _):
        at = span(wide * j, wide, wide)
        gate = jnp.dot(nrm[...], wg[:, at], preferred_element_type=F32)
        ga[:, at] = gate / (1.0 + jnp.exp(-gate))
        for r, kind in enumerate(up_kinds):
            when((j == r) & (mid == 0), lambda kind=kind: gu_pass(kind, last, n_end))
        return 0

    def up_term(src, at):
        rows = span(depth * src, depth, depth)
        return jnp.dot(nrm[:, rows], wu[rows, at], preferred_element_type=F32)

    def up_tile(j, _):
        at = span(wide * j, wide, wide)
        upa[:, at] = up_term(s, at) + up_term(near, at) + up_term(third, at)
        return 0

    def hid_tile(j, _):
        at = span(wide * j, wide, wide)
        hid[:, at] = (ga[:, at] * (upa[:, at] + up_term(last, at))).astype(BF)
        return 0

    lax.fori_loop(0, n_mid // wide, gate_tile, 0)
    def end_down():
        dn_to(far)
        for k in range(subs):
            dn_pass(k, near)

    when(mid == 0, end_down)
    gu_got(1, near)
    gu_got(2, near)
    gu_got(1, third)
    gu_got(2, third)
    lax.fori_loop(0, n_mid // wide, up_tile, 0)
    gu_got(1, last)
    gu_got(2, last)
    lax.fori_loop(0, n_mid // wide, hid_tile, 0)

    def chunk(i):
        at = lax.div(i, subs)
        k = lax.rem(i, subs)
        b = pick(at, (0, 0, 1, 2, 2, 1, 3, 3))
        first = pick(at, (0, 1, 0, 0, 1, 1, 0, 1))
        half = first * (1 - g) + (1 - first) * g
        source = pick(b, (s, far, near, adj))
        return b, first, k, half * subs + k, source

    def ec(xo, ch):
        return remote(ec_out.at[xo, ch], ec_in.at[xo, ch], ec_s.at[xo, ch], ec_r.at[xo, ch], c_peer)

    def ex(ch):
        return remote(ex_out.at[ch], ex_in.at[ch], ex_s.at[ch], ex_r.at[ch], x_peer)

    def ez(ch):
        return remote(ez_out.at[ch], ez_in.at[ch], ez_s.at[ch], ez_r.at[ch], z_peer)

    steps = 4 * nch

    def produce(i):
        b, first, k, ch, source = chunk(i)
        when((b > 0) & (first == 1), lambda: dn_got(k, source))
        xo, co = lax.div(source, 2), lax.rem(source, 2)
        term = jnp.dot(
            hid[...], wd[:, span(cols * source + CHUNK * ch, CHUNK, CHUNK)],
            preferred_element_type=F32,
        )

        def send():
            ec_out[xo, ch] = term.astype(BF)
            ec(xo, ch).start()

        def keep():
            e_own[xo, ch] = term

        when(co != c, send)
        when(co == c, keep)

    def ahead(stage):
        lax.fori_loop(0, steps, lambda j, _: when(soon(j) == stage, lambda: deliver(j)) or 0, 0)

    def soon(i):
        return pick(lax.div(i, subs), (1, 1, 1, 2, 3, 3, 0, 0))

    def combine(i):
        _, _, _, ch, source = chunk(i)
        xo, co = lax.div(source, 2), lax.rem(source, 2)

        def mine():
            ec(xo, ch).wait_recv()
            value = e_own[xo, ch] + ec_in[xo, ch].astype(F32)

            def send():
                ex_out[ch] = value.astype(BF)
                ex(ch).start()

            def keep():
                e_own[xo, ch] = value

            when(xo != x, send)
            when(xo == x, keep)

        when(co == c, mine)

    def deliver(i):
        _, _, _, ch, source = chunk(i)

        def mine():
            ex(ch).wait_recv()
            theirs = span(tok * other_par, tok, tok)
            ours = span(tok * par, tok, tok)
            ez_out[ch] = (e_own[x, ch, theirs, :] + ex_in[ch, theirs, :].astype(F32)).astype(BF)
            ez(ch).start()
            e_fin[ch] = e_own[x, ch, ours, :] + ex_in[ch, ours, :].astype(F32)

        when(source == t, mine)


    def stretch(first, stop):
        def go(i, _):
            when(i < stop, lambda: produce(i))
            when(i >= first + 2, lambda: combine(i - 2))
            return 0

        lax.fori_loop(first, stop + 2, go, 0)

    stretch(0, 2 * subs)
    for k in range(subs):
        dn_pass(k, far)
    stretch(2 * subs, 6 * subs)
    when(mid == 1, lambda: ahead(1))
    for k in range(subs):
        dn_pass(k, adj)
    stretch(6 * subs, 7 * subs)
    when(mid == 1, lambda: ahead(2))
    stretch(7 * subs, steps)
    when(mid == 0, lambda: ahead(1))
    when(mid == 0, lambda: ahead(2))
    ahead(3)
    ahead(0)

    def finish(ch, _):
        ez(ch).wait_recv()
        at = span(CHUNK * ch, CHUNK, CHUNK)
        base = st[span(tok * par, tok, tok), span(cols * t + CHUNK * ch, CHUNK, CHUNK)]
        out[:, at] = (base.astype(F32) + (e_fin[ch] + ez_in[ch].astype(F32))).astype(BF)
        return 0

    lax.fori_loop(0, nch, finish, 0)

    when(s < 3, lambda: halo_right().wait_send())
    when(s > 0, lambda: halo_left().wait_send())
    for d in range(4):
        def sent(d=d):
            for kind in range(3):
                gu_send(kind, d).wait_send()
            for k in range(subs):
                dn_send(k, d).wait_send()

        when((s != d) & ((mid == 1) | (adj != d)), sent)

    def hopped():
        for kind in range(3):
            gu_hop(kind).wait_send()
        for k in range(subs):
            dn_hop(k).wait_send()

    when(mid == 1, hopped)

    def relayed(n, at):
        for src in (near, far, adj):
            for kind in range(3):
                piece = gu_piece(kind, src, g, n)
                remote(piece, piece, yg_s.at[kind, src], yg_r.at[kind, src], y_peer).wait_send()
            for k in range(subs):
                piece = wd.at[pl.ds(0, n), span(cols * src + half_c * g + CHUNK * k, CHUNK, CHUNK)]
                remote(piece, piece, yd_s.at[k, src], yd_r.at[k, src], y_peer).wait_send()

    by_role(relayed)

    def blocks_sent(b, _):
        c_copy(b).wait_send()
        x_copy(b).wait_send()
        ag_z(par, b).wait_send()
        for slot in range(2):
            ag_c(slot, b).wait_send()
            ag_x(slot, b).wait_send()
            ag_f(slot, b).wait_send()
        return 0

    lax.fori_loop(0, blocks, blocks_sent, 0)

    def chunks_sent(ch, _):
        for xo in range(2):
            ec(xo, ch).wait_send()
        ex(ch).wait_send()
        ez(ch).wait_send()
        return 0

    lax.fori_loop(0, nch, chunks_sent, 0)


def fused_body(
    resid, queries, keys_values, sink, out_weight, norm_gain, gate_weight, up_weight, down_weight
):
    tok, cols = queries.shape
    width = norm_gain.shape[0]
    ff = gate_weight.shape[1]
    n_mid = ff - (ff // LANE // 2) * LANE
    blocks = tok // WINDOW
    padded = tok + 2 * WINDOW
    nch = cols // CHUNK
    subs = nch // 2
    vmem = lambda shape, dtype=BF: pltpu.VMEM(shape, dtype)
    dma = lambda *shape: pltpu.SemaphoreType.DMA(shape)
    in_vmem = pl.BlockSpec(memory_space=pltpu.VMEM)
    in_hbm = pl.BlockSpec(memory_space=pl.ANY)
    scratch = [
        vmem((tok, cols)), vmem((tok, cols)), vmem((padded, 256)),
        vmem((padded, LANE), F32), vmem((padded, LANE), F32),
        vmem((2, padded, 256)), vmem((2, padded, 256)), vmem(out_weight.shape),
        vmem((width, n_mid)), vmem((width, n_mid)), vmem((n_mid, width)),
        vmem((2 * tok, width)), vmem((2 * tok, width)), vmem((2 * tok, n_mid)),
        vmem((2 * tok, n_mid), F32), vmem((2 * tok, n_mid), F32),
        vmem((blocks, WINDOW, 2 * cols), F32), vmem((blocks, WINDOW, 2 * cols)),
        vmem((blocks, WINDOW, 2 * cols)), vmem((blocks, WINDOW, cols)), vmem((blocks, WINDOW, cols)),
        vmem((2, nch, 2 * tok, CHUNK)), vmem((2, nch, 2 * tok, CHUNK)),
        vmem((2, nch, 2 * tok, CHUNK), F32),
        vmem((nch, 2 * tok, CHUNK)), vmem((nch, 2 * tok, CHUNK)),
        vmem((nch, tok, CHUNK)), vmem((nch, tok, CHUNK)), vmem((nch, tok, CHUNK), F32),
        dma(7), dma(2), dma(2),
        dma(3, 4), dma(3, 4), dma(3, 4), dma(3, 4),
        dma(subs, 4), dma(subs, 4), dma(subs, 4), dma(subs, 4), dma(3), dma(subs),
        dma(blocks), dma(blocks), dma(blocks), dma(blocks),
        dma(2, blocks), dma(2, blocks), dma(2, blocks), dma(2, blocks),
        dma(2, blocks), dma(2, blocks), dma(blocks), dma(blocks),
        dma(2, nch), dma(2, nch), dma(nch), dma(nch), dma(nch), dma(nch),
    ]
    return pl.pallas_call(
        fused_kernel,
        out_shape=jax.ShapeDtypeStruct((tok, cols), BF),
        in_specs=[pl.BlockSpec(memory_space=pltpu.SMEM)] + [in_vmem] * 5 + [in_hbm] * 7,
        out_specs=in_vmem,
        scratch_shapes=scratch,
        compiler_params=pltpu.CompilerParams(
            collective_id=0, has_side_effects=True, vmem_limit_bytes=WHOLE_VMEM
        ),
    )(
        sink, *angle_tables(tok * 4), norm_gain.reshape(1, width),
        resid, queries, keys_values.reshape(tok, -1), out_weight, gate_weight, up_weight, down_weight,
    )


def solution(mesh):
    return jax.shard_map(
        fused_body if fits(mesh) else body,
        mesh=mesh,
        in_specs=(
            P(("grp", "sp"), "tp"),
            P(("grp", "sp"), "tp"),
            P(("grp", "sp"), "tp", None),
            P("tp"),
            P("tp", None),
            P(),
            P("sp", "tp"),
            P("sp", "tp"),
            P("tp", "sp"),
        ),
        out_specs=P(("grp", "sp"), "tp"),
        check_vma=False,
    )
```

```python
import jax
import jax.numpy as jnp
from jax import lax
from jax.experimental import pallas as pl
from jax.experimental.pallas import tpu as pltpu
from jax.sharding import PartitionSpec as P
import numpy as np

HEAD_DIM = 64
WINDOW = 128
GRID_W = 64


def with_halo(cells, sides, width):
    for axis, dim in sides:
        count = lax.axis_size(axis)
        ends = count - 1
        head = lax.slice_in_dim(cells, 0, width, axis=dim)
        tail = lax.slice_in_dim(cells, cells.shape[dim] - width, cells.shape[dim], axis=dim)
        cells = jnp.concatenate(
            [
                lax.ppermute(tail, axis, [(i, (i + 1) % count) for i in range(ends)]),
                cells,
                lax.ppermute(head, axis, [((i + 1) % count, i) for i in range(ends)]),
            ],
            axis=dim,
        )
    return cells


def rotate(values, positions):
    quarter = 16
    inverse = 10000.0 ** (-jnp.arange(quarter, dtype=jnp.float32) / quarter)

    def turn(part, place):
        angle = place.astype(jnp.float32)[:, None] * inverse[None, :]
        cosine = jnp.cos(angle)[:, None, :]
        sine = jnp.sin(angle)[:, None, :]
        first, second = (part[..., :quarter], part[..., quarter:])
        return jnp.concatenate(
            [first * cosine - second * sine, second * cosine + first * sine], axis=-1
        )

    grid_row = positions // GRID_W
    grid_col = positions % GRID_W
    return jnp.concatenate(
        [turn(values[..., :32], grid_row), turn(values[..., 32:], grid_col)], axis=-1
    )


def share(weight, axis):
    parts = lax.axis_size("grp")
    size = weight.shape[axis] // parts
    part = lax.dynamic_slice_in_dim(weight, lax.axis_index("grp") * size, size, axis)
    return lax.all_gather(part, ("sp", "grp"), axis=axis, tiled=True)


def relay(blocks, axes, first_column):
    count, parts = lax.axis_size("sp"), lax.axis_size("grp")
    here, group = lax.axis_index("sp"), lax.axis_index("grp")

    def place(whole, value, axis, block, source, part):
        rows = block.shape[0]
        start = part * (rows // parts)
        at = (source * rows + start, 0)
        if axis == 1:
            columns = block.shape[1] * count
            at = (start, lax.rem(source * block.shape[1] + columns - first_column, columns))
        if axis == 1 and part is not group:
            value = jnp.where(here < count, value, jnp.zeros_like(value))
        return lax.dynamic_update_slice(whole, value, at)

    wholes, right, left, late = [], [], [], []
    for block, axis in zip(blocks, axes):
        shape = list(block.shape)
        shape[axis] *= count
        wholes.append(place(jnp.zeros(shape, block.dtype), block, axis, block, here, 0))
        rows = block.shape[0] // parts
        part = lax.dynamic_slice_in_dim(block, group * rows, rows, 0)
        right.append([part])
        left.append([part])
    for step in range(1, count):
        source = jnp.where(here >= step, here - step, step)
        for index, (block, axis) in enumerate(zip(blocks, axes)):
            right[index].append(
                lax.ppermute(
                    right[index][-1], "sp", [(i, i + 1) for i in range(step - 1, count - 1)]
                )
            )
            left[index].append(
                lax.ppermute(left[index][-1], "sp", [(i + 1, i) for i in range(count - step)])
            )
            came = [left[index][step - i] for i in range(step)] + [right[index][step]]
            value = lax.select_n(jnp.minimum(here, step), *came)
            whole = place(wholes[index], value, axis, block, source, group)
            for shift in range(1, parts):
                other = lax.ppermute(value, "grp", [(i, (i + shift) % parts) for i in range(parts)])
                part = (group - shift) % parts
                if step == count - 1 and index == len(blocks) - 1:
                    late.append((other, axis, block, source, part))
                    continue
                whole = place(whole, other, axis, block, source, part)
            wholes[index] = whole

    def finish(whole):
        for piece in late:
            whole = place(whole, *piece)
        return whole

    return wholes, finish


def swap(value, bit):
    return lax.ppermute(value, "tp", [(i, i ^ bit) for i in range(lax.axis_size("tp"))])


def sum_columns(terms, bit):
    here = lax.axis_index("tp")
    while bit:
        half = terms.shape[1] // 2
        mine = jnp.where((here & bit) > 0, half, 0)
        theirs = lax.dynamic_slice_in_dim(terms, half - mine, half, 1).astype(jnp.bfloat16)
        own = lax.dynamic_slice_in_dim(terms, mine, half, 1)
        terms = own + swap(theirs, bit).astype(jnp.float32)
        bit //= 2
    return terms


def body(
    resid, queries, keys_values, sink, out_weight, norm_gain, gate_weight, up_weight, down_weight
):
    tok = queries.shape[0]
    heads_here = queries.shape[1] // HEAD_DIM
    kv_here = keys_values.shape[1]
    group = heads_here // kv_here
    cols = resid.shape[1]
    offset = lax.axis_index("sp") * tok
    total_tokens = tok * lax.axis_size("sp")
    positions = offset + jnp.arange(tok, dtype=jnp.int32)
    rotated_q = rotate(
        queries.astype(jnp.float32).reshape(tok, heads_here, HEAD_DIM), positions
    ).astype(jnp.bfloat16)
    padded = with_halo(keys_values, (("sp", 0),), WINDOW)
    ranks, members = lax.axis_size("sp"), lax.axis_size("tp")
    high = members // 2
    direct = ranks <= 8 and ranks % 2 == 0 and members >= 2 and members & (members - 1) == 0
    if direct:
        half_columns = resid.shape[1] * members // 2
        near = jnp.where((lax.axis_index("tp") & high) > 0, half_columns, 0)
        padded, gate_weight, up_weight, down_weight = lax.optimization_barrier(
            (padded, gate_weight, up_weight, down_weight)
        )
        both = jnp.concatenate([gate_weight, up_weight], axis=1)
        (whole_both, whole_down), late = relay((both, down_weight), (0, 1), near)
    else:
        whole_both = jnp.concatenate([share(gate_weight, 0), share(up_weight, 0)], axis=1)
        whole_down = share(down_weight, 1)
    whole_out = lax.all_gather(out_weight, "tp", axis=0, tiled=True)
    key_positions = offset - WINDOW + jnp.arange(tok + 2 * WINDOW, dtype=jnp.int32)
    rotated_k = rotate(padded[..., :HEAD_DIM].astype(jnp.float32), key_positions).astype(
        jnp.bfloat16
    )
    padded = jnp.concatenate([rotated_k, padded[..., HEAD_DIM:]], axis=-1)
    blocks = tok // WINDOW
    key_blocks = jnp.stack(
        [padded[index * WINDOW : index * WINDOW + 3 * WINDOW] for index in range(blocks)]
    )
    grouped = rotated_q.reshape(blocks, WINDOW, kv_here, group, HEAD_DIM)
    scores = jnp.einsum(
        "nqkgd,njkd->nkgqj", grouped, key_blocks[..., :HEAD_DIM], preferred_element_type=jnp.float32
    ) * HEAD_DIM ** (-0.5)
    block_start = offset + WINDOW * jnp.arange(blocks, dtype=jnp.int32)
    query_pos = block_start[:, None] + jnp.arange(WINDOW, dtype=jnp.int32)[None, :]
    key_pos = block_start[:, None] - WINDOW + jnp.arange(3 * WINDOW, dtype=jnp.int32)[None, :]
    valid = (
        (jnp.abs(query_pos[:, :, None] - key_pos[:, None, :]) <= WINDOW)
        & (key_pos[:, None, :] >= 0)
        & (key_pos[:, None, :] < total_tokens)
    )
    scores = jnp.where(valid[:, None, None], scores, jnp.float32(-1e30))
    sink_grid = sink.reshape(kv_here, group)[None, :, :, None]
    top = jnp.maximum(jnp.max(scores, axis=-1), sink_grid)
    expo = jnp.exp(scores - top[..., None])
    denom = jnp.sum(expo, axis=-1) + jnp.exp(sink_grid - top)
    probs = (expo / denom[..., None]).astype(jnp.bfloat16)
    attended = jnp.einsum(
        "nkgqj,njkd->nqkgd", probs, key_blocks[..., HEAD_DIM:], preferred_element_type=jnp.float32
    )
    attended = attended.astype(jnp.bfloat16).reshape(tok, heads_here * HEAD_DIM)
    attn_rows, resid_rows = (
        lax.all_to_all(attended, "tp", split_axis=0, concat_axis=1, tiled=True),
        lax.all_to_all(resid, "tp", split_axis=0, concat_axis=1, tiled=True),
    )
    stream_part = (
        resid_rows.astype(jnp.float32)
        + jnp.dot(attn_rows, whole_out, preferred_element_type=jnp.float32)
    ).astype(jnp.bfloat16)
    stream = lax.all_gather(stream_part, "tp", axis=0, tiled=True)
    stream_cols = lax.dynamic_slice_in_dim(stream, lax.axis_index("tp") * cols, cols, 1)
    widened = stream.astype(jnp.float32)
    normed = (
        widened * lax.rsqrt(jnp.mean(widened * widened, axis=-1, keepdims=True) + 1e-06) * norm_gain
    ).astype(jnp.bfloat16)
    gate_up = jnp.dot(normed, whole_both, preferred_element_type=jnp.float32)
    gate, up = jnp.split(gate_up, 2, axis=1)
    hidden = (jax.nn.silu(gate) * up).astype(jnp.bfloat16)
    if direct:
        hidden, whole_down = lax.optimization_barrier((hidden, whole_down))
        whole_down = late(whole_down)
        far_terms = jnp.dot(
            hidden, whole_down[:, half_columns:], preferred_element_type=jnp.float32
        )
        far_sum = swap(sum_columns(far_terms, high // 2).astype(jnp.bfloat16), high)
        near_terms = jnp.dot(
            hidden, whole_down[:, :half_columns], preferred_element_type=jnp.float32
        )
        near_sum = sum_columns(near_terms, high // 2)
        return (
            stream_cols.astype(jnp.float32) + (near_sum + far_sum.astype(jnp.float32))
        ).astype(jnp.bfloat16)
    terms = jnp.dot(
        hidden,
        whole_down,
        preferred_element_type=jnp.float32,
    )
    summed = lax.psum_scatter(
        terms.astype(jnp.bfloat16), "tp", scatter_dimension=1, tiled=True
    ).astype(jnp.float32)
    return (stream_cols.astype(jnp.float32) + summed).astype(jnp.bfloat16)


LANE = 128
CHUNK = 128
BF = jnp.bfloat16
F32 = jnp.float32
WHOLE_VMEM = 67_043_328


def fits(mesh):
    return mesh.shape["sp"] == 4 and mesh.shape["tp"] == 4 and mesh.shape["grp"] == 2


def angle_tables(total):
    halo = WINDOW // GRID_W
    rows = np.arange(-halo, total // GRID_W + halo, dtype=np.float64)
    cols = np.arange(GRID_W, dtype=np.float64)
    entry = np.arange(LANE) % HEAD_DIM
    rate = 10000.0 ** (-(entry % 16) / 16.0)
    by_row = (entry // 32 == 0).astype(np.float64)
    sign = np.where(entry % 32 < 16, -1.0, 1.0)

    def table(places, used, wave, scale):
        return jnp.asarray(wave(places[:, None] * rate) * scale * used, jnp.float32)

    return (
        table(rows, by_row, np.cos, 1.0),
        table(rows, by_row, np.sin, sign),
        table(cols, 1 - by_row, np.cos, 1.0),
        table(cols, 1 - by_row, np.sin, sign),
    )


def fused_kernel(
    sink, row_cos, row_sin, col_cos, col_sin, gain,
    resid_in, q_in, kv_in, out_w_in, gate_in, up_in, down_in,
    out_hbm,
    out, q, resid, kv, cos, sin, kd, vd, out_w,
    wg, wu, wd, st, nrm, hid, ga, upa,
    own, c_out, c_in, x_out, x_in,
    ec_out, ec_in, e_own, ex_out, ex_in, ez_out, ez_in, ef_out, ef_in,
    local_sem, out_sem, h_s, h_r,
    zg_s, zg_r, yg_s, yg_r, zd_s, zd_r, yd_s, yd_r, hg_s, hd_s,
    c_s, c_r, x_s, x_r,
    ac_s, ac_r, ax_s, ax_r, af_s, af_r, az_s, az_r,
    ec_s, ec_r, ex_s, ex_r, ez_s, ez_r, ef_s, ef_r,
):
    tok, cols = q.shape
    blocks = tok // WINDOW
    depth, ff = gate_in.shape
    tiles = ff // LANE
    n_end = (tiles // 2) * LANE
    n_mid = ff - n_end
    half_d = depth // 2
    half_c = cols // 2
    subs = half_c // CHUNK
    nch = cols // CHUNK

    g, s, t = lax.axis_index("grp"), lax.axis_index("sp"), lax.axis_index("tp")
    x, c = lax.div(t, 2), lax.rem(t, 2)
    par = lax.rem(s, 2)
    mid = lax.rem(lax.div(s + 1, 2), 2)
    way = 1 - 2 * lax.div(s, 2)
    c_peer = {"tp": t + 1 - 2 * c}
    x_peer = {"tp": t + 2 - 4 * x}
    y_peer = {"grp": 1 - g}
    z_peer = {"sp": s + 1 - 2 * par}
    t_x = t + 2 - 4 * x
    t_c = t + 1 - 2 * c

    def ring(i):
        return lax.rem(s + way * i + 4, 4)

    near = ring(1 + 2 * mid)
    far = ring(3 - mid)
    adj = ring(2 - mid)

    def pick(i, values):
        found = values[0]
        for at in range(1, len(values)):
            found = jnp.where(i == at, values[at], found)
        return found

    def when(flag, fn):
        pl.when(flag)(fn)

    def by_role(fn):
        when(mid == 1, lambda: fn(n_mid, n_end))
        when(mid == 0, lambda: fn(n_end, 0))

    def span(start, size, unit):
        return pl.ds(pl.multiple_of(start, unit), size)

    def remote(src, dst, send, recv, to):
        return pltpu.make_async_remote_copy(
            src_ref=src, dst_ref=dst, send_sem=send, recv_sem=recv,
            device_id=to, device_id_type=pl.DeviceIdType.MESH,
        )

    locals_ = [
        pltpu.make_async_copy(kv_in, kv.at[pl.ds(WINDOW, tok)], local_sem.at[0]),
        pltpu.make_async_copy(q_in, q, local_sem.at[1]),
        pltpu.make_async_copy(out_w_in, out_w, local_sem.at[2]),
        pltpu.make_async_copy(resid_in, resid, local_sem.at[3]),
    ]
    for copy in locals_:
        copy.start()

    barrier = pltpu.get_barrier_semaphore()
    partners = [c_peer, x_peer, y_peer] + [{"sp": lax.rem(s + k, 4)} for k in (1, 2, 3)]
    for to in partners:
        pl.semaphore_signal(barrier, inc=1, device_id=to, device_id_type=pl.DeviceIdType.MESH)
    pl.semaphore_wait(barrier, len(partners))

    def halo_right():
        return remote(kv_in.at[pl.ds(tok - WINDOW, WINDOW)], kv.at[pl.ds(0, WINDOW)],
                      h_s.at[0], h_r.at[0], {"sp": lax.rem(s + 1, 4)})

    def halo_left():
        return remote(kv_in.at[pl.ds(0, WINDOW)], kv.at[pl.ds(tok + WINDOW, WINDOW)],
                      h_s.at[1], h_r.at[1], {"sp": lax.rem(s + 3, 4)})

    when(s < 3, lambda: halo_right().start())
    when(s > 0, lambda: halo_left().start())

    pieces = (
        (gate_in, wg, 0, half_d),
        (up_in, wu, 0, half_d // 2),
        (up_in, wu, half_d // 2, half_d // 2),
    )

    def gu_send(kind, d):
        n, at = (n_mid, n_end) if d in (1, 2) else (n_end, 0)
        src, dst, skip, rows = pieces[kind]
        return remote(
            src.at[span(half_d * g + skip, rows, rows), pl.ds(at, n)],
            dst.at[span(depth * s + half_d * g + skip, rows, rows), pl.ds(0, n)],
            zg_s.at[kind, d], zg_r.at[kind, s], {"sp": d},
        )

    def gu_piece(kind, src, which, n):
        _, ref, skip, rows = pieces[kind]
        return ref.at[span(depth * src + half_d * which + skip, rows, rows), pl.ds(0, n)]

    cut = n_mid // LANE // 2 * LANE

    def dn_rows(part, n):
        return (cut, n - cut) if part else (0, cut)

    def dn_send(q, d):
        n, at = (n_mid, n_end) if d in (1, 2) else (n_end, 0)
        k, part = divmod(q, 2)
        row, rows = dn_rows(part, n)
        return remote(
            down_in.at[pl.ds(at + row, rows), span(half_c * g + CHUNK * k, CHUNK, CHUNK)],
            wd.at[pl.ds(row, rows), span(cols * s + half_c * g + CHUNK * k, CHUNK, CHUNK)],
            zd_s.at[q, d], zd_r.at[q, s], {"sp": d},
        )

    def dn_piece(k, part, src, which, n):
        row, rows = dn_rows(part, n)
        return wd.at[pl.ds(row, rows), span(cols * src + half_c * which + CHUNK * k, CHUNK, CHUNK)]

    pair = s + 1 - 2 * par

    def to(d, send):
        for static in range(4):
            when(d == static, lambda static=static: send(static))

    def gu_to(d, kinds):
        to(d, lambda at: [gu_send(kind, at).start() for kind in kinds] and None)

    def dn_to(d):
        to(d, lambda at: [dn_send(q, at).start() for q in range(2 * subs)] and None)

    gate_kind, up_kinds = (0,), (1, 2)

    def first_sends(inner):
        gu_to(pair, gate_kind)
        if inner:
            gu_to(adj, gate_kind)
            gu_to(far, gate_kind)
            gu_to(pair, up_kinds)
            gu_to(adj, up_kinds)
        else:
            gu_to(far, gate_kind)
            gu_to(pair, up_kinds)

    when(mid == 1, lambda: first_sends(True))
    when(mid == 0, lambda: first_sends(False))

    def own_copies(n, at):
        return [
            pltpu.make_async_copy(gate_in.at[:, pl.ds(at, n)],
                                  wg.at[span(depth * s, depth, depth), pl.ds(0, n)], local_sem.at[4]),
            pltpu.make_async_copy(up_in.at[:, pl.ds(at, n)],
                                  wu.at[span(depth * s, depth, depth), pl.ds(0, n)], local_sem.at[5]),
            pltpu.make_async_copy(down_in.at[pl.ds(at, n), :],
                                  wd.at[pl.ds(0, n), span(cols * s, cols, cols)], local_sem.at[6]),
        ]


    def one_hot(pick):
        i = lax.broadcasted_iota(jnp.int32, (256, 256), 0)
        j = lax.broadcasted_iota(jnp.int32, (256, 256), 1)
        return jnp.where(i == pick(j), 1.0, 0.0).astype(BF)

    swap_m = one_hot(lambda j: j + 16 - 32 * lax.rem(lax.div(j, 16), 2))
    for i in range((tok + 2 * WINDOW) // GRID_W):
        r = lax.div(tok, GRID_W) * s + i
        here = pl.ds(GRID_W * i, GRID_W)
        cos[here, :] = row_cos[pl.ds(r, 1), :] + col_cos[...]
        sin[here, :] = row_sin[pl.ds(r, 1), :] + col_sin[...]

    def no_left():
        kv[pl.ds(0, WINDOW)] = jnp.zeros((WINDOW, *kv.shape[1:]), BF)

    def no_right():
        kv[pl.ds(tok + WINDOW, WINDOW)] = jnp.zeros((WINDOW, *kv.shape[1:]), BF)

    when(s == 0, no_left)
    when(s == 3, no_right)
    if n_mid > n_end:
        def no_pad():
            wd[pl.ds(n_end, n_mid - n_end), :] = jnp.zeros((n_mid - n_end, wd.shape[1]), BF)
            wg[:, pl.ds(n_end, n_mid - n_end)] = jnp.zeros((wg.shape[0], n_mid - n_end), BF)
            wu[:, pl.ds(n_end, n_mid - n_end)] = jnp.zeros((wu.shape[0], n_mid - n_end), BF)

        when(mid == 0, no_pad)

    locals_[0].wait()
    when(s > 0, lambda: halo_right().wait_recv())
    when(s < 3, lambda: halo_left().wait_recv())

    for i in range(tok // WINDOW + 2):
        here = pl.ds(WINDOW * i, WINDOW)
        raw = jnp.concatenate([kv[here, k, :] for k in range(2)], axis=1)
        lane = lax.broadcasted_iota(jnp.int32, (WINDOW, 256), 1)
        is_key = lax.rem(lane, 128) < HEAD_DIM
        turn_c = jnp.concatenate([cos[here, :]] * 2, axis=1)
        turn_s = jnp.concatenate([sin[here, :]] * 2, axis=1)
        other = jnp.dot(raw, swap_m, preferred_element_type=F32)
        value = raw.astype(F32)
        turned = jnp.where(is_key, value * turn_c + other * turn_s, value).astype(BF)
        for k in range(2):
            kd[k, here, :] = jnp.dot(
                turned, one_hot(lambda j: 128 * k + lax.rem(j, 64)), preferred_element_type=F32
            ).astype(BF)
            vd[k, here, :] = jnp.dot(
                turned, one_hot(lambda j: 128 * k + 64 + lax.rem(j, 64)), preferred_element_type=F32
            ).astype(BF)

    locals_[1].wait()
    locals_[2].wait()
    locals_[3].wait()

    def c_copy(b):
        return remote(c_out.at[b], c_in.at[b], c_s.at[b], c_r.at[b], c_peer)

    def x_copy(b):
        return remote(x_out.at[b], x_in.at[b], x_s.at[b], x_r.at[b], x_peer)

    def part(slot, b, owner):
        return st.at[span(tok * slot + WINDOW * b, WINDOW, WINDOW), span(cols * owner, cols, cols)]

    def ag_c(slot, b):
        ref = part(slot, b, t)
        return remote(ref, ref, ac_s.at[slot, b], ac_r.at[slot, b], c_peer)

    def ag_x(slot, b):
        ref = part(slot, b, t)
        return remote(ref, ref, ax_s.at[slot, b], ax_r.at[slot, b], x_peer)

    def ag_f(slot, b):
        ref = part(slot, b, t_x)
        return remote(ref, ref, af_s.at[slot, b], af_r.at[slot, b], c_peer)

    def ag_z(slot, b):
        ref = part(slot, b, t)
        return remote(ref, ref, az_s.at[b], az_r.at[b], z_peer)

    total = tok * 4

    def attend(b):
        rows = span(WINDOW * b, WINDOW, WINDOW)
        keys_at = span(WINDOW * b, 3 * WINDOW, WINDOW)
        place = span(WINDOW * b + WINDOW, WINDOW, WINDOW)
        turn_c = jnp.concatenate([cos[place, :]] * 2, axis=1)
        turn_s = jnp.concatenate([sin[place, :]] * 2, axis=1)
        head_of = lax.div(lax.broadcasted_iota(jnp.int32, (WINDOW, 256), 1), HEAD_DIM)
        i = lax.broadcasted_iota(jnp.int32, (WINDOW, 3 * WINDOW), 0)
        j = lax.broadcasted_iota(jnp.int32, (WINDOW, 3 * WINDOW), 1)
        first = tok * s + WINDOW * b - WINDOW
        valid = (j >= i) & (j <= i + 2 * WINDOW) & (j >= -first) & (j < total - first)
        bias = jnp.where(valid, 0.0, -1e30)
        outs = []
        for k in range(2):
            raw = q[rows, pl.ds(256 * k, 256)]
            other = jnp.dot(raw, swap_m, preferred_element_type=F32)
            turned = raw.astype(F32) * turn_c + other * turn_s
            stacked = jnp.concatenate(
                [jnp.where(head_of == h, turned, 0.0) for h in range(4)], axis=0
            ).astype(BF)
            scores = lax.dot_general(
                stacked, kd[k, keys_at, :], (((1,), (1,)), ((), ())), preferred_element_type=F32
            )
            probs = []
            for h in range(4):
                one = scores[WINDOW * h : WINDOW * (h + 1)] * HEAD_DIM ** (-0.5) + bias
                level = sink[4 * k + h]
                top = jnp.maximum(jnp.max(one, axis=1, keepdims=True), level)
                expo = jnp.exp(one - top)
                denom = jnp.sum(expo, axis=1, keepdims=True) + jnp.exp(level - top)
                probs.append((expo * (1.0 / denom)).astype(BF))
            mixed = jnp.dot(
                jnp.concatenate(probs, axis=0), vd[k, keys_at, :], preferred_element_type=F32
            )
            acc = jnp.zeros((WINDOW, 256), F32)
            for h in range(4):
                acc = jnp.where(head_of == h, mixed[WINDOW * h : WINDOW * (h + 1)], acc)
            outs.append(acc.astype(BF))
        att = jnp.concatenate(outs, axis=1)
        for xx in range(2):
            at = pl.ds(cols * xx, cols)
            c_out[b, :, at] = jnp.dot(
                att, out_w[:, span((2 * xx + 1 - c) * cols, cols, cols)], preferred_element_type=F32
            ).astype(BF)
            own[b, :, at] = jnp.dot(
                att, out_w[:, span((2 * xx + c) * cols, cols, cols)], preferred_element_type=F32
            )
        c_copy(b).start()

    def over_x(b):
        c_copy(b).wait_recv()
        mine, theirs = span(cols * x, cols, cols), span(cols * (1 - x), cols, cols)
        x_out[b] = (own[b, :, theirs] + c_in[b, :, theirs].astype(F32)).astype(BF)
        own[b, :, mine] = own[b, :, mine] + c_in[b, :, mine].astype(F32)
        x_copy(b).start()

    def to_stream(b):
        x_copy(b).wait_recv()
        rows = span(WINDOW * b, WINDOW, WINDOW)
        value = resid[rows, :].astype(F32) + (
            own[b, :, span(cols * x, cols, cols)] + x_in[b].astype(F32)
        )
        st[span(tok * par + WINDOW * b, WINDOW, WINDOW), span(cols * t, cols, cols)] = value.astype(BF)
        ag_z(par, b).start()
        ag_x(par, b).start()
        ag_c(par, b).start()


    def recv_x(slot, b):
        ref = part(slot, b, t_x)
        remote(ref, ref, ax_s.at[slot, b], ax_r.at[slot, b], x_peer).wait_recv()

    def recv_c(slot, b):
        ref = part(slot, b, t_c)
        remote(ref, ref, ac_s.at[slot, b], ac_r.at[slot, b], c_peer).wait_recv()

    def recv_f(slot, b):
        ref = part(slot, b, t_c + 2 - 4 * x)
        remote(ref, ref, af_s.at[slot, b], af_r.at[slot, b], c_peer).wait_recv()

    def recv_z(slot, b):
        ref = part(slot, b, t)
        remote(ref, ref, az_s.at[b], az_r.at[b], z_peer).wait_recv()

    def gu_pass(kind, src, n):
        piece = gu_piece(kind, src, g, n)
        remote(piece, piece, zg_s.at[kind, src], zg_r.at[kind, src], z_peer).wait_recv()
        remote(piece, piece, yg_s.at[kind, src], yg_r.at[kind, src], y_peer).start()
        if src is near and n == n_mid:
            gu_hop(kind).start()

    def gu_hop(kind):
        piece = gu_piece(kind, near, g, n_mid)
        return remote(piece, piece, hg_s.at[kind], zg_r.at[kind, near], {"sp": adj})

    def dn_hop(q):
        piece = dn_piece(q // 2, q % 2, near, g, n_mid)
        return remote(piece, piece, hd_s.at[q], zd_r.at[q, near], {"sp": adj})

    def gu_got(kind, src):
        def go(n, at):
            piece = gu_piece(kind, src, 1 - g, n)
            remote(piece, piece, yg_s.at[kind, src], yg_r.at[kind, src], y_peer).wait_recv()

        by_role(go)

    def dn_pass(k, src):
        def go(n, at):
            for part in range(2):
                q = 2 * k + part
                piece = dn_piece(k, part, src, g, n)
                remote(piece, piece, zd_s.at[q, src], zd_r.at[q, src], z_peer).wait_recv()
                remote(piece, piece, yd_s.at[q, src], yd_r.at[q, src], y_peer).start()
                if src is near and n == n_mid:
                    dn_hop(q).start()

        by_role(go)

    def dn_got(k, src):
        def go(n, at):
            for part in range(2):
                q = 2 * k + part
                piece = dn_piece(k, part, src, 1 - g, n)
                remote(piece, piece, yd_s.at[q, src], yd_r.at[q, src], y_peer).wait_recv()

        by_role(go)

    def normalize(slot, b):
        rows_at_once = 32

        def rows_of(i, _):
            here = span(tok * slot + WINDOW * b + rows_at_once * i, rows_at_once, rows_at_once)
            wide = st[here, :].astype(F32)
            scale = lax.rsqrt(jnp.mean(wide * wide, axis=1, keepdims=True) + 1e-06)
            nrm[here, :] = (wide * scale * gain[...]).astype(BF)
            return 0

        lax.fori_loop(0, WINDOW // rows_at_once, rows_of, 0)

    last, third = ring(2), ring(3 - 2 * mid)
    relay_mid = ((gate_kind, near), (gate_kind, adj), (up_kinds, near),
                 (up_kinds, adj), (gate_kind, far), (up_kinds, far))
    relay_end = ((gate_kind, near), (gate_kind, far), (up_kinds, near),
                 (gate_kind, adj), (up_kinds, far), (up_kinds, adj))

    def relay(r):
        def go(table, n):
            kinds, src = table[r]
            for kind in kinds:
                gu_pass(kind, src, n)

        def inner():
            go(relay_mid, n_mid)
            if r == 2:
                gu_to(far, up_kinds)

        when(mid == 1, inner)
        when(mid == 0, lambda: go(relay_end, n_end))

    def own_pass(b):
        recv_x(par, b)
        ag_f(par, b).start()

    def step(i, _):
        for r in range(3):
            when(i == 3 + r, lambda r=r: relay(r))
        when(i < blocks, lambda: attend(i))
        when((i >= 1) & (i < blocks + 1), lambda: over_x(i - 1))
        when((i >= 2) & (i < blocks + 2), lambda: to_stream(i - 2))
        when(i >= 3, lambda: own_pass(i - 3))
        return 0

    lax.fori_loop(0, blocks + 3, step, 0)

    def late():
        gu_to(far, up_kinds)
        dn_to(pair)

    when(mid == 0, late)
    when(mid == 1, lambda: dn_to(pair))
    by_role(lambda n, at: [copy.start() for copy in own_copies(n, at)] and None)
    relay(3)

    other_par = 1 - par

    def pair_pass(b, _):
        def first():
            recv_z(other_par, b)
            ag_x(other_par, b).start()
            ag_c(other_par, b).start()

        def second():
            recv_x(other_par, b - 2)
            ag_f(other_par, b - 2).start()

        def third():
            recv_c(par, b)
            recv_f(par, b)
            normalize(par, b)

        when(b < blocks, first)
        when(b < blocks, third)
        when(b >= 2, second)
        when(b == 3 - mid, lambda: relay(4))
        return 0

    lax.fori_loop(0, blocks + 2, pair_pass, 0)

    def pair_in(b, _):
        recv_c(other_par, b)
        recv_f(other_par, b)
        normalize(other_par, b)
        return 0

    def inner_down():
        for k in range(subs):
            dn_pass(k, near)
        dn_to(far)
        dn_to(adj)

    when(mid == 1, lambda: relay(5))
    when(mid == 1, inner_down)
    lax.fori_loop(0, blocks, pair_in, 0)
    by_role(lambda n, at: [copy.wait() for copy in own_copies(n, at)] and None)
    for src in (near, adj, far):
        gu_got(0, src)
    wide = 2 * LANE

    def gate_tile(j, _):
        at = span(wide * j, wide, wide)
        gate = jnp.dot(nrm[...], wg[:, at], preferred_element_type=F32)
        ga[:, at] = gate / (1.0 + jnp.exp(-gate))
        for r, kind in enumerate(up_kinds):
            when((j == r) & (mid == 0), lambda kind=kind: gu_pass(kind, last, n_end))
        return 0

    def up_term(src, at):
        rows = span(depth * src, depth, depth)
        return jnp.dot(nrm[:, rows], wu[rows, at], preferred_element_type=F32)

    def up_tile(j, _):
        at = span(wide * j, wide, wide)
        upa[:, at] = up_term(s, at) + up_term(near, at) + up_term(third, at)
        return 0

    def hid_tile(j, _):
        at = span(wide * j, wide, wide)
        hid[:, at] = (ga[:, at] * (upa[:, at] + up_term(last, at))).astype(BF)
        return 0

    lax.fori_loop(0, n_mid // wide, gate_tile, 0)
    def end_down():
        dn_to(far)
        for k in range(subs):
            dn_pass(k, near)

    when(mid == 0, end_down)
    gu_got(1, near)
    gu_got(2, near)
    gu_got(1, third)
    gu_got(2, third)
    lax.fori_loop(0, n_mid // wide, up_tile, 0)
    gu_got(1, last)
    gu_got(2, last)
    lax.fori_loop(0, n_mid // wide, hid_tile, 0)

    def chunk(i):
        at = lax.div(i, subs)
        k = lax.rem(i, subs)
        b = pick(at, (0, 0, 1, 2, 2, 1, 3, 3))
        first = pick(at, (0, 1, 0, 0, 1, 1, 0, 1))
        half = first * (1 - g) + (1 - first) * g
        source = pick(b, (s, far, near, adj))
        return b, first, k, half * subs + k, source

    def ec(xo, ch):
        return remote(ec_out.at[xo, ch], ec_in.at[xo, ch], ec_s.at[xo, ch], ec_r.at[xo, ch], c_peer)

    def ex(ch, which):
        rows = span(tok * (other_par, par)[which], tok, tok)
        return remote(ex_out.at[ch, rows], ex_in.at[ch, rows],
                      ex_s.at[which, ch], ex_r.at[which, ch], x_peer)

    def ez(ch):
        return remote(ez_out.at[ch], ez_in.at[ch], ez_s.at[ch], ez_r.at[ch], z_peer)

    steps = 4 * nch

    def produce(i):
        b, first, k, ch, source = chunk(i)
        when((b > 0) & (first == 1), lambda: dn_got(k, source))
        xo, co = lax.div(source, 2), lax.rem(source, 2)
        term = jnp.dot(
            hid[...], wd[:, span(cols * source + CHUNK * ch, CHUNK, CHUNK)],
            preferred_element_type=F32,
        )

        def send():
            ec_out[xo, ch] = term.astype(BF)
            ec(xo, ch).start()

        def keep():
            e_own[xo, ch] = term

        when(co != c, send)
        when(co == c, keep)

    def combine(i):
        _, _, _, ch, source = chunk(i)
        xo, co = lax.div(source, 2), lax.rem(source, 2)

        def mine():
            ec(xo, ch).wait_recv()
            value = e_own[xo, ch] + ec_in[xo, ch].astype(F32)

            def send():
                ex_out[ch] = value.astype(BF)
                ex(ch, 0).start()

            def keep():
                e_own[xo, ch] = value

            when(xo != x, send)
            when(xo == x, keep)

        when(co == c, mine)

    theirs = span(tok * other_par, tok, tok)
    ours = span(tok * par, tok, tok)

    def rest(i):
        _, _, _, ch, source = chunk(i)
        when((lax.rem(source, 2) == c) & (lax.div(source, 2) != x), lambda: ex(ch, 1).start())

    def deliver(i):
        _, _, _, ch, source = chunk(i)

        def mine():
            ex(ch, 0).wait_recv()
            ez_out[ch] = (e_own[x, ch, theirs, :] + ex_in[ch, theirs, :].astype(F32)).astype(BF)
            ez(ch).start()

        when(source == t, mine)

    def ahead(stage):
        lax.fori_loop(0, steps, lambda j, _: when(soon(j) == stage, lambda: deliver(j)) or 0, 0)

    def soon(i):
        return pick(lax.div(i, subs), (1, 2, 1, 2, 3, 3, 0, 0))

    adj_x, adj_c = lax.div(adj, 2), lax.rem(adj, 2)

    def ef(ch):
        return remote(ef_out.at[ch], ef_in.at[ch], ef_s.at[ch], ef_r.at[ch], z_peer)

    def combine_adj(i):
        _, _, _, ch, _ = chunk(i)

        def mine():
            ec(adj_x, ch).wait_recv()
            ef_out[ch] = (e_own[adj_x, ch, theirs, :] + ec_in[adj_x, ch, theirs, :].astype(F32)).astype(BF)
            ef(ch).start()
            e_own[adj_x, ch, ours, :] = (
                e_own[adj_x, ch, ours, :] + ec_in[adj_x, ch, ours, :].astype(F32)
            )

        when(adj_c == c, mine)

    def relay_adj(i):
        _, _, _, ch, _ = chunk(i)

        def mine():
            ef(ch).wait_recv()
            value = e_own[adj_x, ch, ours, :] + ef_in[ch].astype(F32)

            def send():
                ex_out[ch, ours, :] = value.astype(BF)
                ex(ch, 1).start()

            def keep():
                e_own[adj_x, ch, ours, :] = value

            when(adj_x != x, send)
            when(adj_x == x, keep)

        when(adj_c == c, mine)

    def stretch(first, stop, join=combine):
        def go(i, _):
            when(i < stop, lambda: produce(i))
            when(i >= first + 2, lambda: join(i - 2))
            return 0

        lax.fori_loop(first, stop + 2, go, 0)

    def relays(first, stop):
        lax.fori_loop(first, stop, lambda i, _: relay_adj(i) or 0, 0)

    stretch(0, 2 * subs)
    for k in range(subs):
        dn_pass(k, far)
    stretch(2 * subs, 6 * subs)
    lax.fori_loop(0, 6 * subs, lambda i, _: rest(i) or 0, 0)
    ahead(1)
    for k in range(subs):
        dn_pass(k, adj)
        if k == 0:
            when(mid == 1, lambda: ahead(2))
    stretch(6 * subs, 7 * subs, combine_adj)
    stretch(7 * subs, steps, combine_adj)
    when(mid == 0, lambda: ahead(2))
    ahead(3)
    relays(6 * subs, steps)

    def leave(ch):
        at = span(CHUNK * ch, CHUNK, CHUNK)
        return pltpu.make_async_copy(out.at[:, at], out_hbm.at[:, at], out_sem.at[ch])

    def finish(ch, _):
        ex(ch, 1).wait_recv()
        when(t != adj, lambda: ez(ch).wait_recv())
        at = span(CHUNK * ch, CHUNK, CHUNK)
        base = st[ours, span(cols * t + CHUNK * ch, CHUNK, CHUNK)].astype(F32)
        mine = e_own[x, ch, ours, :] + ex_in[ch, ours, :].astype(F32)

        def joined():
            out[:, at] = (base + (mine + ez_in[ch].astype(F32))).astype(BF)

        def whole():
            out[:, at] = (base + mine).astype(BF)

        when(t != adj, joined)
        when(t == adj, whole)
        leave(ch).start()
        return 0

    lax.fori_loop(0, nch, finish, 0)

    when(s < 3, lambda: halo_right().wait_send())
    when(s > 0, lambda: halo_left().wait_send())
    for d in range(4):
        def sent(d=d):
            for kind in range(3):
                gu_send(kind, d).wait_send()
            for q in range(2 * subs):
                dn_send(q, d).wait_send()

        when((s != d) & ((mid == 1) | (adj != d)), sent)

    def hopped():
        for kind in range(3):
            gu_hop(kind).wait_send()
        for q in range(2 * subs):
            dn_hop(q).wait_send()

    when(mid == 1, hopped)

    def relayed(n, at):
        for src in (near, far, adj):
            for kind in range(3):
                piece = gu_piece(kind, src, g, n)
                remote(piece, piece, yg_s.at[kind, src], yg_r.at[kind, src], y_peer).wait_send()
            for q in range(2 * subs):
                piece = dn_piece(q // 2, q % 2, src, g, n)
                remote(piece, piece, yd_s.at[q, src], yd_r.at[q, src], y_peer).wait_send()

    by_role(relayed)

    def blocks_sent(b, _):
        c_copy(b).wait_send()
        x_copy(b).wait_send()
        ag_z(par, b).wait_send()
        for slot in range(2):
            ag_c(slot, b).wait_send()
            ag_x(slot, b).wait_send()
            ag_f(slot, b).wait_send()
        return 0

    lax.fori_loop(0, blocks, blocks_sent, 0)

    def chunks_sent(ch, _):
        for xo in range(2):
            ec(xo, ch).wait_send()
        when(t_x != adj, lambda: ex(ch, 0).wait_send())
        ex(ch, 1).wait_send()
        leave(ch).wait()
        when(t != adj, lambda: ez(ch).wait_send())
        when(adj_c == c, lambda: ef(ch).wait_send())
        return 0

    lax.fori_loop(0, nch, chunks_sent, 0)


def fused_body(
    resid, queries, keys_values, sink, out_weight, norm_gain, gate_weight, up_weight, down_weight
):
    tok, cols = queries.shape
    width = norm_gain.shape[0]
    ff = gate_weight.shape[1]
    n_mid = ff - (ff // LANE // 2) * LANE
    blocks = tok // WINDOW
    padded = tok + 2 * WINDOW
    nch = cols // CHUNK
    subs = nch // 2
    vmem = lambda shape, dtype=BF: pltpu.VMEM(shape, dtype)
    dma = lambda *shape: pltpu.SemaphoreType.DMA(shape)
    in_vmem = pl.BlockSpec(memory_space=pltpu.VMEM)
    in_hbm = pl.BlockSpec(memory_space=pl.ANY)
    scratch = [
        vmem((tok, cols)), vmem((tok, cols)), vmem((tok, cols)), vmem((padded, *keys_values.shape[1:])),
        vmem((padded, LANE), F32), vmem((padded, LANE), F32),
        vmem((2, padded, 256)), vmem((2, padded, 256)), vmem(out_weight.shape),
        vmem((width, n_mid)), vmem((width, n_mid)), vmem((n_mid, width)),
        vmem((2 * tok, width)), vmem((2 * tok, width)), vmem((2 * tok, n_mid)),
        vmem((2 * tok, n_mid), F32), vmem((2 * tok, n_mid), F32),
        vmem((blocks, WINDOW, 2 * cols), F32), vmem((blocks, WINDOW, 2 * cols)),
        vmem((blocks, WINDOW, 2 * cols)), vmem((blocks, WINDOW, cols)), vmem((blocks, WINDOW, cols)),
        vmem((2, nch, 2 * tok, CHUNK)), vmem((2, nch, 2 * tok, CHUNK)),
        vmem((2, nch, 2 * tok, CHUNK), F32),
        vmem((nch, 2 * tok, CHUNK)), vmem((nch, 2 * tok, CHUNK)),
        vmem((nch, tok, CHUNK)), vmem((nch, tok, CHUNK)),
        vmem((nch, tok, CHUNK)), vmem((nch, tok, CHUNK)),
        dma(7), dma(nch), dma(2), dma(2),
        dma(3, 4), dma(3, 4), dma(3, 4), dma(3, 4),
        dma(nch, 4), dma(nch, 4), dma(nch, 4), dma(nch, 4), dma(3), dma(nch),
        dma(blocks), dma(blocks), dma(blocks), dma(blocks),
        dma(2, blocks), dma(2, blocks), dma(2, blocks), dma(2, blocks),
        dma(2, blocks), dma(2, blocks), dma(blocks), dma(blocks),
        dma(2, nch), dma(2, nch), dma(2, nch), dma(2, nch), dma(nch), dma(nch),
        dma(nch), dma(nch),
    ]
    return pl.pallas_call(
        fused_kernel,
        out_shape=jax.ShapeDtypeStruct((tok, cols), BF),
        in_specs=[pl.BlockSpec(memory_space=pltpu.SMEM)] + [in_vmem] * 5 + [in_hbm] * 7,
        out_specs=in_hbm,
        scratch_shapes=scratch,
        compiler_params=pltpu.CompilerParams(
            collective_id=0, has_side_effects=True, vmem_limit_bytes=WHOLE_VMEM
        ),
    )(
        sink, *angle_tables(tok * 4), norm_gain.reshape(1, width),
        resid, queries, keys_values, out_weight, gate_weight, up_weight, down_weight,
    )


def solution(mesh):
    return jax.shard_map(
        fused_body if fits(mesh) else body,
        mesh=mesh,
        in_specs=(
            P(("grp", "sp"), "tp"),
            P(("grp", "sp"), "tp"),
            P(("grp", "sp"), "tp", None),
            P("tp"),
            P("tp", None),
            P(),
            P("sp", "tp"),
            P("sp", "tp"),
            P("tp", "sp"),
        ),
        out_specs=P(("grp", "sp"), "tp"),
        check_vma=False,
    )
```

```python
import jax
import jax.numpy as jnp
from jax import lax
from jax.experimental import pallas as pl
from jax.experimental.pallas import tpu as pltpu
from jax.sharding import PartitionSpec as P
import numpy as np

HEAD_DIM = 64
WINDOW = 128
GRID_W = 64


def with_halo(cells, sides, width):
    for axis, dim in sides:
        count = lax.axis_size(axis)
        ends = count - 1
        head = lax.slice_in_dim(cells, 0, width, axis=dim)
        tail = lax.slice_in_dim(cells, cells.shape[dim] - width, cells.shape[dim], axis=dim)
        cells = jnp.concatenate(
            [
                lax.ppermute(tail, axis, [(i, (i + 1) % count) for i in range(ends)]),
                cells,
                lax.ppermute(head, axis, [((i + 1) % count, i) for i in range(ends)]),
            ],
            axis=dim,
        )
    return cells


def rotate(values, positions):
    quarter = 16
    inverse = 10000.0 ** (-jnp.arange(quarter, dtype=jnp.float32) / quarter)

    def turn(part, place):
        angle = place.astype(jnp.float32)[:, None] * inverse[None, :]
        cosine = jnp.cos(angle)[:, None, :]
        sine = jnp.sin(angle)[:, None, :]
        first, second = (part[..., :quarter], part[..., quarter:])
        return jnp.concatenate(
            [first * cosine - second * sine, second * cosine + first * sine], axis=-1
        )

    grid_row = positions // GRID_W
    grid_col = positions % GRID_W
    return jnp.concatenate(
        [turn(values[..., :32], grid_row), turn(values[..., 32:], grid_col)], axis=-1
    )


def share(weight, axis):
    parts = lax.axis_size("grp")
    size = weight.shape[axis] // parts
    part = lax.dynamic_slice_in_dim(weight, lax.axis_index("grp") * size, size, axis)
    return lax.all_gather(part, ("sp", "grp"), axis=axis, tiled=True)


def relay(blocks, axes, first_column):
    count, parts = lax.axis_size("sp"), lax.axis_size("grp")
    here, group = lax.axis_index("sp"), lax.axis_index("grp")

    def place(whole, value, axis, block, source, part):
        rows = block.shape[0]
        start = part * (rows // parts)
        at = (source * rows + start, 0)
        if axis == 1:
            columns = block.shape[1] * count
            at = (start, lax.rem(source * block.shape[1] + columns - first_column, columns))
        if axis == 1 and part is not group:
            value = jnp.where(here < count, value, jnp.zeros_like(value))
        return lax.dynamic_update_slice(whole, value, at)

    wholes, right, left, late = [], [], [], []
    for block, axis in zip(blocks, axes):
        shape = list(block.shape)
        shape[axis] *= count
        wholes.append(place(jnp.zeros(shape, block.dtype), block, axis, block, here, 0))
        rows = block.shape[0] // parts
        part = lax.dynamic_slice_in_dim(block, group * rows, rows, 0)
        right.append([part])
        left.append([part])
    for step in range(1, count):
        source = jnp.where(here >= step, here - step, step)
        for index, (block, axis) in enumerate(zip(blocks, axes)):
            right[index].append(
                lax.ppermute(
                    right[index][-1], "sp", [(i, i + 1) for i in range(step - 1, count - 1)]
                )
            )
            left[index].append(
                lax.ppermute(left[index][-1], "sp", [(i + 1, i) for i in range(count - step)])
            )
            came = [left[index][step - i] for i in range(step)] + [right[index][step]]
            value = lax.select_n(jnp.minimum(here, step), *came)
            whole = place(wholes[index], value, axis, block, source, group)
            for shift in range(1, parts):
                other = lax.ppermute(value, "grp", [(i, (i + shift) % parts) for i in range(parts)])
                part = (group - shift) % parts
                if step == count - 1 and index == len(blocks) - 1:
                    late.append((other, axis, block, source, part))
                    continue
                whole = place(whole, other, axis, block, source, part)
            wholes[index] = whole

    def finish(whole):
        for piece in late:
            whole = place(whole, *piece)
        return whole

    return wholes, finish


def swap(value, bit):
    return lax.ppermute(value, "tp", [(i, i ^ bit) for i in range(lax.axis_size("tp"))])


def sum_columns(terms, bit):
    here = lax.axis_index("tp")
    while bit:
        half = terms.shape[1] // 2
        mine = jnp.where((here & bit) > 0, half, 0)
        theirs = lax.dynamic_slice_in_dim(terms, half - mine, half, 1).astype(jnp.bfloat16)
        own = lax.dynamic_slice_in_dim(terms, mine, half, 1)
        terms = own + swap(theirs, bit).astype(jnp.float32)
        bit //= 2
    return terms


def body(
    resid, queries, keys_values, sink, out_weight, norm_gain, gate_weight, up_weight, down_weight
):
    tok = queries.shape[0]
    heads_here = queries.shape[1] // HEAD_DIM
    kv_here = keys_values.shape[1]
    group = heads_here // kv_here
    cols = resid.shape[1]
    offset = lax.axis_index("sp") * tok
    total_tokens = tok * lax.axis_size("sp")
    positions = offset + jnp.arange(tok, dtype=jnp.int32)
    rotated_q = rotate(
        queries.astype(jnp.float32).reshape(tok, heads_here, HEAD_DIM), positions
    ).astype(jnp.bfloat16)
    padded = with_halo(keys_values, (("sp", 0),), WINDOW)
    ranks, members = lax.axis_size("sp"), lax.axis_size("tp")
    high = members // 2
    direct = ranks <= 8 and ranks % 2 == 0 and members >= 2 and members & (members - 1) == 0
    if direct:
        half_columns = resid.shape[1] * members // 2
        near = jnp.where((lax.axis_index("tp") & high) > 0, half_columns, 0)
        padded, gate_weight, up_weight, down_weight = lax.optimization_barrier(
            (padded, gate_weight, up_weight, down_weight)
        )
        both = jnp.concatenate([gate_weight, up_weight], axis=1)
        (whole_both, whole_down), late = relay((both, down_weight), (0, 1), near)
    else:
        whole_both = jnp.concatenate([share(gate_weight, 0), share(up_weight, 0)], axis=1)
        whole_down = share(down_weight, 1)
    whole_out = lax.all_gather(out_weight, "tp", axis=0, tiled=True)
    key_positions = offset - WINDOW + jnp.arange(tok + 2 * WINDOW, dtype=jnp.int32)
    rotated_k = rotate(padded[..., :HEAD_DIM].astype(jnp.float32), key_positions).astype(
        jnp.bfloat16
    )
    padded = jnp.concatenate([rotated_k, padded[..., HEAD_DIM:]], axis=-1)
    blocks = tok // WINDOW
    key_blocks = jnp.stack(
        [padded[index * WINDOW : index * WINDOW + 3 * WINDOW] for index in range(blocks)]
    )
    grouped = rotated_q.reshape(blocks, WINDOW, kv_here, group, HEAD_DIM)
    scores = jnp.einsum(
        "nqkgd,njkd->nkgqj", grouped, key_blocks[..., :HEAD_DIM], preferred_element_type=jnp.float32
    ) * HEAD_DIM ** (-0.5)
    block_start = offset + WINDOW * jnp.arange(blocks, dtype=jnp.int32)
    query_pos = block_start[:, None] + jnp.arange(WINDOW, dtype=jnp.int32)[None, :]
    key_pos = block_start[:, None] - WINDOW + jnp.arange(3 * WINDOW, dtype=jnp.int32)[None, :]
    valid = (
        (jnp.abs(query_pos[:, :, None] - key_pos[:, None, :]) <= WINDOW)
        & (key_pos[:, None, :] >= 0)
        & (key_pos[:, None, :] < total_tokens)
    )
    scores = jnp.where(valid[:, None, None], scores, jnp.float32(-1e30))
    sink_grid = sink.reshape(kv_here, group)[None, :, :, None]
    top = jnp.maximum(jnp.max(scores, axis=-1), sink_grid)
    expo = jnp.exp(scores - top[..., None])
    denom = jnp.sum(expo, axis=-1) + jnp.exp(sink_grid - top)
    probs = (expo / denom[..., None]).astype(jnp.bfloat16)
    attended = jnp.einsum(
        "nkgqj,njkd->nqkgd", probs, key_blocks[..., HEAD_DIM:], preferred_element_type=jnp.float32
    )
    attended = attended.astype(jnp.bfloat16).reshape(tok, heads_here * HEAD_DIM)
    attn_rows, resid_rows = (
        lax.all_to_all(attended, "tp", split_axis=0, concat_axis=1, tiled=True),
        lax.all_to_all(resid, "tp", split_axis=0, concat_axis=1, tiled=True),
    )
    stream_part = (
        resid_rows.astype(jnp.float32)
        + jnp.dot(attn_rows, whole_out, preferred_element_type=jnp.float32)
    ).astype(jnp.bfloat16)
    stream = lax.all_gather(stream_part, "tp", axis=0, tiled=True)
    stream_cols = lax.dynamic_slice_in_dim(stream, lax.axis_index("tp") * cols, cols, 1)
    widened = stream.astype(jnp.float32)
    normed = (
        widened * lax.rsqrt(jnp.mean(widened * widened, axis=-1, keepdims=True) + 1e-06) * norm_gain
    ).astype(jnp.bfloat16)
    gate_up = jnp.dot(normed, whole_both, preferred_element_type=jnp.float32)
    gate, up = jnp.split(gate_up, 2, axis=1)
    hidden = (jax.nn.silu(gate) * up).astype(jnp.bfloat16)
    if direct:
        hidden, whole_down = lax.optimization_barrier((hidden, whole_down))
        whole_down = late(whole_down)
        far_terms = jnp.dot(
            hidden, whole_down[:, half_columns:], preferred_element_type=jnp.float32
        )
        far_sum = swap(sum_columns(far_terms, high // 2).astype(jnp.bfloat16), high)
        near_terms = jnp.dot(
            hidden, whole_down[:, :half_columns], preferred_element_type=jnp.float32
        )
        near_sum = sum_columns(near_terms, high // 2)
        return (
            stream_cols.astype(jnp.float32) + (near_sum + far_sum.astype(jnp.float32))
        ).astype(jnp.bfloat16)
    terms = jnp.dot(
        hidden,
        whole_down,
        preferred_element_type=jnp.float32,
    )
    summed = lax.psum_scatter(
        terms.astype(jnp.bfloat16), "tp", scatter_dimension=1, tiled=True
    ).astype(jnp.float32)
    return (stream_cols.astype(jnp.float32) + summed).astype(jnp.bfloat16)


LANE = 128
CHUNK = 128
BF = jnp.bfloat16
F32 = jnp.float32
WHOLE_VMEM = 67_043_328


def fits(mesh):
    return mesh.shape["sp"] == 4 and mesh.shape["tp"] == 4 and mesh.shape["grp"] == 2


def angle_tables(total):
    halo = WINDOW // GRID_W
    rows = np.arange(-halo, total // GRID_W + halo, dtype=np.float64)
    cols = np.arange(GRID_W, dtype=np.float64)
    entry = np.arange(LANE) % HEAD_DIM
    rate = 10000.0 ** (-(entry % 16) / 16.0)
    by_row = (entry // 32 == 0).astype(np.float64)
    sign = np.where(entry % 32 < 16, -1.0, 1.0)

    def table(places, used, wave, scale):
        return jnp.asarray(wave(places[:, None] * rate) * scale * used, jnp.float32)

    return (
        table(rows, by_row, np.cos, 1.0),
        table(rows, by_row, np.sin, sign),
        table(cols, 1 - by_row, np.cos, 1.0),
        table(cols, 1 - by_row, np.sin, sign),
    )


def fused_kernel(
    sink_in, row_cos_in, row_sin_in, col_cos_in, col_sin_in, gain_in,
    resid_in, q_in, kv_in, out_w_in, gate_in, up_in, down_in,
    out_hbm,
    sink, row_cos, row_sin, col_cos, col_sin, gain,
    out, q, resid, kv, cos, sin, kd, vd, out_w,
    wg, wu, wd, st, nrm, hid, ga, upa,
    own, c_out, c_in, x_out, x_in,
    ec_out, ec_in, e_own, ex_out, ex_in, ez_out, ez_in, ef_out, ef_in,
    local_sem, out_sem, h_s, h_r,
    zg_s, zg_r, yg_s, yg_r, zd_s, zd_r, yd_s, yd_r, hg_s, hd_s,
    c_s, c_r, x_s, x_r,
    ac_s, ac_r, ax_s, ax_r, af_s, af_r, az_s, az_r,
    ec_s, ec_r, ex_s, ex_r, ez_s, ez_r, ef_s, ef_r,
):
    tok, cols = q.shape
    blocks = tok // WINDOW
    depth, ff = gate_in.shape
    tiles = ff // LANE
    n_end = (tiles // 2) * LANE
    n_mid = ff - n_end
    half_d = depth // 2
    half_c = cols // 2
    subs = half_c // CHUNK
    nch = cols // CHUNK

    g, s, t = lax.axis_index("grp"), lax.axis_index("sp"), lax.axis_index("tp")
    x, c = lax.div(t, 2), lax.rem(t, 2)
    par = lax.rem(s, 2)
    mid = lax.rem(lax.div(s + 1, 2), 2)
    way = 1 - 2 * lax.div(s, 2)
    c_peer = {"tp": t + 1 - 2 * c}
    x_peer = {"tp": t + 2 - 4 * x}
    y_peer = {"grp": 1 - g}
    z_peer = {"sp": s + 1 - 2 * par}
    t_x = t + 2 - 4 * x
    t_c = t + 1 - 2 * c

    def ring(i):
        return lax.rem(s + way * i + 4, 4)

    near = ring(1 + 2 * mid)
    far = ring(3 - mid)
    adj = ring(2 - mid)

    def pick(i, values):
        found = values[0]
        for at in range(1, len(values)):
            found = jnp.where(i == at, values[at], found)
        return found

    def when(flag, fn):
        pl.when(flag)(fn)

    def by_role(fn):
        when(mid == 1, lambda: fn(n_mid, n_end))
        when(mid == 0, lambda: fn(n_end, 0))

    def span(start, size, unit):
        return pl.ds(pl.multiple_of(start, unit), size)

    def remote(src, dst, send, recv, to):
        return pltpu.make_async_remote_copy(
            src_ref=src, dst_ref=dst, send_sem=send, recv_sem=recv,
            device_id=to, device_id_type=pl.DeviceIdType.MESH,
        )

    barrier = pltpu.get_barrier_semaphore()
    partners = [c_peer, x_peer, y_peer] + [{"sp": lax.rem(s + k, 4)} for k in (1, 2, 3)]
    for to in partners:
        pl.semaphore_signal(barrier, inc=1, device_id=to, device_id_type=pl.DeviceIdType.MESH)
    locals_ = [
        pltpu.make_async_copy(kv_in, kv.at[pl.ds(WINDOW, tok)], local_sem.at[0]),
        pltpu.make_async_copy(q_in, q, local_sem.at[1]),
        pltpu.make_async_copy(out_w_in, out_w, local_sem.at[2]),
        pltpu.make_async_copy(resid_in, resid, local_sem.at[3]),
    ]
    small = [
        pltpu.make_async_copy(src, dst, local_sem.at[7 + i])
        for i, (src, dst) in enumerate((
            (row_cos_in, row_cos), (row_sin_in, row_sin), (col_cos_in, col_cos),
            (col_sin_in, col_sin), (gain_in, gain), (sink_in, sink),
        ))
    ]
    for copy in locals_ + small:
        copy.start()
    pl.semaphore_wait(barrier, len(partners))

    def halo_right():
        return remote(kv_in.at[pl.ds(tok - WINDOW, WINDOW)], kv.at[pl.ds(0, WINDOW)],
                      h_s.at[0], h_r.at[0], {"sp": lax.rem(s + 1, 4)})

    def halo_left():
        return remote(kv_in.at[pl.ds(0, WINDOW)], kv.at[pl.ds(tok + WINDOW, WINDOW)],
                      h_s.at[1], h_r.at[1], {"sp": lax.rem(s + 3, 4)})

    when(s < 3, lambda: halo_right().start())
    when(s > 0, lambda: halo_left().start())

    pieces = (
        (gate_in, wg, 0, half_d),
        (up_in, wu, 0, half_d // 2),
        (up_in, wu, half_d // 2, half_d // 2),
    )

    def gu_send(kind, d):
        n, at = (n_mid, n_end) if d in (1, 2) else (n_end, 0)
        src, dst, skip, rows = pieces[kind]
        return remote(
            src.at[span(half_d * g + skip, rows, rows), pl.ds(at, n)],
            dst.at[span(depth * s + half_d * g + skip, rows, rows), pl.ds(0, n)],
            zg_s.at[kind, d], zg_r.at[kind, s], {"sp": d},
        )

    def gu_piece(kind, src, which, n):
        _, ref, skip, rows = pieces[kind]
        return ref.at[span(depth * src + half_d * which + skip, rows, rows), pl.ds(0, n)]

    cut = n_mid // LANE // 2 * LANE

    def dn_rows(part, n):
        return (cut, n - cut) if part else (0, cut)

    def dn_send(q, d):
        n, at = (n_mid, n_end) if d in (1, 2) else (n_end, 0)
        k, part = divmod(q, 2)
        row, rows = dn_rows(part, n)
        return remote(
            down_in.at[pl.ds(at + row, rows), span(half_c * g + CHUNK * k, CHUNK, CHUNK)],
            wd.at[pl.ds(row, rows), span(cols * s + half_c * g + CHUNK * k, CHUNK, CHUNK)],
            zd_s.at[q, d], zd_r.at[q, s], {"sp": d},
        )

    def dn_piece(k, part, src, which, n):
        row, rows = dn_rows(part, n)
        return wd.at[pl.ds(row, rows), span(cols * src + half_c * which + CHUNK * k, CHUNK, CHUNK)]

    pair = s + 1 - 2 * par

    def to(d, send):
        for static in range(4):
            when(d == static, lambda static=static: send(static))

    def gu_to(d, kinds):
        to(d, lambda at: [gu_send(kind, at).start() for kind in kinds] and None)

    def dn_to(d):
        to(d, lambda at: [dn_send(q, at).start() for q in range(2 * subs)] and None)

    gate_kind, up_kinds = (0,), (1, 2)

    def first_sends(inner):
        gu_to(pair, gate_kind)
        if inner:
            gu_to(adj, gate_kind)
            gu_to(far, gate_kind)
            gu_to(pair, up_kinds)
            gu_to(adj, up_kinds)
        else:
            gu_to(far, gate_kind)
            gu_to(pair, up_kinds)

    when(mid == 1, lambda: first_sends(True))
    when(mid == 0, lambda: first_sends(False))

    def own_copies(n, at):
        return [
            pltpu.make_async_copy(gate_in.at[:, pl.ds(at, n)],
                                  wg.at[span(depth * s, depth, depth), pl.ds(0, n)], local_sem.at[4]),
            pltpu.make_async_copy(up_in.at[:, pl.ds(at, n)],
                                  wu.at[span(depth * s, depth, depth), pl.ds(0, n)], local_sem.at[5]),
            pltpu.make_async_copy(down_in.at[pl.ds(at, n), :],
                                  wd.at[pl.ds(0, n), span(cols * s, cols, cols)], local_sem.at[6]),
        ]


    def one_hot(pick):
        i = lax.broadcasted_iota(jnp.int32, (256, 256), 0)
        j = lax.broadcasted_iota(jnp.int32, (256, 256), 1)
        return jnp.where(i == pick(j), 1.0, 0.0).astype(BF)

    for copy in small:
        copy.wait()
    swap_m = one_hot(lambda j: j + 16 - 32 * lax.rem(lax.div(j, 16), 2))
    for i in range((tok + 2 * WINDOW) // GRID_W):
        r = lax.div(tok, GRID_W) * s + i
        here = pl.ds(GRID_W * i, GRID_W)
        cos[here, :] = row_cos[pl.ds(r, 1), :] + col_cos[...]
        sin[here, :] = row_sin[pl.ds(r, 1), :] + col_sin[...]

    def no_left():
        kv[pl.ds(0, WINDOW)] = jnp.zeros((WINDOW, *kv.shape[1:]), BF)

    def no_right():
        kv[pl.ds(tok + WINDOW, WINDOW)] = jnp.zeros((WINDOW, *kv.shape[1:]), BF)

    when(s == 0, no_left)
    when(s == 3, no_right)
    if n_mid > n_end:
        def no_pad():
            wd[pl.ds(n_end, n_mid - n_end), :] = jnp.zeros((n_mid - n_end, wd.shape[1]), BF)
            wg[:, pl.ds(n_end, n_mid - n_end)] = jnp.zeros((wg.shape[0], n_mid - n_end), BF)
            wu[:, pl.ds(n_end, n_mid - n_end)] = jnp.zeros((wu.shape[0], n_mid - n_end), BF)

        when(mid == 0, no_pad)

    locals_[0].wait()
    when(s > 0, lambda: halo_right().wait_recv())
    when(s < 3, lambda: halo_left().wait_recv())

    for i in range(tok // WINDOW + 2):
        here = pl.ds(WINDOW * i, WINDOW)
        raw = jnp.concatenate([kv[here, k, :] for k in range(2)], axis=1)
        lane = lax.broadcasted_iota(jnp.int32, (WINDOW, 256), 1)
        is_key = lax.rem(lane, 128) < HEAD_DIM
        turn_c = jnp.concatenate([cos[here, :]] * 2, axis=1)
        turn_s = jnp.concatenate([sin[here, :]] * 2, axis=1)
        other = jnp.dot(raw, swap_m, preferred_element_type=F32)
        value = raw.astype(F32)
        turned = jnp.where(is_key, value * turn_c + other * turn_s, value).astype(BF)
        for k in range(2):
            kd[k, here, :] = jnp.dot(
                turned, one_hot(lambda j: 128 * k + lax.rem(j, 64)), preferred_element_type=F32
            ).astype(BF)
            vd[k, here, :] = jnp.dot(
                turned, one_hot(lambda j: 128 * k + 64 + lax.rem(j, 64)), preferred_element_type=F32
            ).astype(BF)

    locals_[1].wait()
    locals_[2].wait()
    locals_[3].wait()

    def c_copy(b):
        return remote(c_out.at[b], c_in.at[b], c_s.at[b], c_r.at[b], c_peer)

    def x_copy(b):
        return remote(x_out.at[b], x_in.at[b], x_s.at[b], x_r.at[b], x_peer)

    def part(slot, b, owner):
        return st.at[span(tok * slot + WINDOW * b, WINDOW, WINDOW), span(cols * owner, cols, cols)]

    def ag_c(slot, b):
        ref = part(slot, b, t)
        return remote(ref, ref, ac_s.at[slot, b], ac_r.at[slot, b], c_peer)

    def ag_x(slot, b):
        ref = part(slot, b, t)
        return remote(ref, ref, ax_s.at[slot, b], ax_r.at[slot, b], x_peer)

    def ag_f(slot, b):
        ref = part(slot, b, t_x)
        return remote(ref, ref, af_s.at[slot, b], af_r.at[slot, b], c_peer)

    def ag_z(slot, b):
        ref = part(slot, b, t)
        return remote(ref, ref, az_s.at[b], az_r.at[b], z_peer)

    total = tok * 4

    def attend(b):
        rows = span(WINDOW * b, WINDOW, WINDOW)
        keys_at = span(WINDOW * b, 3 * WINDOW, WINDOW)
        place = span(WINDOW * b + WINDOW, WINDOW, WINDOW)
        turn_c = jnp.concatenate([cos[place, :]] * 2, axis=1)
        turn_s = jnp.concatenate([sin[place, :]] * 2, axis=1)
        head_of = lax.div(lax.broadcasted_iota(jnp.int32, (WINDOW, 256), 1), HEAD_DIM)
        i = lax.broadcasted_iota(jnp.int32, (WINDOW, 3 * WINDOW), 0)
        j = lax.broadcasted_iota(jnp.int32, (WINDOW, 3 * WINDOW), 1)
        first = tok * s + WINDOW * b - WINDOW
        valid = (j >= i) & (j <= i + 2 * WINDOW) & (j >= -first) & (j < total - first)
        bias = jnp.where(valid, 0.0, -1e30)
        outs = []
        for k in range(2):
            raw = q[rows, pl.ds(256 * k, 256)]
            other = jnp.dot(raw, swap_m, preferred_element_type=F32)
            turned = raw.astype(F32) * turn_c + other * turn_s
            stacked = jnp.concatenate(
                [jnp.where(head_of == h, turned, 0.0) for h in range(4)], axis=0
            ).astype(BF)
            scores = lax.dot_general(
                stacked, kd[k, keys_at, :], (((1,), (1,)), ((), ())), preferred_element_type=F32
            )
            probs = []
            for h in range(4):
                one = scores[WINDOW * h : WINDOW * (h + 1)] * HEAD_DIM ** (-0.5) + bias
                level = sink[:, pl.ds(4 * k + h, 1)]
                top = jnp.maximum(jnp.max(one, axis=1, keepdims=True), level)
                expo = jnp.exp(one - top)
                denom = jnp.sum(expo, axis=1, keepdims=True) + jnp.exp(level - top)
                probs.append((expo * (1.0 / denom)).astype(BF))
            mixed = jnp.dot(
                jnp.concatenate(probs, axis=0), vd[k, keys_at, :], preferred_element_type=F32
            )
            acc = jnp.zeros((WINDOW, 256), F32)
            for h in range(4):
                acc = jnp.where(head_of == h, mixed[WINDOW * h : WINDOW * (h + 1)], acc)
            outs.append(acc.astype(BF))
        att = jnp.concatenate(outs, axis=1)
        for xx in range(2):
            at = pl.ds(cols * xx, cols)
            c_out[b, :, at] = jnp.dot(
                att, out_w[:, span((2 * xx + 1 - c) * cols, cols, cols)], preferred_element_type=F32
            ).astype(BF)
            own[b, :, at] = jnp.dot(
                att, out_w[:, span((2 * xx + c) * cols, cols, cols)], preferred_element_type=F32
            )
        c_copy(b).start()

    def over_x(b):
        c_copy(b).wait_recv()
        mine, theirs = span(cols * x, cols, cols), span(cols * (1 - x), cols, cols)
        x_out[b] = (own[b, :, theirs] + c_in[b, :, theirs].astype(F32)).astype(BF)
        own[b, :, mine] = own[b, :, mine] + c_in[b, :, mine].astype(F32)
        x_copy(b).start()

    def to_stream(b):
        x_copy(b).wait_recv()
        rows = span(WINDOW * b, WINDOW, WINDOW)
        value = resid[rows, :].astype(F32) + (
            own[b, :, span(cols * x, cols, cols)] + x_in[b].astype(F32)
        )
        st[span(tok * par + WINDOW * b, WINDOW, WINDOW), span(cols * t, cols, cols)] = value.astype(BF)
        ag_z(par, b).start()
        ag_x(par, b).start()
        ag_c(par, b).start()


    def recv_x(slot, b):
        ref = part(slot, b, t_x)
        remote(ref, ref, ax_s.at[slot, b], ax_r.at[slot, b], x_peer).wait_recv()

    def recv_c(slot, b):
        ref = part(slot, b, t_c)
        remote(ref, ref, ac_s.at[slot, b], ac_r.at[slot, b], c_peer).wait_recv()

    def recv_f(slot, b):
        ref = part(slot, b, t_c + 2 - 4 * x)
        remote(ref, ref, af_s.at[slot, b], af_r.at[slot, b], c_peer).wait_recv()

    def recv_z(slot, b):
        ref = part(slot, b, t)
        remote(ref, ref, az_s.at[b], az_r.at[b], z_peer).wait_recv()

    def gu_pass(kind, src, n):
        piece = gu_piece(kind, src, g, n)
        remote(piece, piece, zg_s.at[kind, src], zg_r.at[kind, src], z_peer).wait_recv()
        remote(piece, piece, yg_s.at[kind, src], yg_r.at[kind, src], y_peer).start()
        if src is near and n == n_mid:
            gu_hop(kind).start()

    def gu_hop(kind):
        piece = gu_piece(kind, near, g, n_mid)
        return remote(piece, piece, hg_s.at[kind], zg_r.at[kind, near], {"sp": adj})

    def dn_hop(q):
        piece = dn_piece(q // 2, q % 2, near, g, n_mid)
        return remote(piece, piece, hd_s.at[q], zd_r.at[q, near], {"sp": adj})

    def gu_got(kind, src):
        def go(n, at):
            piece = gu_piece(kind, src, 1 - g, n)
            remote(piece, piece, yg_s.at[kind, src], yg_r.at[kind, src], y_peer).wait_recv()

        by_role(go)

    def dn_pass(k, src):
        def go(n, at):
            for part in range(2):
                q = 2 * k + part
                piece = dn_piece(k, part, src, g, n)
                remote(piece, piece, zd_s.at[q, src], zd_r.at[q, src], z_peer).wait_recv()
                remote(piece, piece, yd_s.at[q, src], yd_r.at[q, src], y_peer).start()
                if src is near and n == n_mid:
                    dn_hop(q).start()

        by_role(go)

    def dn_got(k, src):
        def go(n, at):
            for part in range(2):
                q = 2 * k + part
                piece = dn_piece(k, part, src, 1 - g, n)
                remote(piece, piece, yd_s.at[q, src], yd_r.at[q, src], y_peer).wait_recv()

        by_role(go)

    def normalize(slot, b):
        rows_at_once = 32

        def rows_of(i, _):
            here = span(tok * slot + WINDOW * b + rows_at_once * i, rows_at_once, rows_at_once)
            wide = st[here, :].astype(F32)
            scale = lax.rsqrt(jnp.mean(wide * wide, axis=1, keepdims=True) + 1e-06)
            nrm[here, :] = (wide * scale * gain[...]).astype(BF)
            return 0

        lax.fori_loop(0, WINDOW // rows_at_once, rows_of, 0)

    last, third = ring(2), ring(3 - 2 * mid)
    relay_mid = ((gate_kind, near), (gate_kind, adj), (up_kinds, near),
                 (up_kinds, adj), (gate_kind, far), (up_kinds, far))
    relay_end = ((gate_kind, near), (gate_kind, far), (up_kinds, near),
                 (gate_kind, adj), (up_kinds, far), (up_kinds, adj))

    def relay(r):
        def go(table, n):
            kinds, src = table[r]
            for kind in kinds:
                gu_pass(kind, src, n)

        def inner():
            go(relay_mid, n_mid)
            if r == 2:
                gu_to(far, up_kinds)

        when(mid == 1, inner)
        when(mid == 0, lambda: go(relay_end, n_end))

    def own_pass(b):
        recv_x(par, b)
        ag_f(par, b).start()

    def step(i, _):
        for r in range(3):
            when(i == 3 + r, lambda r=r: relay(r))
        when(i < blocks, lambda: attend(i))
        when((i >= 1) & (i < blocks + 1), lambda: over_x(i - 1))
        when((i >= 2) & (i < blocks + 2), lambda: to_stream(i - 2))
        when(i >= 3, lambda: own_pass(i - 3))
        return 0

    lax.fori_loop(0, blocks + 3, step, 0)

    def late():
        gu_to(far, up_kinds)
        dn_to(pair)

    when(mid == 0, late)
    when(mid == 1, lambda: dn_to(pair))
    by_role(lambda n, at: [copy.start() for copy in own_copies(n, at)] and None)
    relay(3)

    other_par = 1 - par

    def pair_pass(b, _):
        def first():
            recv_z(other_par, b)
            ag_x(other_par, b).start()
            ag_c(other_par, b).start()

        def second():
            recv_x(other_par, b - 2)
            ag_f(other_par, b - 2).start()

        def third():
            recv_c(par, b)
            recv_f(par, b)
            normalize(par, b)

        when(b < blocks, first)
        when(b < blocks, third)
        when(b >= 2, second)
        when(b == 3 - mid, lambda: relay(4))
        return 0

    lax.fori_loop(0, blocks + 2, pair_pass, 0)

    def pair_in(b, _):
        recv_c(other_par, b)
        recv_f(other_par, b)
        normalize(other_par, b)
        return 0

    def inner_down():
        for k in range(subs):
            dn_pass(k, near)
        dn_to(far)
        dn_to(adj)

    when(mid == 1, lambda: relay(5))
    when(mid == 1, inner_down)
    lax.fori_loop(0, blocks, pair_in, 0)
    by_role(lambda n, at: [copy.wait() for copy in own_copies(n, at)] and None)
    for src in (near, adj, far):
        gu_got(0, src)
    wide = 2 * LANE

    def gate_tile(j, _):
        at = span(wide * j, wide, wide)
        gate = jnp.dot(nrm[...], wg[:, at], preferred_element_type=F32)
        ga[:, at] = gate / (1.0 + jnp.exp(-gate))
        for r, kind in enumerate(up_kinds):
            when((j == r) & (mid == 0), lambda kind=kind: gu_pass(kind, last, n_end))
        return 0

    def up_term(src, at):
        rows = span(depth * src, depth, depth)
        return jnp.dot(nrm[:, rows], wu[rows, at], preferred_element_type=F32)

    def up_tile(j, _):
        at = span(wide * j, wide, wide)
        upa[:, at] = up_term(s, at) + up_term(near, at) + up_term(third, at)
        return 0

    def hid_tile(j, _):
        at = span(wide * j, wide, wide)
        hid[:, at] = (ga[:, at] * (upa[:, at] + up_term(last, at))).astype(BF)
        return 0

    lax.fori_loop(0, n_mid // wide, gate_tile, 0)
    def end_down():
        dn_to(far)
        for k in range(subs):
            dn_pass(k, near)

    when(mid == 0, end_down)
    gu_got(1, near)
    gu_got(2, near)
    gu_got(1, third)
    gu_got(2, third)
    lax.fori_loop(0, n_mid // wide, up_tile, 0)
    gu_got(1, last)
    gu_got(2, last)
    lax.fori_loop(0, n_mid // wide, hid_tile, 0)

    def chunk(i):
        at = lax.div(i, subs)
        k = lax.rem(i, subs)
        b = pick(at, (0, 0, 1, 2, 2, 1, 3, 3))
        first = pick(at, (0, 1, 0, 0, 1, 1, 0, 1))
        half = first * (1 - g) + (1 - first) * g
        source = pick(b, (s, far, near, adj))
        return b, first, k, half * subs + k, source

    def ec(xo, ch):
        return remote(ec_out.at[xo, ch], ec_in.at[xo, ch], ec_s.at[xo, ch], ec_r.at[xo, ch], c_peer)

    def ex(ch, which):
        rows = span(tok * (other_par, par)[which], tok, tok)
        return remote(ex_out.at[ch, rows], ex_in.at[ch, rows],
                      ex_s.at[which, ch], ex_r.at[which, ch], x_peer)

    def ez(ch):
        return remote(ez_out.at[ch], ez_in.at[ch], ez_s.at[ch], ez_r.at[ch], z_peer)

    steps = 4 * nch

    def produce(i):
        b, first, k, ch, source = chunk(i)
        when((b > 0) & (first == 1), lambda: dn_got(k, source))
        xo, co = lax.div(source, 2), lax.rem(source, 2)
        term = jnp.dot(
            hid[...], wd[:, span(cols * source + CHUNK * ch, CHUNK, CHUNK)],
            preferred_element_type=F32,
        )

        def send():
            ec_out[xo, ch] = term.astype(BF)
            ec(xo, ch).start()

        def keep():
            e_own[xo, ch] = term

        when(co != c, send)
        when(co == c, keep)

    def combine(i):
        _, _, _, ch, source = chunk(i)
        xo, co = lax.div(source, 2), lax.rem(source, 2)

        def mine():
            ec(xo, ch).wait_recv()
            value = e_own[xo, ch] + ec_in[xo, ch].astype(F32)

            def send():
                ex_out[ch] = value.astype(BF)
                ex(ch, 0).start()

            def keep():
                e_own[xo, ch] = value

            when(xo != x, send)
            when(xo == x, keep)

        when(co == c, mine)

    theirs = span(tok * other_par, tok, tok)
    ours = span(tok * par, tok, tok)

    def rest(i):
        _, _, _, ch, source = chunk(i)
        when((lax.rem(source, 2) == c) & (lax.div(source, 2) != x), lambda: ex(ch, 1).start())

    def deliver(i):
        _, _, _, ch, source = chunk(i)

        def mine():
            ex(ch, 0).wait_recv()
            ez_out[ch] = (e_own[x, ch, theirs, :] + ex_in[ch, theirs, :].astype(F32)).astype(BF)
            ez(ch).start()

        when(source == t, mine)

    def ahead(stage):
        lax.fori_loop(0, steps, lambda j, _: when(soon(j) == stage, lambda: deliver(j)) or 0, 0)

    def soon(i):
        return pick(lax.div(i, subs), (1, 1, 1, 2, 3, 2, 0, 0))

    adj_x, adj_c = lax.div(adj, 2), lax.rem(adj, 2)

    def ef(ch):
        return remote(ef_out.at[ch], ef_in.at[ch], ef_s.at[ch], ef_r.at[ch], z_peer)

    def combine_adj(i):
        _, _, _, ch, _ = chunk(i)

        def mine():
            ec(adj_x, ch).wait_recv()
            ef_out[ch] = (e_own[adj_x, ch, theirs, :] + ec_in[adj_x, ch, theirs, :].astype(F32)).astype(BF)
            ef(ch).start()
            e_own[adj_x, ch, ours, :] = (
                e_own[adj_x, ch, ours, :] + ec_in[adj_x, ch, ours, :].astype(F32)
            )

        when(adj_c == c, mine)

    def relay_adj(i):
        _, _, _, ch, _ = chunk(i)

        def mine():
            ef(ch).wait_recv()
            value = e_own[adj_x, ch, ours, :] + ef_in[ch].astype(F32)

            def send():
                ex_out[ch, ours, :] = value.astype(BF)
                ex(ch, 1).start()

            def keep():
                e_own[adj_x, ch, ours, :] = value

            when(adj_x != x, send)
            when(adj_x == x, keep)

        when(adj_c == c, mine)

    def stretch(first, stop, join=combine):
        def go(i, _):
            when(i < stop, lambda: produce(i))
            when(i >= first + 2, lambda: join(i - 2))
            return 0

        lax.fori_loop(first, stop + 2, go, 0)

    def relays(first, stop):
        lax.fori_loop(first, stop, lambda i, _: relay_adj(i) or 0, 0)

    stretch(0, 2 * subs)
    for k in range(subs):
        dn_pass(k, far)
    stretch(2 * subs, 6 * subs)
    lax.fori_loop(0, 6 * subs, lambda i, _: rest(i) or 0, 0)
    ahead(1)
    for k in range(subs):
        dn_pass(k, adj)
    when(mid == 1, lambda: ahead(2))
    stretch(6 * subs, 7 * subs, combine_adj)
    when(mid == 1, lambda: relays(6 * subs, 7 * subs))
    stretch(7 * subs, steps, combine_adj)
    when(mid == 0, lambda: ahead(2))
    ahead(3)
    when(s < 3, lambda: halo_right().wait_send())
    when(s > 0, lambda: halo_left().wait_send())
    for d in range(4):
        def sent(d=d):
            for kind in range(3):
                gu_send(kind, d).wait_send()
            for q in range(2 * subs):
                dn_send(q, d).wait_send()

        when((s != d) & ((mid == 1) | (adj != d)), sent)

    def hopped():
        for kind in range(3):
            gu_hop(kind).wait_send()
        for q in range(2 * subs):
            dn_hop(q).wait_send()

    when(mid == 1, hopped)

    def relayed(n, at):
        for src in (near, far, adj):
            for kind in range(3):
                piece = gu_piece(kind, src, g, n)
                remote(piece, piece, yg_s.at[kind, src], yg_r.at[kind, src], y_peer).wait_send()
            for q in range(2 * subs):
                piece = dn_piece(q // 2, q % 2, src, g, n)
                remote(piece, piece, yd_s.at[q, src], yd_r.at[q, src], y_peer).wait_send()

    by_role(relayed)

    def blocks_sent(b, _):
        c_copy(b).wait_send()
        x_copy(b).wait_send()
        ag_z(par, b).wait_send()
        for slot in range(2):
            ag_c(slot, b).wait_send()
            ag_x(slot, b).wait_send()
            ag_f(slot, b).wait_send()
        return 0

    lax.fori_loop(0, blocks, blocks_sent, 0)

    def cores_sent(ch, _):
        for xo in range(2):
            ec(xo, ch).wait_send()
        return 0

    lax.fori_loop(0, nch, cores_sent, 0)

    when(mid == 0, lambda: relays(6 * subs, 7 * subs))
    relays(7 * subs, steps)

    def leave(ch):
        at = span(CHUNK * ch, CHUNK, CHUNK)
        return pltpu.make_async_copy(out.at[:, at], out_hbm.at[:, at], out_sem.at[ch])

    def finish(ch, _):
        ex(ch, 1).wait_recv()
        when(t != adj, lambda: ez(ch).wait_recv())
        at = span(CHUNK * ch, CHUNK, CHUNK)
        base = st[ours, span(cols * t + CHUNK * ch, CHUNK, CHUNK)].astype(F32)
        mine = e_own[x, ch, ours, :] + ex_in[ch, ours, :].astype(F32)

        def joined():
            out[:, at] = (base + (mine + ez_in[ch].astype(F32))).astype(BF)

        def whole():
            out[:, at] = (base + mine).astype(BF)

        when(t != adj, joined)
        when(t == adj, whole)
        leave(ch).start()
        return 0

    lax.fori_loop(0, nch, finish, 0)

    def chunks_sent(ch, _):
        when(t_x != adj, lambda: ex(ch, 0).wait_send())
        ex(ch, 1).wait_send()
        leave(ch).wait()
        when(t != adj, lambda: ez(ch).wait_send())
        when(adj_c == c, lambda: ef(ch).wait_send())
        return 0

    lax.fori_loop(0, nch, chunks_sent, 0)


def fused_body(
    resid, queries, keys_values, sink, out_weight, norm_gain, gate_weight, up_weight, down_weight
):
    tok, cols = queries.shape
    width = norm_gain.shape[0]
    ff = gate_weight.shape[1]
    n_mid = ff - (ff // LANE // 2) * LANE
    blocks = tok // WINDOW
    padded = tok + 2 * WINDOW
    nch = cols // CHUNK
    subs = nch // 2
    vmem = lambda shape, dtype=BF: pltpu.VMEM(shape, dtype)
    dma = lambda *shape: pltpu.SemaphoreType.DMA(shape)
    in_hbm = pl.BlockSpec(memory_space=pl.ANY)
    rows = tok * 4 // GRID_W + 2 * (WINDOW // GRID_W)
    scratch = [
        vmem((1, sink.shape[0]), F32), vmem((rows, LANE), F32), vmem((rows, LANE), F32),
        vmem((GRID_W, LANE), F32), vmem((GRID_W, LANE), F32), vmem((1, width), F32),
        vmem((tok, cols)), vmem((tok, cols)), vmem((tok, cols)), vmem((padded, *keys_values.shape[1:])),
        vmem((padded, LANE), F32), vmem((padded, LANE), F32),
        vmem((2, padded, 256)), vmem((2, padded, 256)), vmem(out_weight.shape),
        vmem((width, n_mid)), vmem((width, n_mid)), vmem((n_mid, width)),
        vmem((2 * tok, width)), vmem((2 * tok, width)), vmem((2 * tok, n_mid)),
        vmem((2 * tok, n_mid), F32), vmem((2 * tok, n_mid), F32),
        vmem((blocks, WINDOW, 2 * cols), F32), vmem((blocks, WINDOW, 2 * cols)),
        vmem((blocks, WINDOW, 2 * cols)), vmem((blocks, WINDOW, cols)), vmem((blocks, WINDOW, cols)),
        vmem((2, nch, 2 * tok, CHUNK)), vmem((2, nch, 2 * tok, CHUNK)),
        vmem((2, nch, 2 * tok, CHUNK), F32),
        vmem((nch, 2 * tok, CHUNK)), vmem((nch, 2 * tok, CHUNK)),
        vmem((nch, tok, CHUNK)), vmem((nch, tok, CHUNK)),
        vmem((nch, tok, CHUNK)), vmem((nch, tok, CHUNK)),
        dma(13), dma(nch), dma(2), dma(2),
        dma(3, 4), dma(3, 4), dma(3, 4), dma(3, 4),
        dma(nch, 4), dma(nch, 4), dma(nch, 4), dma(nch, 4), dma(3), dma(nch),
        dma(blocks), dma(blocks), dma(blocks), dma(blocks),
        dma(2, blocks), dma(2, blocks), dma(2, blocks), dma(2, blocks),
        dma(2, blocks), dma(2, blocks), dma(blocks), dma(blocks),
        dma(2, nch), dma(2, nch), dma(2, nch), dma(2, nch), dma(nch), dma(nch),
        dma(nch), dma(nch),
    ]
    return pl.pallas_call(
        fused_kernel,
        out_shape=jax.ShapeDtypeStruct((tok, cols), BF),
        in_specs=[in_hbm] * 13,
        out_specs=in_hbm,
        scratch_shapes=scratch,
        compiler_params=pltpu.CompilerParams(
            collective_id=0, has_side_effects=True, vmem_limit_bytes=WHOLE_VMEM
        ),
    )(
        sink.reshape(1, -1), *angle_tables(tok * 4), norm_gain.reshape(1, width),
        resid, queries, keys_values, out_weight, gate_weight, up_weight, down_weight,
    )


def solution(mesh):
    return jax.shard_map(
        fused_body if fits(mesh) else body,
        mesh=mesh,
        in_specs=(
            P(("grp", "sp"), "tp"),
            P(("grp", "sp"), "tp"),
            P(("grp", "sp"), "tp", None),
            P("tp"),
            P("tp", None),
            P(),
            P("sp", "tp"),
            P("sp", "tp"),
            P("tp", "sp"),
        ),
        out_specs=P(("grp", "sp"), "tp"),
        check_vma=False,
    )
```

```python
import jax
import jax.numpy as jnp
from jax import lax
from jax.experimental import pallas as pl
from jax.experimental.pallas import tpu as pltpu
from jax.sharding import PartitionSpec as P
import numpy as np

HEAD_DIM = 64
WINDOW = 128
GRID_W = 64


def with_halo(cells, sides, width):
    for axis, dim in sides:
        count = lax.axis_size(axis)
        ends = count - 1
        head = lax.slice_in_dim(cells, 0, width, axis=dim)
        tail = lax.slice_in_dim(cells, cells.shape[dim] - width, cells.shape[dim], axis=dim)
        cells = jnp.concatenate(
            [
                lax.ppermute(tail, axis, [(i, (i + 1) % count) for i in range(ends)]),
                cells,
                lax.ppermute(head, axis, [((i + 1) % count, i) for i in range(ends)]),
            ],
            axis=dim,
        )
    return cells


def rotate(values, positions):
    quarter = 16
    inverse = 10000.0 ** (-jnp.arange(quarter, dtype=jnp.float32) / quarter)

    def turn(part, place):
        angle = place.astype(jnp.float32)[:, None] * inverse[None, :]
        cosine = jnp.cos(angle)[:, None, :]
        sine = jnp.sin(angle)[:, None, :]
        first, second = (part[..., :quarter], part[..., quarter:])
        return jnp.concatenate(
            [first * cosine - second * sine, second * cosine + first * sine], axis=-1
        )

    grid_row = positions // GRID_W
    grid_col = positions % GRID_W
    return jnp.concatenate(
        [turn(values[..., :32], grid_row), turn(values[..., 32:], grid_col)], axis=-1
    )


def share(weight, axis):
    parts = lax.axis_size("grp")
    size = weight.shape[axis] // parts
    part = lax.dynamic_slice_in_dim(weight, lax.axis_index("grp") * size, size, axis)
    return lax.all_gather(part, ("sp", "grp"), axis=axis, tiled=True)


def relay(blocks, axes, first_column):
    count, parts = lax.axis_size("sp"), lax.axis_size("grp")
    here, group = lax.axis_index("sp"), lax.axis_index("grp")

    def place(whole, value, axis, block, source, part):
        rows = block.shape[0]
        start = part * (rows // parts)
        at = (source * rows + start, 0)
        if axis == 1:
            columns = block.shape[1] * count
            at = (start, lax.rem(source * block.shape[1] + columns - first_column, columns))
        if axis == 1 and part is not group:
            value = jnp.where(here < count, value, jnp.zeros_like(value))
        return lax.dynamic_update_slice(whole, value, at)

    wholes, right, left, late = [], [], [], []
    for block, axis in zip(blocks, axes):
        shape = list(block.shape)
        shape[axis] *= count
        wholes.append(place(jnp.zeros(shape, block.dtype), block, axis, block, here, 0))
        rows = block.shape[0] // parts
        part = lax.dynamic_slice_in_dim(block, group * rows, rows, 0)
        right.append([part])
        left.append([part])
    for step in range(1, count):
        source = jnp.where(here >= step, here - step, step)
        for index, (block, axis) in enumerate(zip(blocks, axes)):
            right[index].append(
                lax.ppermute(
                    right[index][-1], "sp", [(i, i + 1) for i in range(step - 1, count - 1)]
                )
            )
            left[index].append(
                lax.ppermute(left[index][-1], "sp", [(i + 1, i) for i in range(count - step)])
            )
            came = [left[index][step - i] for i in range(step)] + [right[index][step]]
            value = lax.select_n(jnp.minimum(here, step), *came)
            whole = place(wholes[index], value, axis, block, source, group)
            for shift in range(1, parts):
                other = lax.ppermute(value, "grp", [(i, (i + shift) % parts) for i in range(parts)])
                part = (group - shift) % parts
                if step == count - 1 and index == len(blocks) - 1:
                    late.append((other, axis, block, source, part))
                    continue
                whole = place(whole, other, axis, block, source, part)
            wholes[index] = whole

    def finish(whole):
        for piece in late:
            whole = place(whole, *piece)
        return whole

    return wholes, finish


def swap(value, bit):
    return lax.ppermute(value, "tp", [(i, i ^ bit) for i in range(lax.axis_size("tp"))])


def sum_columns(terms, bit):
    here = lax.axis_index("tp")
    while bit:
        half = terms.shape[1] // 2
        mine = jnp.where((here & bit) > 0, half, 0)
        theirs = lax.dynamic_slice_in_dim(terms, half - mine, half, 1).astype(jnp.bfloat16)
        own = lax.dynamic_slice_in_dim(terms, mine, half, 1)
        terms = own + swap(theirs, bit).astype(jnp.float32)
        bit //= 2
    return terms


def body(
    resid, queries, keys_values, sink, out_weight, norm_gain, gate_weight, up_weight, down_weight
):
    tok = queries.shape[0]
    heads_here = queries.shape[1] // HEAD_DIM
    kv_here = keys_values.shape[1]
    group = heads_here // kv_here
    cols = resid.shape[1]
    offset = lax.axis_index("sp") * tok
    total_tokens = tok * lax.axis_size("sp")
    positions = offset + jnp.arange(tok, dtype=jnp.int32)
    rotated_q = rotate(
        queries.astype(jnp.float32).reshape(tok, heads_here, HEAD_DIM), positions
    ).astype(jnp.bfloat16)
    padded = with_halo(keys_values, (("sp", 0),), WINDOW)
    ranks, members = lax.axis_size("sp"), lax.axis_size("tp")
    high = members // 2
    direct = ranks <= 8 and ranks % 2 == 0 and members >= 2 and members & (members - 1) == 0
    if direct:
        half_columns = resid.shape[1] * members // 2
        near = jnp.where((lax.axis_index("tp") & high) > 0, half_columns, 0)
        padded, gate_weight, up_weight, down_weight = lax.optimization_barrier(
            (padded, gate_weight, up_weight, down_weight)
        )
        both = jnp.concatenate([gate_weight, up_weight], axis=1)
        (whole_both, whole_down), late = relay((both, down_weight), (0, 1), near)
    else:
        whole_both = jnp.concatenate([share(gate_weight, 0), share(up_weight, 0)], axis=1)
        whole_down = share(down_weight, 1)
    whole_out = lax.all_gather(out_weight, "tp", axis=0, tiled=True)
    key_positions = offset - WINDOW + jnp.arange(tok + 2 * WINDOW, dtype=jnp.int32)
    rotated_k = rotate(padded[..., :HEAD_DIM].astype(jnp.float32), key_positions).astype(
        jnp.bfloat16
    )
    padded = jnp.concatenate([rotated_k, padded[..., HEAD_DIM:]], axis=-1)
    blocks = tok // WINDOW
    key_blocks = jnp.stack(
        [padded[index * WINDOW : index * WINDOW + 3 * WINDOW] for index in range(blocks)]
    )
    grouped = rotated_q.reshape(blocks, WINDOW, kv_here, group, HEAD_DIM)
    scores = jnp.einsum(
        "nqkgd,njkd->nkgqj", grouped, key_blocks[..., :HEAD_DIM], preferred_element_type=jnp.float32
    ) * HEAD_DIM ** (-0.5)
    block_start = offset + WINDOW * jnp.arange(blocks, dtype=jnp.int32)
    query_pos = block_start[:, None] + jnp.arange(WINDOW, dtype=jnp.int32)[None, :]
    key_pos = block_start[:, None] - WINDOW + jnp.arange(3 * WINDOW, dtype=jnp.int32)[None, :]
    valid = (
        (jnp.abs(query_pos[:, :, None] - key_pos[:, None, :]) <= WINDOW)
        & (key_pos[:, None, :] >= 0)
        & (key_pos[:, None, :] < total_tokens)
    )
    scores = jnp.where(valid[:, None, None], scores, jnp.float32(-1e30))
    sink_grid = sink.reshape(kv_here, group)[None, :, :, None]
    top = jnp.maximum(jnp.max(scores, axis=-1), sink_grid)
    expo = jnp.exp(scores - top[..., None])
    denom = jnp.sum(expo, axis=-1) + jnp.exp(sink_grid - top)
    probs = (expo / denom[..., None]).astype(jnp.bfloat16)
    attended = jnp.einsum(
        "nkgqj,njkd->nqkgd", probs, key_blocks[..., HEAD_DIM:], preferred_element_type=jnp.float32
    )
    attended = attended.astype(jnp.bfloat16).reshape(tok, heads_here * HEAD_DIM)
    attn_rows, resid_rows = (
        lax.all_to_all(attended, "tp", split_axis=0, concat_axis=1, tiled=True),
        lax.all_to_all(resid, "tp", split_axis=0, concat_axis=1, tiled=True),
    )
    stream_part = (
        resid_rows.astype(jnp.float32)
        + jnp.dot(attn_rows, whole_out, preferred_element_type=jnp.float32)
    ).astype(jnp.bfloat16)
    stream = lax.all_gather(stream_part, "tp", axis=0, tiled=True)
    stream_cols = lax.dynamic_slice_in_dim(stream, lax.axis_index("tp") * cols, cols, 1)
    widened = stream.astype(jnp.float32)
    normed = (
        widened * lax.rsqrt(jnp.mean(widened * widened, axis=-1, keepdims=True) + 1e-06) * norm_gain
    ).astype(jnp.bfloat16)
    gate_up = jnp.dot(normed, whole_both, preferred_element_type=jnp.float32)
    gate, up = jnp.split(gate_up, 2, axis=1)
    hidden = (jax.nn.silu(gate) * up).astype(jnp.bfloat16)
    if direct:
        hidden, whole_down = lax.optimization_barrier((hidden, whole_down))
        whole_down = late(whole_down)
        far_terms = jnp.dot(
            hidden, whole_down[:, half_columns:], preferred_element_type=jnp.float32
        )
        far_sum = swap(sum_columns(far_terms, high // 2).astype(jnp.bfloat16), high)
        near_terms = jnp.dot(
            hidden, whole_down[:, :half_columns], preferred_element_type=jnp.float32
        )
        near_sum = sum_columns(near_terms, high // 2)
        return (
            stream_cols.astype(jnp.float32) + (near_sum + far_sum.astype(jnp.float32))
        ).astype(jnp.bfloat16)
    terms = jnp.dot(
        hidden,
        whole_down,
        preferred_element_type=jnp.float32,
    )
    summed = lax.psum_scatter(
        terms.astype(jnp.bfloat16), "tp", scatter_dimension=1, tiled=True
    ).astype(jnp.float32)
    return (stream_cols.astype(jnp.float32) + summed).astype(jnp.bfloat16)


LANE = 128
CHUNK = 128
PARTS = 3
BF = jnp.bfloat16
F32 = jnp.float32
WHOLE_VMEM = 67_043_328


def fits(mesh):
    return mesh.shape["sp"] == 4 and mesh.shape["tp"] == 4 and mesh.shape["grp"] == 2


def angle_tables(total):
    halo = WINDOW // GRID_W
    rows = np.arange(-halo, total // GRID_W + halo, dtype=np.float64)
    cols = np.arange(GRID_W, dtype=np.float64)
    entry = np.arange(LANE) % HEAD_DIM
    rate = 10000.0 ** (-(entry % 16) / 16.0)
    by_row = (entry // 32 == 0).astype(np.float64)
    sign = np.where(entry % 32 < 16, -1.0, 1.0)

    def table(places, used, wave, scale):
        return jnp.asarray(wave(places[:, None] * rate) * scale * used, jnp.float32)

    return (
        table(rows, by_row, np.cos, 1.0),
        table(rows, by_row, np.sin, sign),
        table(cols, 1 - by_row, np.cos, 1.0),
        table(cols, 1 - by_row, np.sin, sign),
    )


def fused_kernel(
    sink_in, row_cos_in, row_sin_in, col_cos_in, col_sin_in, gain_in,
    resid_in, q_in, kv_in, out_w_in, gate_in, up_in, down_in,
    out_hbm,
    sink, row_cos, row_sin, col_cos, col_sin, gain,
    out, q, resid, kv, cos, sin, kd, vd, out_w,
    wg, wu, wd, st, nrm, hid, ga, upa,
    own, c_out, c_in, x_out, x_in,
    ec_out, ec_in, e_own, ex_out, ex_in, ez_out, ez_in, ef_out, ef_in,
    local_sem, out_sem, h_s, h_r,
    zg_s, zg_r, yg_s, yg_r, zd_s, zd_r, yd_s, yd_r, hg_s, hd_s,
    c_s, c_r, x_s, x_r,
    ac_s, ac_r, ax_s, ax_r, af_s, af_r, az_s, az_r,
    ec_s, ec_r, ex_s, ex_r, ez_s, ez_r, ef_s, ef_r,
):
    tok, cols = q.shape
    blocks = tok // WINDOW
    depth, ff = gate_in.shape
    tiles = ff // LANE
    n_end = (tiles // 2) * LANE
    n_mid = ff - n_end
    half_d = depth // 2
    half_c = cols // 2
    subs = half_c // CHUNK
    nch = cols // CHUNK

    g, s, t = lax.axis_index("grp"), lax.axis_index("sp"), lax.axis_index("tp")
    x, c = lax.div(t, 2), lax.rem(t, 2)
    par = lax.rem(s, 2)
    mid = lax.rem(lax.div(s + 1, 2), 2)
    way = 1 - 2 * lax.div(s, 2)
    c_peer = {"tp": t + 1 - 2 * c}
    x_peer = {"tp": t + 2 - 4 * x}
    y_peer = {"grp": 1 - g}
    z_peer = {"sp": s + 1 - 2 * par}
    t_x = t + 2 - 4 * x
    t_c = t + 1 - 2 * c

    def ring(i):
        return lax.rem(s + way * i + 4, 4)

    near = ring(1 + 2 * mid)
    far = ring(3 - mid)
    adj = ring(2 - mid)

    def pick(i, values):
        found = values[0]
        for at in range(1, len(values)):
            found = jnp.where(i == at, values[at], found)
        return found

    def when(flag, fn):
        pl.when(flag)(fn)

    def by_role(fn):
        when(mid == 1, lambda: fn(n_mid, n_end))
        when(mid == 0, lambda: fn(n_end, 0))

    def span(start, size, unit):
        return pl.ds(pl.multiple_of(start, unit), size)

    def remote(src, dst, send, recv, to):
        return pltpu.make_async_remote_copy(
            src_ref=src, dst_ref=dst, send_sem=send, recv_sem=recv,
            device_id=to, device_id_type=pl.DeviceIdType.MESH,
        )

    barrier = pltpu.get_barrier_semaphore()
    partners = [c_peer, x_peer, y_peer] + [{"sp": lax.rem(s + k, 4)} for k in (1, 2, 3)]
    for to in partners:
        pl.semaphore_signal(barrier, inc=1, device_id=to, device_id_type=pl.DeviceIdType.MESH)
    locals_ = [
        pltpu.make_async_copy(kv_in, kv.at[pl.ds(WINDOW, tok)], local_sem.at[0]),
        pltpu.make_async_copy(q_in, q, local_sem.at[1]),
        pltpu.make_async_copy(out_w_in, out_w, local_sem.at[2]),
        pltpu.make_async_copy(resid_in, resid, local_sem.at[3]),
    ]
    small = [
        pltpu.make_async_copy(src, dst, local_sem.at[7 + i])
        for i, (src, dst) in enumerate((
            (row_cos_in, row_cos), (row_sin_in, row_sin), (col_cos_in, col_cos),
            (col_sin_in, col_sin), (gain_in, gain), (sink_in, sink),
        ))
    ]
    for copy in locals_ + small:
        copy.start()
    pl.semaphore_wait(barrier, len(partners))

    def halo_right():
        return remote(kv_in.at[pl.ds(tok - WINDOW, WINDOW)], kv.at[pl.ds(0, WINDOW)],
                      h_s.at[0], h_r.at[0], {"sp": lax.rem(s + 1, 4)})

    def halo_left():
        return remote(kv_in.at[pl.ds(0, WINDOW)], kv.at[pl.ds(tok + WINDOW, WINDOW)],
                      h_s.at[1], h_r.at[1], {"sp": lax.rem(s + 3, 4)})

    when(s < 3, lambda: halo_right().start())
    when(s > 0, lambda: halo_left().start())

    pieces = (
        (gate_in, wg, 0, half_d),
        (up_in, wu, 0, half_d // 2),
        (up_in, wu, half_d // 2, half_d // 2),
    )

    def gu_send(kind, d):
        n, at = (n_mid, n_end) if d in (1, 2) else (n_end, 0)
        src, dst, skip, rows = pieces[kind]
        return remote(
            src.at[span(half_d * g + skip, rows, rows), pl.ds(at, n)],
            dst.at[span(depth * s + half_d * g + skip, rows, rows), pl.ds(0, n)],
            zg_s.at[kind, d], zg_r.at[kind, s], {"sp": d},
        )

    def gu_piece(kind, src, which, n):
        _, ref, skip, rows = pieces[kind]
        return ref.at[span(depth * src + half_d * which + skip, rows, rows), pl.ds(0, n)]

    cut = -(-n_mid // LANE // PARTS) * LANE

    def dn_rows(part, n):
        return cut * part, min(cut, n - cut * part)

    def dn_send(q, d):
        n, at = (n_mid, n_end) if d in (1, 2) else (n_end, 0)
        k, part = divmod(q, PARTS)
        row, rows = dn_rows(part, n)
        return remote(
            down_in.at[pl.ds(at + row, rows), span(half_c * g + CHUNK * k, CHUNK, CHUNK)],
            wd.at[pl.ds(row, rows), span(cols * s + half_c * g + CHUNK * k, CHUNK, CHUNK)],
            zd_s.at[q, d], zd_r.at[q, s], {"sp": d},
        )

    def dn_piece(k, part, src, which, n):
        row, rows = dn_rows(part, n)
        return wd.at[pl.ds(row, rows), span(cols * src + half_c * which + CHUNK * k, CHUNK, CHUNK)]

    pair = s + 1 - 2 * par

    def to(d, send):
        for static in range(4):
            when(d == static, lambda static=static: send(static))

    def gu_to(d, kinds):
        to(d, lambda at: [gu_send(kind, at).start() for kind in kinds] and None)

    def dn_to(d):
        to(d, lambda at: [dn_send(q, at).start() for q in range(PARTS * subs)] and None)

    gate_kind, up_kinds = (0,), (1, 2)

    def first_sends(inner):
        gu_to(pair, gate_kind)
        if inner:
            gu_to(adj, gate_kind)
            gu_to(far, gate_kind)
            gu_to(pair, up_kinds)
            gu_to(adj, up_kinds)
        else:
            gu_to(far, gate_kind)
            gu_to(pair, up_kinds)

    when(mid == 1, lambda: first_sends(True))
    when(mid == 0, lambda: first_sends(False))

    def own_copies(n, at):
        return [
            pltpu.make_async_copy(gate_in.at[:, pl.ds(at, n)],
                                  wg.at[span(depth * s, depth, depth), pl.ds(0, n)], local_sem.at[4]),
            pltpu.make_async_copy(up_in.at[:, pl.ds(at, n)],
                                  wu.at[span(depth * s, depth, depth), pl.ds(0, n)], local_sem.at[5]),
            pltpu.make_async_copy(down_in.at[pl.ds(at, n), :],
                                  wd.at[pl.ds(0, n), span(cols * s, cols, cols)], local_sem.at[6]),
        ]


    def one_hot(pick):
        i = lax.broadcasted_iota(jnp.int32, (256, 256), 0)
        j = lax.broadcasted_iota(jnp.int32, (256, 256), 1)
        return jnp.where(i == pick(j), 1.0, 0.0).astype(BF)

    for copy in small:
        copy.wait()
    swap_m = one_hot(lambda j: j + 16 - 32 * lax.rem(lax.div(j, 16), 2))
    for i in range((tok + 2 * WINDOW) // GRID_W):
        r = lax.div(tok, GRID_W) * s + i
        here = pl.ds(GRID_W * i, GRID_W)
        cos[here, :] = row_cos[pl.ds(r, 1), :] + col_cos[...]
        sin[here, :] = row_sin[pl.ds(r, 1), :] + col_sin[...]

    def no_left():
        kv[pl.ds(0, WINDOW)] = jnp.zeros((WINDOW, *kv.shape[1:]), BF)

    def no_right():
        kv[pl.ds(tok + WINDOW, WINDOW)] = jnp.zeros((WINDOW, *kv.shape[1:]), BF)

    when(s == 0, no_left)
    when(s == 3, no_right)
    if n_mid > n_end:
        def no_pad():
            wd[pl.ds(n_end, n_mid - n_end), :] = jnp.zeros((n_mid - n_end, wd.shape[1]), BF)
            wg[:, pl.ds(n_end, n_mid - n_end)] = jnp.zeros((wg.shape[0], n_mid - n_end), BF)
            wu[:, pl.ds(n_end, n_mid - n_end)] = jnp.zeros((wu.shape[0], n_mid - n_end), BF)

        when(mid == 0, no_pad)

    locals_[0].wait()
    when(s > 0, lambda: halo_right().wait_recv())
    when(s < 3, lambda: halo_left().wait_recv())

    for i in range(tok // WINDOW + 2):
        here = pl.ds(WINDOW * i, WINDOW)
        raw = jnp.concatenate([kv[here, k, :] for k in range(2)], axis=1)
        lane = lax.broadcasted_iota(jnp.int32, (WINDOW, 256), 1)
        is_key = lax.rem(lane, 128) < HEAD_DIM
        turn_c = jnp.concatenate([cos[here, :]] * 2, axis=1)
        turn_s = jnp.concatenate([sin[here, :]] * 2, axis=1)
        other = jnp.dot(raw, swap_m, preferred_element_type=F32)
        value = raw.astype(F32)
        turned = jnp.where(is_key, value * turn_c + other * turn_s, value).astype(BF)
        for k in range(2):
            kd[k, here, :] = jnp.dot(
                turned, one_hot(lambda j: 128 * k + lax.rem(j, 64)), preferred_element_type=F32
            ).astype(BF)
            vd[k, here, :] = jnp.dot(
                turned, one_hot(lambda j: 128 * k + 64 + lax.rem(j, 64)), preferred_element_type=F32
            ).astype(BF)

    locals_[1].wait()
    locals_[2].wait()
    locals_[3].wait()

    def c_copy(b):
        return remote(c_out.at[b], c_in.at[b], c_s.at[b], c_r.at[b], c_peer)

    def x_copy(b):
        return remote(x_out.at[b], x_in.at[b], x_s.at[b], x_r.at[b], x_peer)

    def part(slot, b, owner):
        return st.at[span(tok * slot + WINDOW * b, WINDOW, WINDOW), span(cols * owner, cols, cols)]

    def ag_c(slot, b):
        ref = part(slot, b, t)
        return remote(ref, ref, ac_s.at[slot, b], ac_r.at[slot, b], c_peer)

    def ag_x(slot, b):
        ref = part(slot, b, t)
        return remote(ref, ref, ax_s.at[slot, b], ax_r.at[slot, b], x_peer)

    def ag_f(slot, b):
        ref = part(slot, b, t_x)
        return remote(ref, ref, af_s.at[slot, b], af_r.at[slot, b], c_peer)

    def ag_z(slot, b):
        ref = part(slot, b, t)
        return remote(ref, ref, az_s.at[b], az_r.at[b], z_peer)

    total = tok * 4

    def attend(b):
        rows = span(WINDOW * b, WINDOW, WINDOW)
        keys_at = span(WINDOW * b, 3 * WINDOW, WINDOW)
        place = span(WINDOW * b + WINDOW, WINDOW, WINDOW)
        turn_c = jnp.concatenate([cos[place, :]] * 2, axis=1)
        turn_s = jnp.concatenate([sin[place, :]] * 2, axis=1)
        head_of = lax.div(lax.broadcasted_iota(jnp.int32, (WINDOW, 256), 1), HEAD_DIM)
        i = lax.broadcasted_iota(jnp.int32, (WINDOW, 3 * WINDOW), 0)
        j = lax.broadcasted_iota(jnp.int32, (WINDOW, 3 * WINDOW), 1)
        first = tok * s + WINDOW * b - WINDOW
        valid = (j >= i) & (j <= i + 2 * WINDOW) & (j >= -first) & (j < total - first)
        bias = jnp.where(valid, 0.0, -1e30)
        outs = []
        for k in range(2):
            raw = q[rows, pl.ds(256 * k, 256)]
            other = jnp.dot(raw, swap_m, preferred_element_type=F32)
            turned = raw.astype(F32) * turn_c + other * turn_s
            stacked = jnp.concatenate(
                [jnp.where(head_of == h, turned, 0.0) for h in range(4)], axis=0
            ).astype(BF)
            scores = lax.dot_general(
                stacked, kd[k, keys_at, :], (((1,), (1,)), ((), ())), preferred_element_type=F32
            )
            probs = []
            for h in range(4):
                one = scores[WINDOW * h : WINDOW * (h + 1)] * HEAD_DIM ** (-0.5) + bias
                level = sink[:, pl.ds(4 * k + h, 1)]
                top = jnp.maximum(jnp.max(one, axis=1, keepdims=True), level)
                expo = jnp.exp(one - top)
                denom = jnp.sum(expo, axis=1, keepdims=True) + jnp.exp(level - top)
                probs.append((expo * (1.0 / denom)).astype(BF))
            mixed = jnp.dot(
                jnp.concatenate(probs, axis=0), vd[k, keys_at, :], preferred_element_type=F32
            )
            acc = jnp.zeros((WINDOW, 256), F32)
            for h in range(4):
                acc = jnp.where(head_of == h, mixed[WINDOW * h : WINDOW * (h + 1)], acc)
            outs.append(acc.astype(BF))
        att = jnp.concatenate(outs, axis=1)
        for xx in range(2):
            at = pl.ds(cols * xx, cols)
            c_out[b, :, at] = jnp.dot(
                att, out_w[:, span((2 * xx + 1 - c) * cols, cols, cols)], preferred_element_type=F32
            ).astype(BF)
            own[b, :, at] = jnp.dot(
                att, out_w[:, span((2 * xx + c) * cols, cols, cols)], preferred_element_type=F32
            )
        c_copy(b).start()

    def over_x(b):
        c_copy(b).wait_recv()
        mine, theirs = span(cols * x, cols, cols), span(cols * (1 - x), cols, cols)
        x_out[b] = (own[b, :, theirs] + c_in[b, :, theirs].astype(F32)).astype(BF)
        own[b, :, mine] = own[b, :, mine] + c_in[b, :, mine].astype(F32)
        x_copy(b).start()

    def to_stream(b):
        x_copy(b).wait_recv()
        rows = span(WINDOW * b, WINDOW, WINDOW)
        value = resid[rows, :].astype(F32) + (
            own[b, :, span(cols * x, cols, cols)] + x_in[b].astype(F32)
        )
        st[span(tok * par + WINDOW * b, WINDOW, WINDOW), span(cols * t, cols, cols)] = value.astype(BF)
        ag_z(par, b).start()
        ag_x(par, b).start()
        ag_c(par, b).start()


    def recv_x(slot, b):
        ref = part(slot, b, t_x)
        remote(ref, ref, ax_s.at[slot, b], ax_r.at[slot, b], x_peer).wait_recv()

    def recv_c(slot, b):
        ref = part(slot, b, t_c)
        remote(ref, ref, ac_s.at[slot, b], ac_r.at[slot, b], c_peer).wait_recv()

    def recv_f(slot, b):
        ref = part(slot, b, t_c + 2 - 4 * x)
        remote(ref, ref, af_s.at[slot, b], af_r.at[slot, b], c_peer).wait_recv()

    def recv_z(slot, b):
        ref = part(slot, b, t)
        remote(ref, ref, az_s.at[b], az_r.at[b], z_peer).wait_recv()

    def gu_pass(kind, src, n):
        piece = gu_piece(kind, src, g, n)
        remote(piece, piece, zg_s.at[kind, src], zg_r.at[kind, src], z_peer).wait_recv()
        remote(piece, piece, yg_s.at[kind, src], yg_r.at[kind, src], y_peer).start()
        if src is near and n == n_mid:
            gu_hop(kind).start()

    def gu_hop(kind):
        piece = gu_piece(kind, near, g, n_mid)
        return remote(piece, piece, hg_s.at[kind], zg_r.at[kind, near], {"sp": adj})

    def dn_hop(q):
        piece = dn_piece(q // PARTS, q % PARTS, near, g, n_mid)
        return remote(piece, piece, hd_s.at[q], zd_r.at[q, near], {"sp": adj})

    def gu_got(kind, src):
        def go(n, at):
            piece = gu_piece(kind, src, 1 - g, n)
            remote(piece, piece, yg_s.at[kind, src], yg_r.at[kind, src], y_peer).wait_recv()

        by_role(go)

    def dn_pass(k, src):
        def go(n, at):
            for part in range(PARTS):
                q = PARTS * k + part
                piece = dn_piece(k, part, src, g, n)
                remote(piece, piece, zd_s.at[q, src], zd_r.at[q, src], z_peer).wait_recv()
                remote(piece, piece, yd_s.at[q, src], yd_r.at[q, src], y_peer).start()
                if src is near and n == n_mid:
                    dn_hop(q).start()

        by_role(go)

    def dn_got(k, src):
        def go(n, at):
            for part in range(PARTS):
                q = PARTS * k + part
                piece = dn_piece(k, part, src, 1 - g, n)
                remote(piece, piece, yd_s.at[q, src], yd_r.at[q, src], y_peer).wait_recv()

        by_role(go)

    def normalize(slot, b):
        rows_at_once = 32

        def rows_of(i, _):
            here = span(tok * slot + WINDOW * b + rows_at_once * i, rows_at_once, rows_at_once)
            wide = st[here, :].astype(F32)
            scale = lax.rsqrt(jnp.mean(wide * wide, axis=1, keepdims=True) + 1e-06)
            nrm[here, :] = (wide * scale * gain[...]).astype(BF)
            return 0

        lax.fori_loop(0, WINDOW // rows_at_once, rows_of, 0)

    last, third = ring(2), ring(3 - 2 * mid)
    relay_mid = ((gate_kind, near), (gate_kind, adj), (up_kinds, near),
                 (up_kinds, adj), (gate_kind, far), (up_kinds, far))
    relay_end = ((gate_kind, near), (gate_kind, far), (up_kinds, near),
                 (gate_kind, adj), (up_kinds, far), (up_kinds, adj))

    def relay(r):
        def go(table, n):
            kinds, src = table[r]
            for kind in kinds:
                gu_pass(kind, src, n)

        def inner():
            go(relay_mid, n_mid)
            if r == 2:
                gu_to(far, up_kinds)

        when(mid == 1, inner)
        when(mid == 0, lambda: go(relay_end, n_end))

    def own_pass(b):
        recv_x(par, b)
        ag_f(par, b).start()

    def step(i, _):
        for r in range(3):
            when(i == 3 + r, lambda r=r: relay(r))
        when(i < blocks, lambda: attend(i))
        when((i >= 1) & (i < blocks + 1), lambda: over_x(i - 1))
        when((i >= 2) & (i < blocks + 2), lambda: to_stream(i - 2))
        when(i >= 3, lambda: own_pass(i - 3))
        return 0

    lax.fori_loop(0, blocks + 3, step, 0)

    def late():
        gu_to(far, up_kinds)
        dn_to(pair)

    when(mid == 0, late)
    when(mid == 1, lambda: dn_to(pair))
    by_role(lambda n, at: [copy.start() for copy in own_copies(n, at)] and None)
    relay(3)

    other_par = 1 - par

    def pair_pass(b, _):
        def first():
            recv_z(other_par, b)
            ag_x(other_par, b).start()
            ag_c(other_par, b).start()

        def second():
            recv_x(other_par, b - 2)
            ag_f(other_par, b - 2).start()

        def third():
            recv_c(par, b)
            recv_f(par, b)
            normalize(par, b)

        when(b < blocks, first)
        when(b < blocks, third)
        when(b >= 2, second)
        when(b == 3 - mid, lambda: relay(4))
        return 0

    lax.fori_loop(0, blocks + 2, pair_pass, 0)

    def pair_in(b, _):
        recv_c(other_par, b)
        recv_f(other_par, b)
        normalize(other_par, b)
        return 0

    def inner_down():
        for k in range(subs):
            dn_pass(k, near)
        dn_to(far)
        dn_to(adj)

    when(mid == 1, lambda: relay(5))
    when(mid == 1, inner_down)
    lax.fori_loop(0, blocks, pair_in, 0)
    by_role(lambda n, at: [copy.wait() for copy in own_copies(n, at)] and None)
    for src in (near, adj, far):
        gu_got(0, src)
    wide = 2 * LANE

    def gate_tile(j, _):
        at = span(wide * j, wide, wide)
        gate = jnp.dot(nrm[...], wg[:, at], preferred_element_type=F32)
        ga[:, at] = gate / (1.0 + jnp.exp(-gate))
        for r, kind in enumerate(up_kinds):
            when((j == r) & (mid == 0), lambda kind=kind: gu_pass(kind, last, n_end))
        return 0

    def up_term(src, at):
        rows = span(depth * src, depth, depth)
        return jnp.dot(nrm[:, rows], wu[rows, at], preferred_element_type=F32)

    def up_tile(j, _):
        at = span(wide * j, wide, wide)
        upa[:, at] = up_term(s, at) + up_term(near, at) + up_term(third, at)
        return 0

    def hid_tile(j, _):
        at = span(wide * j, wide, wide)
        hid[:, at] = (ga[:, at] * (upa[:, at] + up_term(last, at))).astype(BF)
        return 0

    lax.fori_loop(0, n_mid // wide, gate_tile, 0)
    def end_down():
        dn_to(far)
        for k in range(subs):
            dn_pass(k, near)

    when(mid == 0, end_down)
    gu_got(1, near)
    gu_got(2, near)
    gu_got(1, third)
    gu_got(2, third)
    lax.fori_loop(0, n_mid // wide, up_tile, 0)
    gu_got(1, last)
    gu_got(2, last)
    lax.fori_loop(0, n_mid // wide, hid_tile, 0)

    def chunk(i):
        at = lax.div(i, subs)
        k = lax.rem(i, subs)
        b = pick(at, (0, 0, 1, 2, 2, 1, 3, 3))
        first = pick(at, (0, 1, 0, 0, 1, 1, 0, 1))
        half = first * (1 - g) + (1 - first) * g
        source = pick(b, (s, far, near, adj))
        return b, first, k, half * subs + k, source

    def ec(xo, ch):
        return remote(ec_out.at[xo, ch], ec_in.at[xo, ch], ec_s.at[xo, ch], ec_r.at[xo, ch], c_peer)

    def ex(ch, which):
        rows = span(tok * (other_par, par)[which], tok, tok)
        return remote(ex_out.at[ch, rows], ex_in.at[ch, rows],
                      ex_s.at[which, ch], ex_r.at[which, ch], x_peer)

    def ez(ch):
        return remote(ez_out.at[ch], ez_in.at[ch], ez_s.at[ch], ez_r.at[ch], z_peer)

    steps = 4 * nch

    def produce(i):
        b, first, k, ch, source = chunk(i)
        when((b > 0) & (first == 1), lambda: dn_got(k, source))
        xo, co = lax.div(source, 2), lax.rem(source, 2)
        term = jnp.dot(
            hid[...], wd[:, span(cols * source + CHUNK * ch, CHUNK, CHUNK)],
            preferred_element_type=F32,
        )

        def send():
            ec_out[xo, ch] = term.astype(BF)
            ec(xo, ch).start()

        def keep():
            e_own[xo, ch] = term

        when(co != c, send)
        when(co == c, keep)

    def combine(i):
        _, _, _, ch, source = chunk(i)
        xo, co = lax.div(source, 2), lax.rem(source, 2)

        def mine():
            ec(xo, ch).wait_recv()
            value = e_own[xo, ch] + ec_in[xo, ch].astype(F32)

            def send():
                ex_out[ch] = value.astype(BF)
                ex(ch, 0).start()

            def keep():
                e_own[xo, ch] = value

            when(xo != x, send)
            when(xo == x, keep)

        when(co == c, mine)

    theirs = span(tok * other_par, tok, tok)
    ours = span(tok * par, tok, tok)

    def rest(i):
        _, _, _, ch, source = chunk(i)
        when((lax.rem(source, 2) == c) & (lax.div(source, 2) != x), lambda: ex(ch, 1).start())

    def deliver(i):
        _, _, _, ch, source = chunk(i)

        def mine():
            ex(ch, 0).wait_recv()
            ez_out[ch] = (e_own[x, ch, theirs, :] + ex_in[ch, theirs, :].astype(F32)).astype(BF)
            ez(ch).start()

        when(source == t, mine)

    def ahead(stage):
        lax.fori_loop(0, steps, lambda j, _: when(soon(j) == stage, lambda: deliver(j)) or 0, 0)

    def soon(i):
        return pick(lax.div(i, subs), (1, 1, 1, 2, 3, 2, 0, 0))

    adj_x, adj_c = lax.div(adj, 2), lax.rem(adj, 2)

    def ef(ch):
        return remote(ef_out.at[ch], ef_in.at[ch], ef_s.at[ch], ef_r.at[ch], z_peer)

    def combine_adj(i):
        _, _, _, ch, _ = chunk(i)

        def mine():
            ec(adj_x, ch).wait_recv()
            ef_out[ch] = (e_own[adj_x, ch, theirs, :] + ec_in[adj_x, ch, theirs, :].astype(F32)).astype(BF)
            ef(ch).start()
            e_own[adj_x, ch, ours, :] = (
                e_own[adj_x, ch, ours, :] + ec_in[adj_x, ch, ours, :].astype(F32)
            )

        when(adj_c == c, mine)

    def relay_adj(i):
        _, _, _, ch, _ = chunk(i)

        def mine():
            ef(ch).wait_recv()
            value = e_own[adj_x, ch, ours, :] + ef_in[ch].astype(F32)

            def send():
                ex_out[ch, ours, :] = value.astype(BF)
                ex(ch, 1).start()

            def keep():
                e_own[adj_x, ch, ours, :] = value

            when(adj_x != x, send)
            when(adj_x == x, keep)

        when(adj_c == c, mine)

    def stretch(first, stop, join=combine):
        def go(i, _):
            when(i < stop, lambda: produce(i))
            when(i >= first + 2, lambda: join(i - 2))
            return 0

        lax.fori_loop(first, stop + 2, go, 0)

    def relays(first, stop):
        lax.fori_loop(first, stop, lambda i, _: relay_adj(i) or 0, 0)

    stretch(0, 2 * subs)
    for k in range(subs):
        dn_pass(k, far)
    stretch(2 * subs, 6 * subs)
    lax.fori_loop(0, 6 * subs, lambda i, _: rest(i) or 0, 0)
    ahead(1)
    for k in range(subs):
        dn_pass(k, adj)
    when(mid == 1, lambda: ahead(2))
    stretch(6 * subs, 7 * subs, combine_adj)
    when(mid == 1, lambda: relays(6 * subs, 7 * subs))
    stretch(7 * subs, steps, combine_adj)
    when(mid == 0, lambda: ahead(2))
    ahead(3)
    when(s < 3, lambda: halo_right().wait_send())
    when(s > 0, lambda: halo_left().wait_send())
    for d in range(4):
        def sent(d=d):
            for kind in range(3):
                gu_send(kind, d).wait_send()
            for q in range(PARTS * subs):
                dn_send(q, d).wait_send()

        when((s != d) & ((mid == 1) | (adj != d)), sent)

    def hopped():
        for kind in range(3):
            gu_hop(kind).wait_send()
        for q in range(PARTS * subs):
            dn_hop(q).wait_send()

    when(mid == 1, hopped)

    def relayed(n, at):
        for src in (near, far, adj):
            for kind in range(3):
                piece = gu_piece(kind, src, g, n)
                remote(piece, piece, yg_s.at[kind, src], yg_r.at[kind, src], y_peer).wait_send()
            for q in range(PARTS * subs):
                piece = dn_piece(q // PARTS, q % PARTS, src, g, n)
                remote(piece, piece, yd_s.at[q, src], yd_r.at[q, src], y_peer).wait_send()

    by_role(relayed)

    def blocks_sent(b, _):
        c_copy(b).wait_send()
        x_copy(b).wait_send()
        ag_z(par, b).wait_send()
        for slot in range(2):
            ag_c(slot, b).wait_send()
            ag_x(slot, b).wait_send()
            ag_f(slot, b).wait_send()
        return 0

    lax.fori_loop(0, blocks, blocks_sent, 0)

    def cores_sent(ch, _):
        for xo in range(2):
            ec(xo, ch).wait_send()
        return 0

    lax.fori_loop(0, nch, cores_sent, 0)

    when(mid == 0, lambda: relays(6 * subs, 7 * subs))
    relays(7 * subs, steps)

    def leave(ch):
        at = span(CHUNK * ch, CHUNK, CHUNK)
        return pltpu.make_async_copy(out.at[:, at], out_hbm.at[:, at], out_sem.at[ch])

    def finish(ch, _):
        ex(ch, 1).wait_recv()
        when(t != adj, lambda: ez(ch).wait_recv())
        at = span(CHUNK * ch, CHUNK, CHUNK)
        base = st[ours, span(cols * t + CHUNK * ch, CHUNK, CHUNK)].astype(F32)
        mine = e_own[x, ch, ours, :] + ex_in[ch, ours, :].astype(F32)

        def joined():
            out[:, at] = (base + (mine + ez_in[ch].astype(F32))).astype(BF)

        def whole():
            out[:, at] = (base + mine).astype(BF)

        when(t != adj, joined)
        when(t == adj, whole)
        leave(ch).start()
        return 0

    lax.fori_loop(0, nch, finish, 0)

    def chunks_sent(ch, _):
        when(t_x != adj, lambda: ex(ch, 0).wait_send())
        ex(ch, 1).wait_send()
        leave(ch).wait()
        when(t != adj, lambda: ez(ch).wait_send())
        when(adj_c == c, lambda: ef(ch).wait_send())
        return 0

    lax.fori_loop(0, nch, chunks_sent, 0)


def fused_body(
    resid, queries, keys_values, sink, out_weight, norm_gain, gate_weight, up_weight, down_weight
):
    tok, cols = queries.shape
    width = norm_gain.shape[0]
    ff = gate_weight.shape[1]
    n_mid = ff - (ff // LANE // 2) * LANE
    blocks = tok // WINDOW
    padded = tok + 2 * WINDOW
    nch = cols // CHUNK
    subs = nch // 2
    vmem = lambda shape, dtype=BF: pltpu.VMEM(shape, dtype)
    dma = lambda *shape: pltpu.SemaphoreType.DMA(shape)
    in_hbm = pl.BlockSpec(memory_space=pl.ANY)
    rows = tok * 4 // GRID_W + 2 * (WINDOW // GRID_W)
    scratch = [
        vmem((1, sink.shape[0]), F32), vmem((rows, LANE), F32), vmem((rows, LANE), F32),
        vmem((GRID_W, LANE), F32), vmem((GRID_W, LANE), F32), vmem((1, width), F32),
        vmem((tok, cols)), vmem((tok, cols)), vmem((tok, cols)), vmem((padded, *keys_values.shape[1:])),
        vmem((padded, LANE), F32), vmem((padded, LANE), F32),
        vmem((2, padded, 256)), vmem((2, padded, 256)), vmem(out_weight.shape),
        vmem((width, n_mid)), vmem((width, n_mid)), vmem((n_mid, width)),
        vmem((2 * tok, width)), vmem((2 * tok, width)), vmem((2 * tok, n_mid)),
        vmem((2 * tok, n_mid), F32), vmem((2 * tok, n_mid), F32),
        vmem((blocks, WINDOW, 2 * cols), F32), vmem((blocks, WINDOW, 2 * cols)),
        vmem((blocks, WINDOW, 2 * cols)), vmem((blocks, WINDOW, cols)), vmem((blocks, WINDOW, cols)),
        vmem((2, nch, 2 * tok, CHUNK)), vmem((2, nch, 2 * tok, CHUNK)),
        vmem((2, nch, 2 * tok, CHUNK), F32),
        vmem((nch, 2 * tok, CHUNK)), vmem((nch, 2 * tok, CHUNK)),
        vmem((nch, tok, CHUNK)), vmem((nch, tok, CHUNK)),
        vmem((nch, tok, CHUNK)), vmem((nch, tok, CHUNK)),
        dma(13), dma(nch), dma(2), dma(2),
        dma(3, 4), dma(3, 4), dma(3, 4), dma(3, 4),
        *[dma(PARTS * subs, 4)] * 4, dma(3), dma(PARTS * subs),
        dma(blocks), dma(blocks), dma(blocks), dma(blocks),
        dma(2, blocks), dma(2, blocks), dma(2, blocks), dma(2, blocks),
        dma(2, blocks), dma(2, blocks), dma(blocks), dma(blocks),
        dma(2, nch), dma(2, nch), dma(2, nch), dma(2, nch), dma(nch), dma(nch),
        dma(nch), dma(nch),
    ]
    return pl.pallas_call(
        fused_kernel,
        out_shape=jax.ShapeDtypeStruct((tok, cols), BF),
        in_specs=[in_hbm] * 13,
        out_specs=in_hbm,
        scratch_shapes=scratch,
        compiler_params=pltpu.CompilerParams(
            collective_id=0, has_side_effects=True, vmem_limit_bytes=WHOLE_VMEM
        ),
    )(
        sink.reshape(1, -1), *angle_tables(tok * 4), norm_gain.reshape(1, width),
        resid, queries, keys_values, out_weight, gate_weight, up_weight, down_weight,
    )


def solution(mesh):
    return jax.shard_map(
        fused_body if fits(mesh) else body,
        mesh=mesh,
        in_specs=(
            P(("grp", "sp"), "tp"),
            P(("grp", "sp"), "tp"),
            P(("grp", "sp"), "tp", None),
            P("tp"),
            P("tp", None),
            P(),
            P("sp", "tp"),
            P("sp", "tp"),
            P("tp", "sp"),
        ),
        out_specs=P(("grp", "sp"), "tp"),
        check_vma=False,
    )
```
